512 devices in a mesh: ep: 32 (over z, core), tp: 16 (over y, x).
Axes of the slice: x: 4, y: 4, z: 16, core: 2. Of those that a mesh axis runs over, the one named last changes fastest.
Arguments:
- query_pairs: bfloat16 [12288, 2048], P('ep', 'tp'), may hold values from -64 to 64
- key_pairs: bfloat16 [12288, 2048], P('ep', 'tp'), may hold values from -64 to 64
- value_rows: bfloat16 [12288, 2048], P('ep', 'tp'), may hold values from -6 to 6
- head_lambda: float32 [16], P('tp'), may hold values from 0.3 to 0.8
- head_gain: float32 [128], replicated, may hold values from 0.1 to 1.9
- out_weight: bfloat16 [2048, 2048], P('tp'), may hold values from -0.1875 to 0.1875
- moe_input: bfloat16 [5120, 2048], P('ep'), may hold values from -6 to 6
- ffn_gain: float32 [2048], replicated, may hold values from 0.1 to 1.9
- routes: int32 [5120, 2], P('ep'), may hold values from 0 to 31, all different within a row; in each aligned block of 160 rows (0 to 159, 160 to 319, ...) at most 12 rows name the same one
- route_weight: float32 [5120, 2], P('ep'), may hold values from 0.25 to 2.5
- gate_weight: bfloat16 [32, 2048, 2048], P('ep', None, 'tp'), may hold values from -0.125 to 0.125
- up_weight: bfloat16 [32, 2048, 2048], P('ep', None, 'tp'), may hold values from -0.125 to 0.125
- down_weight: bfloat16 [32, 2048, 2048], P('ep', 'tp'), may hold values from -0.1875 to 0.1875
- shared_gate: bfloat16 [2048, 2048], P(None, 'tp'), may hold values from -0.125 to 0.125
- shared_up: bfloat16 [2048, 2048], P(None, 'tp'), may hold values from -0.125 to 0.125
- shared_down: bfloat16 [2048, 2048], P('tp'), may hold values from -0.1875 to 0.1875
Outputs:
- attn_out: bfloat16 [12288, 2048], P('ep', 'tp')
- moe_out: bfloat16 [5120, 2048], P('ep', 'tp')
The draws below stay inside these ranges and needn't reach their ends.
Inputs may be any that keep to these rules, and one draw needn't show every extreme that they name: `routes`: in each aligned block of 160 rows (the rows of one device along ep) no expert is named more than 12 times, a bound that some block reaches; a row names 2 different experts.
All inputs are finite; a program needn't handle non-finite values.
Results may differ from the reference program's by a relative error of at most 0.017.
The reference program's roundings to bfloat16 on the way count: a program that leaves them out, or rounds other values in their place, can miss the bound.
Values may be sent and summed in bfloat16 or wider, within the bound.
A program may use at most 64 MiB of HBM per device.

```python
import math
import jax
import jax.numpy as jnp
import numpy as np
from jax import lax

D = 2048
HEADS = 16
HEAD = 64
VHEAD = 128
FF = 2048
SFF = 2048
TOP_K = 2
KEY_BLOCK = 128
TOK_B = 160
TOKENS_A = 12288
TOKENS_B = 5120
EXPERTS = 32
CAP = 12
N_TP = 16


def paired_draw(key):
    draw_shape = (TOKENS_A, HEADS, 2, HEAD)
    queries = 1.3 * jax.random.truncated_normal(jax.random.fold_in(key, 101), -4.0, 4.0, draw_shape, jnp.float32)
    keyset = 1.3 * jax.random.truncated_normal(jax.random.fold_in(key, 102), -4.0, 4.0, draw_shape, jnp.float32)
    return (jnp.clip(queries, -64.0, 64.0), jnp.clip(keyset, -64.0, 64.0))


def draw_query_pairs(key, part):
    return paired_draw(key)[0].reshape(TOKENS_A, HEADS * 2 * HEAD).astype(jnp.bfloat16)


def draw_key_pairs(key, part):
    return paired_draw(key)[1].reshape(TOKENS_A, HEADS * 2 * HEAD).astype(jnp.bfloat16)


def with_spikes(entries, rng, source, target, blocks, factor):
    owner, partner = [(jnp.arange(entries.shape[axis_at]) // (entries.shape[axis_at] // blocks)).reshape([-1 if axis == axis_at else 1 for axis in range(entries.ndim)]) for axis_at in (source, target)]
    chosen = jax.random.permutation(rng, blocks)[partner]
    strong = (owner == chosen) | (owner == (partner + blocks // 2) % blocks)
    return jnp.where(strong, factor * entries, entries)


def level_of(key, dims, split, smallest, high):
    level, own = 1.0, jax.random.fold_in(key, 6)
    for dim, parts in split:
        draws = jnp.exp(jax.random.uniform(jax.random.fold_in(own, dim), (parts,), jnp.float32, smallest / len(split), high / len(split)))
        level = level * jnp.repeat(draws, dims[dim] // parts).reshape([-1 if axis == dim else 1 for axis in range(len(dims))])
    return level


def routed_block(own_key, own, number, rows, count, top, limit, lean):
    order = jax.random.permutation(own_key, count)
    heavy_load, usual = portions_of(count, rows * top, limit, lean, True), portions_of(count, rows * top, limit, lean, False)
    places = jnp.arange(count)

    def named(tallies, turn):
        used = int((tallies > 0).sum())
        fixed = max(1, used // 4)
        passed = fixed + (places - fixed + turn * (used - fixed)) % max(1, count - fixed)
        return jnp.zeros((count,), jnp.int32).at[order[jnp.where(places < fixed, places, passed)]].set(jnp.asarray(tallies, jnp.int32))

    tallies = jnp.where(number % 4 == 0, named(heavy_load, number // 4), named(usual, number - number // 4 - 1))
    mixed = jax.random.permutation(jax.random.fold_in(own, 3), count)
    source_of, taker = mixed[0:count // 2 * 2:2], mixed[1:count // 2 * 2:2]
    slack = jnp.minimum(tallies[source_of] - 1, limit - tallies[taker]) // 2
    slack = jnp.where((source_of == order[0]) | (taker == order[0]) | (tallies[taker] == 0), 0, jnp.maximum(slack, 0))
    passed = jax.random.randint(jax.random.fold_in(own, 4), (count // 2,), 0, 1 << 20) % (slack + 1)
    tallies = tallies.at[source_of].add(-passed).at[taker].add(passed)
    labels = jnp.searchsorted(jnp.cumsum(tallies), jnp.arange(rows * top), side="right").astype(jnp.int32)
    grid = labels.reshape(top, rows).T
    grid = grid[jax.random.permutation(jax.random.fold_in(own, 1), rows)]
    turn = jax.random.randint(jax.random.fold_in(own, 2), (rows, 1), 0, top)
    return jnp.take_along_axis(grid, (jnp.arange(top)[None, :] + turn) % top, axis=1)


def portions_of(number_of, total, limit, slope, full):
    weights = [(1 << 20) // math.isqrt(standing ** slope) + 1 for standing in range(1, number_of + 1)]
    largest = limit if full else min(limit, max(-(-total // number_of), total * weights[0] // sum(weights)))
    least = 1 if total - largest >= number_of - 1 else 0
    counts, spare = [largest] + [least] * (number_of - 1), total - largest - least * (number_of - 1)
    while spare > 0:
        free = [i for i in range(1, number_of) if counts[i] < largest] or [i for i in range(1, number_of) if counts[i] < limit]
        mass, remaining = sum([weights[i] for i in free]), spare
        for i in free:
            more = min(limit - counts[i], max(1, remaining * weights[i] // mass), spare)
            counts[i] = counts[i] + more
            spare = spare - more
    return np.array(counts)


def scatter_about(rng, dims, scale, bound, shards=(), held_as=jnp.bfloat16):
    loudness = level_of(rng, dims, shards, -0.22, 0.18) if shards else 1.0
    drawn = jax.random.normal(rng, dims, jnp.float32) * scale * loudness
    return jnp.minimum(jnp.maximum(drawn, -bound), bound).astype(held_as)


def bell_draw_with(stream_key, shape, width, limit, shards, heavy, kind=jnp.bfloat16):
    values = width * jax.random.normal(stream_key, shape, jnp.float32)
    if shards:
        values = values * level_of(stream_key, shape, shards, -0.22, 0.18)
    return jnp.clip(with_spikes(values, jax.random.fold_in(stream_key, 3), *heavy), -limit, limit).astype(kind)


def setup_inputs(seed: int = 0) -> dict:
    streams_of = jax.random.split(jax.random.key(seed), 17)
    query_pairs = draw_query_pairs(jax.random.fold_in(streams_of[16], 71), 0)
    key_pairs = draw_key_pairs(jax.random.fold_in(streams_of[16], 71), 0)
    value_rows = scatter_about(streams_of[2], (TOKENS_A, HEADS * VHEAD), 1.0, 6.0, ((0, 32), (1, 16)))
    head_lambda = jnp.clip(0.3 + 0.5 * jax.random.uniform(streams_of[3], (HEADS,), jnp.float32) ** level_of(streams_of[3], (HEADS,), ((0, 16),), -0.2, 0.2), 0.3, 0.8)
    head_gain = jnp.clip(1.0 + 0.18 * jax.random.normal(streams_of[4], (VHEAD,), jnp.float32), 0.1, 1.9)
    out_weight = bell_draw_with(streams_of[5], (HEADS * VHEAD, D), (HEADS * VHEAD) ** -0.5, 0.1875, ((0, 16),), (0, 1, 16, 2.0))
    moe_input = scatter_about(streams_of[6], (TOKENS_B, D), 1.0, 6.0, ((0, 32),))
    ffn_gain = jnp.clip(1.0 + 0.18 * jax.random.normal(streams_of[7], (D,), jnp.float32), 0.1, 1.9)
    routes_keys = jax.random.split(jax.random.fold_in(streams_of[8], 1), TOKENS_B // TOK_B)
    routes_turns = jax.random.permutation(jax.random.fold_in(streams_of[8], 3), TOKENS_B // TOK_B)
    routes = jax.vmap(lambda own, number: routed_block(jax.random.fold_in(streams_of[8], 2), own, number, TOK_B, EXPERTS, TOP_K, CAP, 1))(routes_keys, routes_turns).reshape((TOKENS_B, TOP_K))
    route_weight = jnp.clip(jnp.exp(math.log(2.5) - 2.3025851 * jax.random.uniform(streams_of[9], (TOKENS_B, TOP_K), jnp.float32) ** level_of(streams_of[9], (TOKENS_B, TOP_K), ((0, 32),), -0.2, 0.2)), 0.25, 2.5)
    gate_weight = scatter_about(streams_of[10], (EXPERTS, D, FF), D ** -0.5, 0.125, ((0, 32), (2, 16)))
    up_weight = scatter_about(streams_of[11], (EXPERTS, D, FF), D ** -0.5, 0.125, ((0, 32), (2, 16)))
    down_weight = bell_draw_with(streams_of[12], (EXPERTS, FF, D), FF ** -0.5, 0.1875, ((0, 32), (1, 16)), (1, 2, 16, 2.0))
    shared_gate = scatter_about(streams_of[13], (D, SFF), D ** -0.5, 0.125, ((1, 16),))
    shared_up = scatter_about(streams_of[14], (D, SFF), D ** -0.5, 0.125, ((1, 16),))
    shared_down = bell_draw_with(streams_of[15], (SFF, D), SFF ** -0.5, 0.1875, ((0, 16),), (0, 1, 16, 2.0))
    return {"query_pairs": query_pairs, "key_pairs": key_pairs, "value_rows": value_rows, "head_lambda": head_lambda, "head_gain": head_gain, "out_weight": out_weight, "moe_input": moe_input, "ffn_gain": ffn_gain, "routes": routes, "route_weight": route_weight, "gate_weight": gate_weight, "up_weight": up_weight, "down_weight": down_weight, "shared_gate": shared_gate, "shared_up": shared_up, "shared_down": shared_down}


theta_base = 500000.0
norm_eps = 1e-06
masked_low = -1e+30

def rotate(inputs, positions):
    half_size = inputs.shape[-1] // 2
    frequency = theta_base ** (-(jnp.arange(half_size, dtype=jnp.float32) * 2.0) / inputs.shape[-1])
    angles = positions.astype(jnp.float32)[:, None] * frequency[None, :]
    cosine = jnp.cos(angles)[:, None, None, :]
    sine_part = jnp.sin(angles)[:, None, None, :]
    front_half = inputs[..., :half_size]
    back_half = inputs[..., half_size:]
    return jnp.concatenate([front_half * cosine - back_half * sine_part, back_half * cosine + front_half * sine_part], axis=-1)

def attention(query_pairs, key_pairs, value_rows, head_lambda, head_gain, out_weight):
    total_rows = query_pairs.shape[0]
    head_count = head_lambda.shape[0]
    head_size = query_pairs.shape[1] // (2 * head_count)
    value_size = value_rows.shape[1] // head_count
    positions = jnp.arange(total_rows, dtype=jnp.int32)
    rot_queries = rotate(query_pairs.astype(jnp.float32).reshape(total_rows, head_count, 2, head_size), positions).astype(jnp.bfloat16)
    rot_keys = rotate(key_pairs.astype(jnp.float32).reshape(total_rows, head_count, 2, head_size), positions).astype(jnp.bfloat16)
    key_blocks = total_rows // KEY_BLOCK
    block_keys = rot_keys.reshape(key_blocks, KEY_BLOCK, head_count, 2, head_size).astype(jnp.float32)
    block_values = value_rows.reshape(key_blocks, KEY_BLOCK, head_count, value_size).astype(jnp.float32)
    key_positions = positions.reshape(key_blocks, KEY_BLOCK)
    query_block = math.gcd(total_rows, 256)
    query_count = total_rows // query_block

    def one_block(inputs):
        block_queries, query_positions = inputs
        scores = jnp.einsum('qhmd,bkhmd->hmqbk', block_queries.astype(jnp.float32), block_keys) * head_size ** (-0.5)
        allowed = key_positions[None, :, :] <= query_positions[:, None, None]
        scores = jnp.where(allowed, scores, masked_low)
        block_max = lax.optimization_barrier(jnp.max(scores, axis=-1))
        weights = jnp.where(allowed, jnp.exp(scores - block_max[..., None]), 0.0)
        block_sum = lax.optimization_barrier(jnp.sum(weights, axis=-1))
        rounded = lax.optimization_barrier(weights.astype(jnp.bfloat16)).astype(jnp.float32)
        block_out = jnp.einsum('hmqbk,bkhc->hmqbc', rounded, block_values)
        row_max = lax.optimization_barrier(jnp.max(block_max, axis=-1, keepdims=True))
        rescale = jnp.exp(block_max - row_max)
        summed = lax.optimization_barrier(jnp.sum(rescale * block_sum, axis=-1))
        combined = lax.optimization_barrier(jnp.sum(rescale[..., None] * block_out, axis=-2))
        return combined / summed[..., None]
    outputs = lax.map(one_block, (rot_queries.reshape(query_count, query_block, head_count, 2, head_size), positions.reshape(query_count, query_block)))
    difference = outputs[:, :, 0] - head_lambda[None, :, None, None] * outputs[:, :, 1]
    inverse_rms = lax.rsqrt(lax.optimization_barrier(jnp.mean(difference * difference, axis=-1, keepdims=True)) + norm_eps)
    normed = (difference * inverse_rms * head_gain.astype(jnp.float32)).astype(jnp.bfloat16)
    normed = normed.transpose(0, 2, 1, 3).reshape(total_rows, head_count * value_size)
    group_cols = head_count * value_size // N_TP
    grouped = normed.reshape(total_rows, N_TP, group_cols).transpose(1, 0, 2)
    weight_groups = out_weight.reshape(N_TP, group_cols, out_weight.shape[1])

    def add_group(running, block_parts):
        partial_out = jnp.dot(block_parts[0], block_parts[1], preferred_element_type=jnp.float32)
        return (running + lax.optimization_barrier(partial_out.astype(jnp.bfloat16)).astype(jnp.float32), None)
    result, _ = lax.scan(add_group, jnp.zeros((total_rows, out_weight.shape[1]), jnp.float32), (grouped, weight_groups))
    return result.astype(jnp.bfloat16)

def swiglu_blocks(inputs, gate_w, up_w, down_w):
    model_width = gate_w.shape[0]
    block_width = gate_w.shape[1] // N_TP
    gate_blocks = gate_w.reshape(model_width, N_TP, block_width).transpose(1, 0, 2)
    up_blocks = up_w.reshape(model_width, N_TP, block_width).transpose(1, 0, 2)
    down_blocks = down_w.reshape(N_TP, block_width, down_w.shape[1])

    def add_block(running, block_parts):
        gate_part = jnp.dot(inputs, block_parts[0], preferred_element_type=jnp.float32)
        up_part = jnp.dot(inputs, block_parts[1], preferred_element_type=jnp.float32)
        hidden = (jax.nn.silu(gate_part) * up_part).astype(jnp.bfloat16)
        partial_out = jnp.dot(hidden, block_parts[2], preferred_element_type=jnp.float32)
        return (running + lax.optimization_barrier(partial_out.astype(jnp.bfloat16)).astype(jnp.float32), None)
    result, _ = lax.scan(add_block, jnp.zeros((inputs.shape[0], down_w.shape[1]), jnp.float32), (gate_blocks, up_blocks, down_blocks))
    return result

def mixture(moe_input, ffn_gain, routes, route_weight, gate_weight, up_weight, down_weight, shared_gate, shared_up, shared_down):
    row_values = moe_input.astype(jnp.float32)
    inverse_rms = lax.rsqrt(lax.optimization_barrier(jnp.mean(row_values * row_values, axis=-1, keepdims=True)) + norm_eps)
    normed = (row_values * inverse_rms * ffn_gain.astype(jnp.float32)).astype(jnp.bfloat16)
    total_rows = normed.shape[0]
    experts = gate_weight.shape[0]
    blocks = total_rows // TOK_B
    flat_routes = routes.reshape(blocks, TOK_B * TOP_K)
    onehot = (flat_routes[..., None] == jnp.arange(experts, dtype=jnp.int32)).astype(jnp.int32)
    slot_rank = lax.optimization_barrier(jnp.sum((jnp.cumsum(onehot, axis=1) - 1) * onehot, axis=-1)).astype(jnp.int32)
    token_ids = jnp.arange(blocks, dtype=jnp.int32)[:, None] * TOK_B + jnp.arange(TOK_B * TOP_K, dtype=jnp.int32)[None, :] // TOP_K
    source_ids = jnp.broadcast_to(jnp.arange(blocks, dtype=jnp.int32)[:, None], flat_routes.shape)
    slot_table = jnp.full((experts, blocks, CAP), total_rows, jnp.int32).at[flat_routes, source_ids, slot_rank].set(token_ids)
    padded = jnp.concatenate([normed, jnp.zeros((1, normed.shape[1]), jnp.bfloat16)], axis=0)

    def one_expert(inputs):
        chosen = padded[inputs[0].reshape(-1)]
        return swiglu_blocks(chosen, inputs[1], inputs[2], inputs[3]).astype(jnp.bfloat16)
    expert_out = lax.map(one_expert, (slot_table, gate_weight, up_weight, down_weight))
    expert_out = expert_out.reshape(experts, blocks, CAP, normed.shape[1])
    block_index = (jnp.arange(total_rows, dtype=jnp.int32) // TOK_B)[:, None]
    picked = expert_out[routes, block_index, slot_rank.reshape(total_rows, TOP_K)]
    shared_sum = swiglu_blocks(normed, shared_gate, shared_up, shared_down)
    combined = lax.optimization_barrier(jnp.sum(route_weight[..., None] * picked.astype(jnp.float32), axis=1)) + shared_sum
    return combined.astype(jnp.bfloat16)

def reference(query_pairs, key_pairs, value_rows, head_lambda, head_gain, out_weight, moe_input, ffn_gain, routes, route_weight, gate_weight, up_weight, down_weight, shared_gate, shared_up, shared_down):
    attn_out = attention(query_pairs, key_pairs, value_rows, head_lambda, head_gain, out_weight)
    moe_out = mixture(moe_input, ffn_gain, routes, route_weight, gate_weight, up_weight, down_weight, shared_gate, shared_up, shared_down)
    return (attn_out, moe_out)
```

```python
import functools

import jax
import jax.numpy as jnp
from jax import lax
from jax.experimental import pallas as pl
from jax.experimental.pallas import tpu as pltpu
from jax.sharding import PartitionSpec as P

TOP_K = 2

theta_base = 500000.0
norm_eps = 1e-06
masked_low = -1e30

CORES = 2
LANES = 128
MESH = pl.DeviceIdType.MESH
f32 = jnp.float32
bf16 = jnp.bfloat16


def rotation_tables(rows):
    shape = (rows, LANES)
    lane = lax.broadcasted_iota(jnp.int32, shape, 1)
    place = (lane % 32).astype(f32)
    frequency = theta_base ** (-(place * 2.0) / 64)
    positions = lax.axis_index("ep") * rows + lax.broadcasted_iota(jnp.int32, shape, 0)
    angles = positions.astype(f32) * frequency
    sign = jnp.where(lane % 64 < 32, -1.0, 1.0)
    return jnp.cos(angles), jnp.sin(angles) * sign


def rotated(x, cosine, sine):
    x = x.astype(f32)
    lane = lax.broadcasted_iota(jnp.int32, x.shape, 1)
    swapped = jnp.where(lane % 64 < 32, pltpu.roll(x, 96, 1), pltpu.roll(x, 32, 1))
    return x * cosine + swapped * sine


def split_tp(nx):
    tp = lax.axis_index("tp")
    return tp // nx, tp % nx


class Projection:
    def __init__(self, ny, nx, rows, w_hbm, wb, hx, pr, rr, sems):
        self.ny, self.nx, self.rows = ny, nx, rows
        self.w, self.wb, self.hx, self.pr, self.rr = w_hbm, wb, hx, pr, rr
        self.w_send, self.w_recv, self.w_local, self.h_send, self.h_recv, self.p_send, self.p_recv = sems
        self.y, self.x = split_tp(nx)
        self.ep = lax.axis_index("ep")

    def _device(self, y, x):
        return (self.ep, y * self.nx + x)

    def _weight(self, i):
        y = lax.rem(self.y + i, self.ny)
        width = self.nx * LANES
        cols = pl.ds(pl.multiple_of(y * width, width), width)
        rows = pl.ds(pl.multiple_of(self.y * LANES, LANES), LANES)
        return pltpu.make_async_remote_copy(
            src_ref=self.w.at[:, cols],
            dst_ref=self.wb.at[rows, :],
            send_sem=self.w_send.at[i],
            recv_sem=self.w_recv.at[i],
            device_id=self._device(y, self.x),
            device_id_type=MESH,
        )

    def _weight_own(self):
        width = self.nx * LANES
        cols = pl.ds(pl.multiple_of(self.y * width, width), width)
        rows = pl.ds(pl.multiple_of(self.y * LANES, LANES), LANES)
        return pltpu.make_async_copy(self.w.at[:, cols], self.wb.at[rows, :], self.w_local)

    def start_weights(self):
        self._weight_own().start()
        for i in range(1, self.ny):
            self._weight(i).start()

    def _gather(self, i):
        y = lax.rem(self.y + i, self.ny)
        cols = pl.ds(pl.multiple_of(self.y * LANES, LANES), LANES)
        return pltpu.make_async_remote_copy(
            src_ref=self.hx.at[:, cols],
            dst_ref=self.hx.at[:, cols],
            send_sem=self.h_send.at[i],
            recv_sem=self.h_recv.at[i],
            device_id=self._device(y, self.x),
            device_id_type=MESH,
        )

    def start_gather(self, h):
        cols = pl.ds(pl.multiple_of(self.y * LANES, LANES), LANES)
        self.hx[:, cols] = h
        for i in range(1, self.ny):
            self._gather(i).start()

    def _partial(self, i):
        x = lax.rem(self.x + i, self.nx)
        return pltpu.make_async_remote_copy(
            src_ref=self.pr.at[i],
            dst_ref=self.rr.at[i],
            send_sem=self.p_send.at[i],
            recv_sem=self.p_recv.at[i],
            device_id=self._device(self.y, x),
            device_id_type=MESH,
        )

    def multiply_and_send(self):
        self._weight_own().wait()
        for i in range(1, self.ny):
            self._weight(i).wait()
        for i in range(1, self.ny):
            self._gather(i).wait()
        h = self.hx[...]
        for i in list(range(1, self.nx)) + [0]:
            x = lax.rem(self.x + i, self.nx)
            w = self.wb[:, pl.ds(pl.multiple_of(x * LANES, LANES), LANES)]
            self.pr[i] = jnp.dot(h, w, preferred_element_type=f32).astype(bf16)
            if i:
                self._partial(i).start()

    def finish(self):
        for i in range(1, self.nx):
            self._partial(i).wait()
        total = self.pr[0].astype(f32)
        for i in range(1, self.nx):
            total = total + self.rr[i].astype(f32)
        return total


class Ring:
    def __init__(self, nz, kbuf, vbuf, recv, send, pass_send):
        self.nz = nz
        self.up_steps, self.down_steps = nz // 2, nz - 1 - nz // 2
        self.bufs = (kbuf, vbuf)
        self.recv, self.send, self.pass_send = recv, send, pass_send
        ep = lax.axis_index("ep")
        self.tp = lax.axis_index("tp")
        self.z, self.c = ep // CORES, ep % CORES

    def _device(self, z, c):
        return (z * CORES + c, self.tp)

    def neighbours(self):
        up = lax.rem(self.z + 1, self.nz)
        down = lax.rem(self.z + self.nz - 1, self.nz)
        return [self._device(up, self.c), self._device(down, self.c), self._device(self.z, 1 - self.c)]

    def copy(self, source, part, to_z, sem):
        slot = source * CORES + self.c
        ref = self.bufs[part].at[slot]
        return pltpu.make_async_remote_copy(
            src_ref=ref,
            dst_ref=ref,
            send_sem=self.send.at[sem, part],
            recv_sem=self.recv.at[slot, part],
            device_id=self._device(to_z, self.c),
            device_id_type=MESH,
        )

    def up(self, source, part):
        return self.copy(source, part, lax.rem(self.z + 1, self.nz), source)

    def down(self, source, part, sem=None):
        to = lax.rem(self.z + self.nz - 1, self.nz)
        return self.copy(source, part, to, source if sem is None else sem)

    def handed(self, source, part, core):
        slot = source * CORES + core
        ref = self.bufs[part].at[slot]
        return pltpu.make_async_remote_copy(
            src_ref=ref,
            dst_ref=ref,
            send_sem=self.pass_send.at[source, part],
            recv_sem=self.recv.at[slot, part],
            device_id=self._device(self.z, 1 - self.c),
            device_id_type=MESH,
        )

    def up_source(self, t):
        return self.z - t, self.z - t >= 0

    def down_source(self, t):
        source = lax.rem(self.z + t, self.nz)
        return source, jnp.logical_and(source < self.down_steps, t <= self.down_steps)

    def start_own(self):
        for part in range(2):

            @pl.when(self.z < self.nz - 1)
            def _():
                self.up(self.z, part).start()

            @pl.when(self.z < self.down_steps)
            def _():
                self.down(self.z, part, self.nz).start()

            @pl.when(self.c == 0)
            def _():
                self.handed(self.z, part, self.c).start()

    def serve(self, t, part):
        source, here = self.up_source(t)

        @pl.when(here)
        def _():
            self.up(source, part).wait_recv()

            @pl.when(jnp.logical_and(t < self.up_steps, self.z < self.nz - 1))
            def _():
                self.up(source, part).start()

            self.handed(source, part, self.c).start()

        source_d, here_d = self.down_source(t)

        @pl.when(here_d)
        def _():
            self.down(source_d, part).wait_recv()

            @pl.when(t < self.down_steps)
            def _():
                self.down(source_d, part).start()

            @pl.when(source_d < self.z)
            def _():
                self.handed(source_d, part, self.c).start()

    def wait_handed(self, source):
        for part in range(2):
            self.handed(source, part, 1 - self.c).wait_recv()

    def wait_sends(self):
        for part in range(2):

            @pl.when(self.z < self.nz - 1)
            def _():
                self.up(self.z, part).wait_send()

            @pl.when(self.z < self.down_steps)
            def _():
                self.down(self.z, part, self.nz).wait_send()

            @pl.when(self.c == 0)
            def _():
                self.handed(self.z, part, self.c).wait_send()

        @pl.loop(1, self.up_steps + 1)
        def _(t):
            source, here = self.up_source(t)
            source_d, here_d = self.down_source(t)

            @pl.when(here)
            def _():
                for part in range(2):
                    self.handed(source, part, self.c).wait_send()

                    @pl.when(jnp.logical_and(t < self.up_steps, self.z < self.nz - 1))
                    def _():
                        self.up(source, part).wait_send()

            @pl.when(here_d)
            def _():
                for part in range(2):

                    @pl.when(t < self.down_steps)
                    def _():
                        self.down(source_d, part).wait_send()

                    @pl.when(source_d < self.z)
                    def _():
                        self.handed(source_d, part, self.c).wait_send()


class Softmax:
    def __init__(self, rows, tile, qz, kbuf, vbuf, top, total, acc):
        self.rows, self.tile = rows, tile
        self.qz, self.kbuf, self.vbuf = qz, kbuf, vbuf
        self.top, self.total, self.acc = top, total, acc

    def _tiles(self):
        return [pl.ds(i * self.tile, self.tile) for i in range(2 * self.rows // self.tile)]

    def diagonal(self, slot):
        keys, values = self.kbuf[slot], self.vbuf[slot]
        for i, rows in enumerate(self._tiles()):
            s = lax.dot_general(self.qz[rows, :], keys, (((1,), (1,)), ((), ())), preferred_element_type=f32)
            row = i * self.tile + lax.broadcasted_iota(jnp.int32, s.shape, 0)
            row = jnp.where(row >= self.rows, row - self.rows, row)
            allowed = lax.broadcasted_iota(jnp.int32, s.shape, 1) <= row
            s = jnp.where(allowed, s, masked_low)
            top = jnp.max(s, axis=1, keepdims=True)
            p = jnp.where(allowed, jnp.exp(s - top), 0.0)
            self.top[rows, :] = jnp.broadcast_to(top, (self.tile, LANES))
            self.total[rows, :] = jnp.broadcast_to(jnp.sum(p, axis=1, keepdims=True), (self.tile, LANES))
            self.acc[rows, :] = jnp.dot(p.astype(bf16), values, preferred_element_type=f32)

    def _add(self, keys, values):
        for rows in self._tiles():
            s = lax.dot_general(self.qz[rows, :], keys, (((1,), (1,)), ((), ())), preferred_element_type=f32)
            before = self.top[rows, :]
            top = jnp.maximum(before, jnp.max(s, axis=1, keepdims=True))
            p = jnp.exp(s - top[:, :1])
            scale = jnp.exp(before - top)
            self.top[rows, :] = top
            self.total[rows, :] = self.total[rows, :] * scale + jnp.sum(p, axis=1, keepdims=True)
            self.acc[rows, :] = self.acc[rows, :] * scale + jnp.dot(
                p.astype(bf16), values, preferred_element_type=f32
            )

    def one(self, slot):
        self._add(self.kbuf[slot], self.vbuf[slot])

    def chip(self, source):
        pair = pl.ds(source * CORES, CORES)
        shape = (CORES * self.rows, LANES)
        self._add(self.kbuf[pair].reshape(shape), self.vbuf[pair].reshape(shape))

    def heads(self, lam, gain):
        out = self.acc[...] / self.total[...]
        diff = out[: self.rows] - lam * out[self.rows :]
        mean = jnp.mean(diff * diff, axis=1, keepdims=True)
        return (diff * lax.rsqrt(mean + norm_eps) * gain).astype(bf16)


def attention_kernel(
    dims,
    q_ref, k_ref, v_ref, cos_ref, sin_ref, lam_ref, gain_ref, w_hbm,
    out_ref,
    kbuf, vbuf, qz, top, total, acc, wb, hx, pr, rr,
    ring_recv, ring_send, pass_send, *proj_sems,
):
    nz, ny, nx, rows, tile = dims
    ep = lax.axis_index("ep")
    ring = Ring(nz, kbuf, vbuf, ring_recv, ring_send, pass_send)
    proj = Projection(ny, nx, rows, w_hbm, wb, hx, pr, rr, proj_sems)
    soft = Softmax(rows, tile, qz, kbuf, vbuf, top, total, acc)

    barrier = pltpu.get_barrier_semaphore()
    peers = ring.neighbours()
    peers += [proj._device(lax.rem(proj.y + i, ny), proj.x) for i in range(1, ny)]
    peers += [proj._device(proj.y, lax.rem(proj.x + i, nx)) for i in range(1, nx)]
    for peer in peers:
        pl.semaphore_signal(barrier, inc=1, device_id=peer, device_id_type=MESH)

    cosine, sine = cos_ref[...], sin_ref[...]
    kbuf[ep] = rotated(k_ref[...], cosine, sine).astype(bf16)
    vbuf[ep] = v_ref[...]
    pl.semaphore_wait(barrier, len(peers))
    ring.start_own()
    proj.start_weights()

    q = rotated(q_ref[...], cosine, sine).astype(bf16).astype(f32) * 0.125
    lane = lax.broadcasted_iota(jnp.int32, q.shape, 1)
    qz[:rows, :] = jnp.where(lane < 64, q, 0.0).astype(bf16)
    qz[rows:, :] = jnp.where(lane < 64, 0.0, q).astype(bf16)
    soft.diagonal(ep)

    @pl.when(ring.c == 1)
    def _():
        ring.wait_handed(ring.z)
        soft.one(ep - 1)

    def use(source):
        ring.wait_handed(source)
        soft.chip(source)

    def use_up(t):
        source, here = ring.up_source(t)

        @pl.when(jnp.logical_and(here, t >= 1))
        def _():
            use(source)

    def use_down(t):
        source, here = ring.down_source(t)

        @pl.when(jnp.logical_and(jnp.logical_and(here, t >= 1), source < ring.z))
        def _():
            use(source)

    @pl.loop(1, ring.up_steps + 1)
    def _(t):
        ring.serve(t, 0)
        use_up(t - 1)
        ring.serve(t, 1)
        use_down(t - 1)

    use_up(ring.up_steps)
    use_down(ring.up_steps)

    proj.start_gather(soft.heads(lam_ref[0], gain_ref[...]))
    proj.multiply_and_send()
    ring.wait_sends()
    out_ref[...] = proj.finish().astype(bf16)


def attention(nz, ny, nx, query_pairs, key_pairs, value_rows, head_lambda, head_gain, out_weight):
    rows = query_pairs.shape[0]
    tile = 256 if (2 * rows) % 256 == 0 else 2 * rows
    cosine, sine = rotation_tables(rows)
    vmem = pl.BlockSpec(memory_space=pltpu.VMEM)
    slots = nz * CORES
    dma = pltpu.SemaphoreType.DMA
    return pl.pallas_call(
        functools.partial(attention_kernel, (nz, ny, nx, rows, tile)),
        out_shape=jax.ShapeDtypeStruct((rows, LANES), bf16),
        in_specs=[vmem] * 5
        + [pl.BlockSpec(memory_space=pltpu.SMEM), vmem, pl.BlockSpec(memory_space=pl.ANY)],
        out_specs=vmem,
        scratch_shapes=[
            pltpu.VMEM((slots, rows, LANES), bf16),
            pltpu.VMEM((slots, rows, LANES), bf16),
            pltpu.VMEM((2 * rows, LANES), bf16),
            pltpu.VMEM((2 * rows, LANES), f32),
            pltpu.VMEM((2 * rows, LANES), f32),
            pltpu.VMEM((2 * rows, LANES), f32),
            pltpu.VMEM((ny * LANES, nx * LANES), bf16),
            pltpu.VMEM((rows, ny * LANES), bf16),
            pltpu.VMEM((nx, rows, LANES), bf16),
            pltpu.VMEM((nx, rows, LANES), bf16),
            dma((slots, 2)),
            dma((nz + 1, 2)),
            dma((nz, 2)),
            dma((ny,)),
            dma((ny,)),
            dma(()),
            dma((ny,)),
            dma((ny,)),
            dma((nx,)),
            dma((nx,)),
        ],
        compiler_params=pltpu.CompilerParams(
            collective_id=0, has_side_effects=True, vmem_limit_bytes=56 * 1024 * 1024
        ),
        name="attention",
    )(query_pairs, key_pairs, value_rows, cosine, sine, head_lambda, head_gain.reshape(1, -1), out_weight)


def in_blocks(x, dim, peers):
    shape = x.shape
    pieces = x.reshape(*shape[:dim], peers, shape[dim] // peers, *shape[dim + 1 :])
    return jnp.moveaxis(pieces, dim, 0)


def sum_at_owner(x, axis, dim):
    peers = lax.axis_size(axis)
    pieces = lax.all_to_all(in_blocks(x, dim, peers), axis, 0, 0, tiled=True)
    return jnp.sum(pieces.astype(jnp.float32), axis=0)


def joined_along(pieces, dim):
    shape = list(pieces.shape[1:])
    shape[dim] *= pieces.shape[0]
    return jnp.moveaxis(pieces, 0, dim).reshape(shape)


def copy_for_each(x, axis):
    copies = jnp.broadcast_to(x, (lax.axis_size(axis), *x.shape))
    return lax.all_to_all(copies, axis, split_axis=0, concat_axis=0, tiled=True)


def gather_directly(x, axis, dim):
    return joined_along(copy_for_each(x, axis), dim)


def sent_together(arrays, axis, dim, along):
    both = jnp.concatenate(arrays, axis=along)
    out, at, finished = (sum_at_owner(both, axis, dim), 0, [])
    for a in arrays:
        finished.append(lax.slice_in_dim(out, at, at + a.shape[along], axis=along))
        at += a.shape[along]
    return tuple(finished)


def local(
    sizes,
    query_pairs,
    key_pairs,
    value_rows,
    head_lambda,
    head_gain,
    out_weight,
    moe_input,
    ffn_gain,
    routes,
    route_weight,
    gate_weight,
    up_weight,
    down_weight,
    shared_gate,
    shared_up,
    shared_down,
):
    attn_out = attention(*sizes, query_pairs, key_pairs, value_rows, head_lambda, head_gain, out_weight)
    row_values = moe_input.astype(jnp.float32)
    inverse_norm = lax.rsqrt(jnp.mean(row_values * row_values, axis=-1, keepdims=True) + norm_eps)
    normed = (row_values * inverse_norm * ffn_gain).astype(jnp.bfloat16)
    token_rows = normed.shape[0]
    experts = lax.axis_size("ep")
    capacity = token_rows * TOP_K * 6 // (5 * experts)
    flat_routes = routes.reshape(-1)
    onehot = (flat_routes[:, None] == jnp.arange(experts, dtype=jnp.int32)).astype(jnp.int32)
    slot_rank = jnp.sum((jnp.cumsum(onehot, axis=0) - 1) * onehot, axis=-1)
    slot_index = flat_routes * capacity + slot_rank
    token_index = jnp.arange(token_rows * TOP_K, dtype=jnp.int32) // TOP_K
    slot_rows = (
        jnp.full((experts * capacity,), token_rows, jnp.int32).at[slot_index].set(token_index)
    )
    padded = jnp.concatenate([normed, jnp.zeros((1, normed.shape[1]), jnp.bfloat16)], axis=0)
    column_width = normed.shape[1] // lax.axis_size("tp")
    padded_cols = lax.dynamic_slice_in_dim(
        padded, lax.axis_index("tp") * column_width, column_width, 1
    )
    outgoing = padded_cols[slot_rows]
    arrived = lax.all_to_all(outgoing, "ep", split_axis=0, concat_axis=0, tiled=True)
    pieces = gather_directly(arrived, "tp", 1)
    gate_rows = gate_weight[0]
    up_rows = up_weight[0]
    gate_part = jnp.dot(pieces, gate_rows, preferred_element_type=jnp.float32)
    up_part = jnp.dot(pieces, up_rows, preferred_element_type=jnp.float32)
    hidden = (jax.nn.silu(gate_part) * up_part).astype(jnp.bfloat16)
    expert_terms = jnp.dot(hidden, down_weight[0], preferred_element_type=jnp.float32)
    shared_gated = jnp.dot(normed, shared_gate, preferred_element_type=jnp.float32)
    shared_lifted = jnp.dot(normed, shared_up, preferred_element_type=jnp.float32)
    shared_hidden = (jax.nn.silu(shared_gated) * shared_lifted).astype(jnp.bfloat16)
    shared_terms = jnp.dot(shared_hidden, shared_down, preferred_element_type=jnp.float32)
    expert_sum, shared_sum = sent_together(
        (expert_terms.astype(jnp.bfloat16), shared_terms.astype(jnp.bfloat16)), "tp", 1, 0
    )
    returned = lax.all_to_all(
        expert_sum.astype(jnp.bfloat16), "ep", split_axis=0, concat_axis=0, tiled=True
    )
    picked = returned[slot_index.reshape(token_rows, TOP_K)]
    moe_out = (
        jnp.sum(route_weight[..., None] * picked.astype(jnp.float32), axis=1) + shared_sum
    ).astype(jnp.bfloat16)
    return (attn_out, moe_out)


def grid_of(mesh):
    side = int(round(mesh.shape["tp"] ** 0.5))
    return mesh.shape["ep"] // CORES, mesh.shape["tp"] // side, side


def solution(mesh):
    return jax.shard_map(
        functools.partial(local, grid_of(mesh)),
        mesh=mesh,
        in_specs=(
            P("ep", "tp"),
            P("ep", "tp"),
            P("ep", "tp"),
            P("tp"),
            P(),
            P("tp", None),
            P("ep", None),
            P(),
            P("ep", None),
            P("ep", None),
            P("ep", None, "tp"),
            P("ep", None, "tp"),
            P("ep", "tp", None),
            P(None, "tp"),
            P(None, "tp"),
            P("tp", None),
        ),
        out_specs=(P("ep", "tp"), P("ep", "tp")),
        check_vma=False,
    )
```

```python
import functools

import jax
import jax.numpy as jnp
from jax import lax
from jax.experimental import pallas as pl
from jax.experimental.pallas import tpu as pltpu
from jax.sharding import PartitionSpec as P

TOP_K = 2

theta_base = 500000.0
norm_eps = 1e-06
masked_low = -1e30

CORES = 2
LANES = 128
PAD = 16
MESH = pl.DeviceIdType.MESH
f32 = jnp.float32
bf16 = jnp.bfloat16

AXES = ("y", "x", "x")
SPREAD_AT, SHARED_AT, EXPERT_AT = 2, 3, 6


def rotation_tables(rows):
    shape = (rows, LANES)
    lane = lax.broadcasted_iota(jnp.int32, shape, 1)
    place = (lane % 32).astype(f32)
    frequency = theta_base ** (-(place * 2.0) / 64)
    positions = lax.axis_index("ep") * rows + lax.broadcasted_iota(jnp.int32, shape, 0)
    angles = positions.astype(f32) * frequency
    sign = jnp.where(lane % 64 < 32, -1.0, 1.0)
    return jnp.cos(angles), jnp.sin(angles) * sign


def rotated(x, cosine, sine):
    x = x.astype(f32)
    lane = lax.broadcasted_iota(jnp.int32, x.shape, 1)
    swapped = jnp.where(lane % 64 < 32, pltpu.roll(x, 96, 1), pltpu.roll(x, 32, 1))
    return x * cosine + swapped * sine


def block(i, width=LANES):
    return pl.ds(pl.multiple_of(i * width, width), width)


def split_tp(nx):
    tp = lax.axis_index("tp")
    return tp // nx, tp % nx


class Projection:
    def __init__(self, grid, axis, w_hbm, wb, hx, pr, rr, sems):
        self.ny, self.nx = grid
        self.axis = axis
        self.w, self.wb, self.hx, self.pr, self.rr = w_hbm, wb, hx, pr, rr
        self.w_send, self.w_recv, self.w_local, self.h_send, self.h_recv, self.p_send, self.p_recv = sems
        y, x = split_tp(self.nx)
        self.g, self.o, self.ng, self.no = (y, x, self.ny, self.nx) if axis == "y" else (x, y, self.nx, self.ny)
        self.ep = lax.axis_index("ep")

    @staticmethod
    def scratch(grid, axis, rows):
        ng, no = grid if axis == "y" else grid[::-1]
        dma = pltpu.SemaphoreType.DMA
        return [
            pltpu.VMEM((ng * LANES, no * LANES), bf16),
            pltpu.VMEM((rows, ng * LANES), bf16),
            pltpu.VMEM((no, rows, LANES), bf16),
            pltpu.VMEM((no, rows, LANES), bf16),
            dma((ng, no)),
            dma((ng, no)),
            dma((no,)),
            dma((ng,)),
            dma((ng,)),
            dma((no,)),
            dma((no,)),
        ]

    def _tp(self, g, o):
        return g * self.nx + o if self.axis == "y" else o * self.nx + g

    def _weights(self, g):
        rows = block(self.g)
        if self.axis == "y":
            width = self.no * LANES
            yield 0, self.w.at[:, block(g, width)], self.wb.at[rows, :]
            return
        for o in range(self.no):
            yield o, self.w.at[:, block(self._tp(g, o))], self.wb.at[rows, pl.ds(o * LANES, LANES)]

    def _weights_out(self):
        for i in range(1, self.ng):
            g = lax.rem(self.g + i, self.ng)
            for k, source, target in self._weights(g):
                yield pltpu.make_async_remote_copy(
                    src_ref=source,
                    dst_ref=target,
                    send_sem=self.w_send.at[i, k],
                    recv_sem=self.w_recv.at[i, k],
                    device_id=(self.ep, self._tp(g, self.o)),
                    device_id_type=MESH,
                )

    def _weights_own(self):
        for k, source, target in self._weights(self.g):
            yield pltpu.make_async_copy(source, target, self.w_local.at[k])

    def start_own_weights(self):
        for copy in self._weights_own():
            copy.start()

    def start_weights(self):
        for copy in self._weights_out():
            copy.start()

    def _gather(self, i):
        own = self.hx.at[:, block(self.g)]
        return pltpu.make_async_remote_copy(
            src_ref=own,
            dst_ref=own,
            send_sem=self.h_send.at[i],
            recv_sem=self.h_recv.at[i],
            device_id=(self.ep, self._tp(lax.rem(self.g + i, self.ng), self.o)),
            device_id_type=MESH,
        )

    def start_gather(self, h):
        self.hx[:, block(self.g)] = h
        for i in range(1, self.ng):
            self._gather(i).start()

    def _partial(self, i):
        return pltpu.make_async_remote_copy(
            src_ref=self.pr.at[i],
            dst_ref=self.rr.at[i],
            send_sem=self.p_send.at[i],
            recv_sem=self.p_recv.at[i],
            device_id=(self.ep, self._tp(self.g, lax.rem(self.o + i, self.no))),
            device_id_type=MESH,
        )

    def wait_weights(self):
        for copy in self._weights_own():
            copy.wait()
        for copy in self._weights_out():
            copy.wait()

    def multiply_and_send(self):
        for i in range(1, self.ng):
            self._gather(i).wait()
        h = self.hx[...]
        for i in list(range(1, self.no)) + [0]:
            w = self.wb[:, block(lax.rem(self.o + i, self.no))]
            self.pr[i] = jnp.dot(h, w, preferred_element_type=f32).astype(bf16)
            if i:
                self._partial(i).start()

    def finish(self):
        for i in range(1, self.no):
            self._partial(i).wait()
        total = self.pr[0].astype(f32)
        for i in range(1, self.no):
            total = total + self.rr[i].astype(f32)
        return total


class Exchange:
    def __init__(self, axis, size, send_at, recv_at, send, recv):
        self.axis, self.size = axis, size
        self.send_at, self.recv_at, self.send, self.recv = send_at, recv_at, send, recv
        self.me = lax.axis_index(axis)

    def _copy(self, i):
        to = lax.rem(self.me + i, self.size)
        return pltpu.make_async_remote_copy(
            src_ref=self.send_at(to),
            dst_ref=self.recv_at(self.me),
            send_sem=self.send.at[i],
            recv_sem=self.recv.at[i],
            device_id={self.axis: to},
            device_id_type=MESH,
        )

    def start(self):
        @pl.loop(1, self.size)
        def _(i):
            self._copy(i).start()

    def wait(self):
        @pl.loop(1, self.size)
        def _(i):
            self._copy(i).wait()


class Routing:
    def __init__(self, tokens, experts, cap):
        self.tokens, self.experts, self.cap = tokens, experts, cap

    @staticmethod
    def _iota(shape, dim):
        return lax.broadcasted_iota(jnp.int32, shape, dim)

    @staticmethod
    def _ones(cond):
        return jnp.where(cond, 1.0, 0.0).astype(bf16)

    def to_slots(self, routes_t):
        n, e = self.tokens, self.experts
        expert = self._iota((e, n), 0)
        member = self._ones(jnp.logical_or(expert == routes_t[0:1, :], expert == routes_t[1:2, :]))
        earlier = self._ones(self._iota((n, n), 0) < self._iota((n, n), 1))
        place = jnp.dot(member, earlier, preferred_element_type=f32).astype(bf16)
        spread = self._ones(self._iota((e * PAD, e), 0) // PAD == self._iota((e * PAD, e), 1))
        member = jnp.dot(spread, member, preferred_element_type=f32)
        place = jnp.dot(spread, place, preferred_element_type=f32)
        here = (self._iota((e * PAD, n), 0) % PAD).astype(f32)
        return self._ones(jnp.logical_and(member > 0.5, place == here))

    def from_slots(self, routes):
        n, e = self.tokens, self.experts
        expert = self._iota((n, e), 1)
        members = [self._ones(expert == routes[:, k : k + 1]) for k in range(TOP_K)]
        earlier = self._ones(self._iota((n, n), 1) < self._iota((n, n), 0))
        place = jnp.dot(earlier, members[0] + members[1], preferred_element_type=f32).astype(bf16)
        spread = self._ones(self._iota((e, e * PAD), 1) // PAD == self._iota((e, e * PAD), 0))
        place = jnp.dot(place, spread, preferred_element_type=f32)
        here = (self._iota((n, e * PAD), 1) % PAD).astype(f32)
        out = []
        for member in members:
            member = jnp.dot(member, spread, preferred_element_type=f32)
            out.append(self._ones(jnp.logical_and(member > 0.5, place == here)))
        return out

    def packing(self, transposed):
        small, large = self.experts * self.cap, self.experts * PAD
        shape, dims = ((large, small), (1, 0)) if transposed else ((small, large), (0, 1))
        row, col = self._iota(shape, dims[0]), self._iota(shape, dims[1])
        return self._ones(jnp.logical_and(row == col // PAD * self.cap + col % PAD, col % PAD < self.cap))


def swiglu(x, weights):
    both = jnp.dot(x, weights, preferred_element_type=f32)
    gate, up = both[:, :LANES], both[:, LANES:]
    return (gate / (1.0 + jnp.exp(-gate)) * up).astype(bf16)


class Ring:
    def __init__(self, nz, kbuf, vbuf, recv, send, pass_send):
        self.nz = nz
        self.up_steps, self.down_steps = nz // 2, nz - 1 - nz // 2
        self.bufs = (kbuf, vbuf)
        self.recv, self.send, self.pass_send = recv, send, pass_send
        ep = lax.axis_index("ep")
        self.tp = lax.axis_index("tp")
        self.z, self.c = ep // CORES, ep % CORES

    def _device(self, z, c):
        return (z * CORES + c, self.tp)

    def neighbours(self):
        up = lax.rem(self.z + 1, self.nz)
        down = lax.rem(self.z + self.nz - 1, self.nz)
        return [self._device(up, self.c), self._device(down, self.c), self._device(self.z, 1 - self.c)]

    def copy(self, source, part, to_z, sem):
        slot = source * CORES + self.c
        ref = self.bufs[part].at[slot]
        return pltpu.make_async_remote_copy(
            src_ref=ref,
            dst_ref=ref,
            send_sem=self.send.at[sem, part],
            recv_sem=self.recv.at[slot, part],
            device_id=self._device(to_z, self.c),
            device_id_type=MESH,
        )

    def up(self, source, part):
        return self.copy(source, part, lax.rem(self.z + 1, self.nz), source)

    def down(self, source, part, sem=None):
        to = lax.rem(self.z + self.nz - 1, self.nz)
        return self.copy(source, part, to, source if sem is None else sem)

    def handed(self, source, part, core):
        slot = source * CORES + core
        ref = self.bufs[part].at[slot]
        return pltpu.make_async_remote_copy(
            src_ref=ref,
            dst_ref=ref,
            send_sem=self.pass_send.at[source, part],
            recv_sem=self.recv.at[slot, part],
            device_id=self._device(self.z, 1 - self.c),
            device_id_type=MESH,
        )

    def up_source(self, t):
        return self.z - t, self.z - t >= 0

    def down_source(self, t):
        source = lax.rem(self.z + t, self.nz)
        return source, jnp.logical_and(source < self.down_steps, t <= self.down_steps)

    def start_own(self):
        for part in range(2):

            @pl.when(self.z < self.nz - 1)
            def _():
                self.up(self.z, part).start()

            @pl.when(self.z < self.down_steps)
            def _():
                self.down(self.z, part, self.nz).start()

            @pl.when(self.c == 0)
            def _():
                self.handed(self.z, part, self.c).start()

    def serve(self, t, part):
        source, here = self.up_source(t)

        @pl.when(here)
        def _():
            self.up(source, part).wait_recv()

            @pl.when(jnp.logical_and(t < self.up_steps, self.z < self.nz - 1))
            def _():
                self.up(source, part).start()

            self.handed(source, part, self.c).start()

        source_d, here_d = self.down_source(t)

        @pl.when(here_d)
        def _():
            self.down(source_d, part).wait_recv()

            @pl.when(t < self.down_steps)
            def _():
                self.down(source_d, part).start()

            @pl.when(source_d < self.z)
            def _():
                self.handed(source_d, part, self.c).start()

    def wait_handed(self, source):
        for part in range(2):
            self.handed(source, part, 1 - self.c).wait_recv()

    def wait_sends(self):
        for part in range(2):

            @pl.when(self.z < self.nz - 1)
            def _():
                self.up(self.z, part).wait_send()

            @pl.when(self.z < self.down_steps)
            def _():
                self.down(self.z, part, self.nz).wait_send()

            @pl.when(self.c == 0)
            def _():
                self.handed(self.z, part, self.c).wait_send()

        @pl.loop(1, self.up_steps + 1)
        def _(t):
            source, here = self.up_source(t)
            source_d, here_d = self.down_source(t)

            @pl.when(here)
            def _():
                for part in range(2):
                    self.handed(source, part, self.c).wait_send()

                    @pl.when(jnp.logical_and(t < self.up_steps, self.z < self.nz - 1))
                    def _():
                        self.up(source, part).wait_send()

            @pl.when(here_d)
            def _():
                for part in range(2):

                    @pl.when(t < self.down_steps)
                    def _():
                        self.down(source_d, part).wait_send()

                    @pl.when(source_d < self.z)
                    def _():
                        self.handed(source_d, part, self.c).wait_send()


class Softmax:
    def __init__(self, rows, tile, qz, kbuf, vbuf, top, total, acc):
        self.rows, self.tile = rows, tile
        self.qz, self.kbuf, self.vbuf = qz, kbuf, vbuf
        self.top, self.total, self.acc = top, total, acc

    def _tiles(self):
        return [pl.ds(i * self.tile, self.tile) for i in range(2 * self.rows // self.tile)]

    def diagonal(self, slot):
        keys, values = self.kbuf[slot], self.vbuf[slot]
        for i, rows in enumerate(self._tiles()):
            s = lax.dot_general(self.qz[rows, :], keys, (((1,), (1,)), ((), ())), preferred_element_type=f32)
            row = i * self.tile + lax.broadcasted_iota(jnp.int32, s.shape, 0)
            row = jnp.where(row >= self.rows, row - self.rows, row)
            allowed = lax.broadcasted_iota(jnp.int32, s.shape, 1) <= row
            s = jnp.where(allowed, s, masked_low)
            top = jnp.max(s, axis=1, keepdims=True)
            p = jnp.where(allowed, jnp.exp(s - top), 0.0)
            self.top[rows, :] = jnp.broadcast_to(top, (self.tile, LANES))
            self.total[rows, :] = jnp.broadcast_to(jnp.sum(p, axis=1, keepdims=True), (self.tile, LANES))
            self.acc[rows, :] = jnp.dot(p.astype(bf16), values, preferred_element_type=f32)

    def _add(self, keys, values):
        for rows in self._tiles():
            s = lax.dot_general(self.qz[rows, :], keys, (((1,), (1,)), ((), ())), preferred_element_type=f32)
            before = self.top[rows, :]
            top = jnp.maximum(before, jnp.max(s, axis=1, keepdims=True))
            p = jnp.exp(s - top[:, :1])
            scale = jnp.exp(before - top)
            self.top[rows, :] = top
            self.total[rows, :] = self.total[rows, :] * scale + jnp.sum(p, axis=1, keepdims=True)
            self.acc[rows, :] = self.acc[rows, :] * scale + jnp.dot(
                p.astype(bf16), values, preferred_element_type=f32
            )

    def one(self, slot):
        self._add(self.kbuf[slot], self.vbuf[slot])

    def chip(self, source):
        pair = pl.ds(source * CORES, CORES)
        shape = (CORES * self.rows, LANES)
        self._add(self.kbuf[pair].reshape(shape), self.vbuf[pair].reshape(shape))

    def heads(self, lam, gain):
        out = self.acc[...] / self.total[...]
        diff = out[: self.rows] - lam * out[self.rows :]
        mean = jnp.mean(diff * diff, axis=1, keepdims=True)
        return (diff * lax.rsqrt(mean + norm_eps) * gain).astype(bf16)


def kernel(dims, *refs):
    nz, ny, nx, rows, tile, tokens, experts, cap = dims
    refs = list(refs)

    def take(n):
        out = refs[:n]
        del refs[:n]
        return out

    q_ref, k_ref, v_ref, cos_ref, sin_ref, lam_ref, gain_ref, wo_hbm = take(8)
    x_ref, fgain_ref, routes_ref, routes_t_ref, rweight_ref = take(5)
    wg_hbm, wu_hbm, wd_hbm, sg_hbm, su_hbm, sd_hbm = take(6)
    attn_ref, moe_ref = take(2)
    kbuf, vbuf, qz, top, total, acc, ring_recv, ring_send, pass_send = take(9)
    xn, wgu, sgu, w_sem = take(4)
    out_slots, in_slots, xg, back_out, back_in = take(5)
    a_send, a_recv, g_send, g_recv, b_send, b_recv = take(6)
    grid = (ny, nx)
    ep, tp = lax.axis_index("ep"), lax.axis_index("tp")
    eps, tps = nz * CORES, ny * nx

    ring = Ring(nz, kbuf, vbuf, ring_recv, ring_send, pass_send)
    soft = Softmax(rows, tile, qz, kbuf, vbuf, top, total, acc)
    projections = []
    for axis, weight in zip(AXES, (wo_hbm, wd_hbm, sd_hbm)):
        wb, hx, pr, rr = take(4)
        projections.append(Projection(grid, axis, weight, wb, hx, pr, rr, take(7)))
    out_proj, down, shared_down = projections
    routing = Routing(tokens, experts, cap)

    barrier = pltpu.get_barrier_semaphore()
    for axis, me, size in (("ep", ep, eps), ("tp", tp, tps)):

        @pl.loop(1, size)
        def _(i):
            to = lax.rem(me + i, size)
            pl.semaphore_signal(barrier, inc=1, device_id={axis: to}, device_id_type=MESH)

    loads = [
        pltpu.make_async_copy(source, buf.at[:, pl.ds(k * LANES, LANES)], w_sem.at[i])
        for i, (source, buf, k) in enumerate(
            ((sg_hbm, sgu, 0), (su_hbm, sgu, 1), (wg_hbm, wgu, 0), (wu_hbm, wgu, 1))
        )
    ]
    for load in loads:
        load.start()
    for projection in projections:
        projection.start_own_weights()

    cosine, sine = cos_ref[...], sin_ref[...]
    kbuf[ep] = rotated(k_ref[...], cosine, sine).astype(bf16)
    vbuf[ep] = v_ref[...]
    x = x_ref[...].astype(f32)
    inverse = lax.rsqrt(jnp.mean(x * x, axis=1, keepdims=True) + norm_eps)
    xn[...] = (x * inverse * fgain_ref[...]).astype(bf16)
    to_slots = routing.to_slots(routes_t_ref[...])
    sent = jnp.dot(to_slots, xn[:, block(tp)], preferred_element_type=f32).astype(bf16)
    sent = sent.reshape(experts, PAD, LANES)
    out_slots[...] = sent
    in_slots[ep] = out_slots[ep]

    pl.semaphore_wait(barrier, eps + tps - 2)
    ring.start_own()
    there = Exchange("ep", eps, lambda i: out_slots.at[i], lambda i: in_slots.at[i], a_send, a_recv)
    spread = Exchange("tp", tps, lambda i: xg.at[:, block(tp)], lambda i: xg.at[:, block(i)], g_send, g_recv)
    back = Exchange("ep", eps, lambda i: back_out.at[i], lambda i: back_in.at[i], b_send, b_recv)
    there.start()
    shared_down.start_weights()
    down.start_weights()
    out_proj.start_weights()

    q = rotated(q_ref[...], cosine, sine).astype(bf16).astype(f32) * 0.125
    lane = lax.broadcasted_iota(jnp.int32, q.shape, 1)
    qz[:rows, :] = jnp.where(lane < 64, q, 0.0).astype(bf16)
    qz[rows:, :] = jnp.where(lane < 64, 0.0, q).astype(bf16)
    loads[0].wait()
    loads[1].wait()
    shared_down.start_gather(swiglu(xn[...], sgu[...]))
    soft.diagonal(ep)

    @pl.when(ring.c == 1)
    def _():
        ring.wait_handed(ring.z)
        soft.one(ep - 1)

    def use(source):
        ring.wait_handed(source)
        soft.chip(source)

    def use_up(t):
        source, here = ring.up_source(t)

        @pl.when(jnp.logical_and(here, t >= 1))
        def _():
            use(source)

    def use_down(t):
        source, here = ring.down_source(t)

        @pl.when(jnp.logical_and(jnp.logical_and(here, t >= 1), source < ring.z))
        def _():
            use(source)

    @pl.loop(1, ring.up_steps + 1)
    def _(t):
        ring.serve(t, 0)
        use_up(t - 1)
        ring.serve(t, 1)
        use_down(t - 1)

        @pl.when(t == SPREAD_AT)
        def _():
            there.wait()
            arrived = in_slots[...].reshape(experts * PAD, LANES)
            arrived = jnp.dot(routing.packing(False), arrived, preferred_element_type=f32)
            xg[:, block(tp)] = arrived.astype(bf16)
            spread.start()

        @pl.when(t == SHARED_AT)
        def _():
            shared_down.wait_weights()
            shared_down.multiply_and_send()

        @pl.when(t == EXPERT_AT)
        def _():
            loads[2].wait()
            loads[3].wait()
            spread.wait()
            down.start_gather(swiglu(xg[...], wgu[...]))

    use_up(ring.up_steps)
    use_down(ring.up_steps)

    out_proj.start_gather(soft.heads(lam_ref[0], gain_ref[...]))
    down.wait_weights()
    down.multiply_and_send()
    out_proj.wait_weights()
    out_proj.multiply_and_send()
    y = down.finish().astype(bf16)
    y = jnp.dot(routing.packing(True), y, preferred_element_type=f32).astype(bf16)
    back_out[...] = y.reshape(experts, PAD, LANES)
    back_in[ep] = back_out[ep]
    back.start()
    attn_ref[...] = out_proj.finish().astype(bf16)
    mixed = shared_down.finish()
    chosen = routing.from_slots(routes_ref[...])
    ring.wait_sends()
    back.wait()
    returned = back_in[...].reshape(experts * PAD, LANES)
    picked = [jnp.dot(c, returned, preferred_element_type=f32) for c in chosen]
    weight = rweight_ref[...]
    mixed = weight[:, 0:1] * picked[0] + weight[:, 1:2] * picked[1] + mixed
    moe_ref[...] = mixed.astype(bf16)


def local(
    sizes,
    query_pairs,
    key_pairs,
    value_rows,
    head_lambda,
    head_gain,
    out_weight,
    moe_input,
    ffn_gain,
    routes,
    route_weight,
    gate_weight,
    up_weight,
    down_weight,
    shared_gate,
    shared_up,
    shared_down,
):
    nz, ny, nx = sizes
    grid = (ny, nx)
    rows, tokens, width = query_pairs.shape[0], moe_input.shape[0], moe_input.shape[1]
    slots, experts = nz * CORES, nz * CORES
    cap = 12
    tile = 256 if (2 * rows) % 256 == 0 else 2 * rows
    cosine, sine = rotation_tables(rows)
    vmem, hbm = pl.BlockSpec(memory_space=pltpu.VMEM), pl.BlockSpec(memory_space=pl.ANY)
    dma = pltpu.SemaphoreType.DMA
    scratch = [
        pltpu.VMEM((slots, rows, LANES), bf16),
        pltpu.VMEM((slots, rows, LANES), bf16),
        pltpu.VMEM((2 * rows, LANES), bf16),
        pltpu.VMEM((2 * rows, LANES), f32),
        pltpu.VMEM((2 * rows, LANES), f32),
        pltpu.VMEM((2 * rows, LANES), f32),
        dma((slots, 2)),
        dma((nz + 1, 2)),
        dma((nz, 2)),
        pltpu.VMEM((tokens, width), bf16),
        pltpu.VMEM((width, 2 * LANES), bf16),
        pltpu.VMEM((width, 2 * LANES), bf16),
        dma((4,)),
        pltpu.VMEM((experts, PAD, LANES), bf16),
        pltpu.VMEM((experts, PAD, LANES), bf16),
        pltpu.VMEM((experts * cap, width), bf16),
        pltpu.VMEM((experts, PAD, LANES), bf16),
        pltpu.VMEM((experts, PAD, LANES), bf16),
        dma((slots,)),
        dma((slots,)),
        dma((ny * nx,)),
        dma((ny * nx,)),
        dma((slots,)),
        dma((slots,)),
    ]
    for axis, height in zip(AXES, (rows, experts * cap, tokens)):
        scratch += Projection.scratch(grid, axis, height)
    return tuple(
        pl.pallas_call(
            functools.partial(kernel, (nz, ny, nx, rows, tile, tokens, experts, cap)),
            out_shape=[
                jax.ShapeDtypeStruct((rows, LANES), bf16),
                jax.ShapeDtypeStruct((tokens, LANES), bf16),
            ],
            in_specs=[vmem] * 5
            + [pl.BlockSpec(memory_space=pltpu.SMEM), vmem, hbm]
            + [vmem] * 5
            + [hbm] * 6,
            out_specs=[vmem, vmem],
            scratch_shapes=scratch,
            compiler_params=pltpu.CompilerParams(
                collective_id=0, has_side_effects=True, vmem_limit_bytes=56 * 1024 * 1024
            ),
            name="layer",
        )(
            query_pairs,
            key_pairs,
            value_rows,
            cosine,
            sine,
            head_lambda,
            head_gain.reshape(1, -1),
            out_weight,
            moe_input,
            ffn_gain.reshape(1, -1),
            routes,
            routes.T,
            route_weight,
            gate_weight[0],
            up_weight[0],
            down_weight[0],
            shared_gate,
            shared_up,
            shared_down,
        )
    )


def grid_of(mesh):
    side = int(round(mesh.shape["tp"] ** 0.5))
    return mesh.shape["ep"] // CORES, mesh.shape["tp"] // side, side


def solution(mesh):
    return jax.shard_map(
        functools.partial(local, grid_of(mesh)),
        mesh=mesh,
        in_specs=(
            P("ep", "tp"),
            P("ep", "tp"),
            P("ep", "tp"),
            P("tp"),
            P(),
            P("tp", None),
            P("ep", None),
            P(),
            P("ep", None),
            P("ep", None),
            P("ep", None, "tp"),
            P("ep", None, "tp"),
            P("ep", "tp", None),
            P(None, "tp"),
            P(None, "tp"),
            P("tp", None),
        ),
        out_specs=(P("ep", "tp"), P("ep", "tp")),
        check_vma=False,
    )
```

```python
import functools

import jax
import jax.numpy as jnp
from jax import lax
from jax.experimental import pallas as pl
from jax.experimental.pallas import tpu as pltpu
from jax.sharding import PartitionSpec as P

TOP_K = 2

theta_base = 500000.0
norm_eps = 1e-06
masked_low = -1e30

CORES = 2
LANES = 128
PAD = 16
MESH = pl.DeviceIdType.MESH
f32 = jnp.float32
bf16 = jnp.bfloat16

AXES = ("x", "x", "y")
SPREAD_AT, RELAY_AT, SHARED_AT, EXPERT_AT, DOWN_AT, BACK_AT = 1, 2, 3, 5, 6, 8


def frequencies():
    place = (jnp.arange(LANES, dtype=jnp.int32) % 32).astype(f32)
    return (theta_base ** (-(place * 2.0) / 64)).reshape(1, LANES)


def angle_tables(ep, rows, frequency):
    quarter = rows // 4
    shape = (quarter, LANES)
    lane = lax.broadcasted_iota(jnp.int32, shape, 1)
    group = lane // 32
    positions = ep * rows + group * quarter + lax.broadcasted_iota(jnp.int32, shape, 0)
    angles = positions.astype(f32) * frequency
    sign = jnp.where(lane % 64 < 32, -1.0, 1.0)

    def spread(table, g):
        x = jnp.where(group == g, table, 0.0)
        x = x + pltpu.roll(x, 32, 1)
        return x + pltpu.roll(x, 64, 1)

    cosine, sine = jnp.cos(angles), jnp.sin(angles)
    return (
        jnp.concatenate([spread(cosine, g) for g in range(4)], axis=0),
        jnp.concatenate([spread(sine, g) * sign for g in range(4)], axis=0),
    )


def rotated(x, cosine, sine):
    x = x.astype(f32)
    lane = lax.broadcasted_iota(jnp.int32, x.shape, 1)
    swapped = jnp.where(lane % 64 < 32, pltpu.roll(x, 96, 1), pltpu.roll(x, 32, 1))
    return x * cosine + swapped * sine


def block(i, width=LANES):
    return pl.ds(pl.multiple_of(i * width, width), width)


def split_tp(nx):
    tp = lax.axis_index("tp")
    return tp // nx, tp % nx


def arrived(ref, sem):
    pltpu.make_async_copy(ref, ref, sem).wait()


class Projection:
    def __init__(self, grid, axis, w_hbm, wb, hx, pr, rr, sems):
        self.ny, self.nx = grid
        self.axis = axis
        self.w, self.wb, self.hx, self.pr, self.rr = w_hbm, wb, hx, pr, rr
        names = ("w_send", "w_recv", "w_local", "h_send", "h_recv", "p_send", "p_recv")
        for i, name in enumerate(names):
            setattr(self, name, sems.at[i])
        y, x = split_tp(self.nx)
        self.g, self.o, self.ng, self.no = (y, x, self.ny, self.nx) if axis == "y" else (x, y, self.nx, self.ny)
        self.ep = lax.axis_index("ep")

    @staticmethod
    def scratch(grid, axis, rows):
        ng, no = grid if axis == "y" else grid[::-1]
        dma = pltpu.SemaphoreType.DMA
        return [
            pltpu.VMEM((ng * LANES, no * LANES), bf16),
            pltpu.VMEM((rows, ng * LANES), bf16),
            pltpu.VMEM((no, rows, LANES), bf16),
            pltpu.VMEM((no, rows, LANES), bf16),
            dma((7,)),
        ]

    def _tp(self, g, o):
        return g * self.nx + o if self.axis == "y" else o * self.nx + g

    def _weights(self, g):
        rows = block(self.g)
        if self.axis == "y":
            width = self.no * LANES
            yield self.w.at[:, block(g, width)], self.wb.at[rows, :]
            return
        for o in range(self.no):
            yield self.w.at[:, block(self._tp(g, o))], self.wb.at[rows, pl.ds(o * LANES, LANES)]

    def start_own_weights(self):
        for source, target in self._weights(self.g):
            pltpu.make_async_copy(source, target, self.w_local).start()

    def start_weights(self):
        for i in range(1, self.ng):
            g = lax.rem(self.g + i, self.ng)
            for source, target in self._weights(g):
                pltpu.make_async_remote_copy(
                    src_ref=source,
                    dst_ref=target,
                    send_sem=self.w_send,
                    recv_sem=self.w_recv,
                    device_id=(self.ep, self._tp(g, self.o)),
                    device_id_type=MESH,
                ).start()

    def wait_weights(self):
        one, others = self.wb.at[pl.ds(0, LANES), :], self.wb.at[pl.ds(0, (self.ng - 1) * LANES), :]
        arrived(one, self.w_local)
        arrived(others, self.w_recv)
        arrived(others, self.w_send)

    def _gather(self, i):
        own = self.hx.at[:, block(self.g)]
        return pltpu.make_async_remote_copy(
            src_ref=own,
            dst_ref=own,
            send_sem=self.h_send,
            recv_sem=self.h_recv,
            device_id=(self.ep, self._tp(lax.rem(self.g + i, self.ng), self.o)),
            device_id_type=MESH,
        )

    def start_gather(self, h):
        self.hx[:, block(self.g)] = h
        for i in range(1, self.ng):
            self._gather(i).start()

    def _partial(self, i):
        return pltpu.make_async_remote_copy(
            src_ref=self.pr.at[i],
            dst_ref=self.rr.at[i],
            send_sem=self.p_send,
            recv_sem=self.p_recv,
            device_id=(self.ep, self._tp(self.g, lax.rem(self.o + i, self.no))),
            device_id_type=MESH,
        )

    def multiply_and_send(self):
        others = self.hx.at[:, pl.ds(0, (self.ng - 1) * LANES)]
        arrived(others, self.h_recv)
        arrived(others, self.h_send)
        h = self.hx[...]
        for i in list(range(1, self.no)) + [0]:
            w = self.wb[:, block(lax.rem(self.o + i, self.no))]
            self.pr[i] = jnp.dot(h, w, preferred_element_type=f32).astype(bf16)
            if i:
                self._partial(i).start()

    def finish(self):
        others = self.rr.at[pl.ds(1, self.no - 1)]
        arrived(others, self.p_recv)
        arrived(others, self.p_send)
        total = self.pr[0].astype(f32)
        for i in range(1, self.no):
            total = total + self.rr[i].astype(f32)
        return total


class Exchange:
    def __init__(self, axis, size, send_at, recv_at, others, sems):
        self.axis, self.size = axis, size
        self.send_at, self.recv_at, self.others = send_at, recv_at, others
        self.send, self.recv = sems.at[0], sems.at[1]
        self.me = lax.axis_index(axis)

    def start(self):
        @pl.loop(1, self.size)
        def _(i):
            to = lax.rem(self.me + i, self.size)
            pltpu.make_async_remote_copy(
                src_ref=self.send_at(to),
                dst_ref=self.recv_at(self.me),
                send_sem=self.send,
                recv_sem=self.recv,
                device_id={self.axis: to},
                device_id_type=MESH,
            ).start()

    def wait(self):
        arrived(self.others, self.recv)
        arrived(self.others, self.send)


class Spread:
    def __init__(self, grid, ref, sems):
        self.ny, self.nx = grid
        self.ref, self.sems = ref, sems
        self.y, self.x = split_tp(self.nx)
        self.ep, self.tp = lax.axis_index("ep"), lax.axis_index("tp")
        half = ref.shape[0] // 2
        self.upper, self.lower = pl.ds(0, half), pl.ds(half, half)

    def _send(self, ref, y, x, stage):
        pltpu.make_async_remote_copy(
            src_ref=ref,
            dst_ref=ref,
            send_sem=self.sems.at[stage],
            recv_sem=self.sems.at[4 + stage],
            device_id=(self.ep, y * self.nx + x),
            device_id_type=MESH,
        ).start()

    def _wait(self, rows, blocks, stage):
        ref = self.ref.at[rows, pl.ds(0, blocks * LANES)]
        arrived(ref, self.sems.at[4 + stage])
        return lambda: arrived(ref, self.sems.at[stage])

    def start(self):
        for i in range(1, self.nx):
            self._send(self.ref.at[self.upper, block(self.tp)], self.y, lax.rem(self.x + i, self.nx), 0)
        for i in range(1, self.ny):
            self._send(self.ref.at[self.lower, block(self.tp)], lax.rem(self.y + i, self.ny), self.x, 1)

    def relay(self):
        sent = [self._wait(self.upper, self.nx - 1, 0), self._wait(self.lower, self.ny - 1, 1)]
        for i in range(1, self.ny):
            ref = self.ref.at[self.upper, block(self.y, self.nx * LANES)]
            self._send(ref, lax.rem(self.y + i, self.ny), self.x, 2)
        for i in range(1, self.nx):
            for y in range(self.ny):
                ref = self.ref.at[self.lower, block(y * self.nx + self.x)]
                self._send(ref, self.y, lax.rem(self.x + i, self.nx), 3)
        for wait in sent:
            wait()

    def wait(self):
        blocks = (self.nx - 1) * self.ny
        sent = [self._wait(self.upper, (self.ny - 1) * self.nx, 2), self._wait(self.lower, blocks, 3)]
        for wait in sent:
            wait()


class Routing:
    def __init__(self, tokens, experts, cap):
        self.tokens, self.experts, self.cap = tokens, experts, cap

    @staticmethod
    def _iota(shape, dim):
        return lax.broadcasted_iota(jnp.int32, shape, dim)

    @staticmethod
    def _ones(cond):
        return jnp.where(cond, 1.0, 0.0).astype(bf16)

    def to_slots(self, routes_t):
        n, e = self.tokens, self.experts
        expert = self._iota((e, n), 0)
        member = self._ones(jnp.logical_or(expert == routes_t[0:1, :], expert == routes_t[1:2, :]))
        earlier = self._ones(self._iota((n, n), 0) < self._iota((n, n), 1))
        place = jnp.dot(member, earlier, preferred_element_type=f32).astype(bf16)
        spread = self._ones(self._iota((e * PAD, e), 0) // PAD == self._iota((e * PAD, e), 1))
        member = jnp.dot(spread, member, preferred_element_type=f32)
        place = jnp.dot(spread, place, preferred_element_type=f32)
        here = (self._iota((e * PAD, n), 0) % PAD).astype(f32)
        return self._ones(jnp.logical_and(member > 0.5, place == here))

    def column(self, row):
        n = self.tokens
        same = self._iota((n, n), 0) == self._iota((n, n), 1)
        return jnp.sum(jnp.where(same, row.astype(f32), 0.0), axis=1, keepdims=True)

    def from_slots(self, routes_t):
        n, e = self.tokens, self.experts
        expert = self._iota((n, e), 1).astype(f32)
        members = [self._ones(expert == self.column(routes_t[k : k + 1, :])) for k in range(TOP_K)]
        earlier = self._ones(self._iota((n, n), 1) < self._iota((n, n), 0))
        place = jnp.dot(earlier, members[0] + members[1], preferred_element_type=f32).astype(bf16)
        spread = self._ones(self._iota((e, e * PAD), 1) // PAD == self._iota((e, e * PAD), 0))
        place = jnp.dot(place, spread, preferred_element_type=f32)
        here = (self._iota((n, e * PAD), 1) % PAD).astype(f32)
        out = []
        for member in members:
            member = jnp.dot(member, spread, preferred_element_type=f32)
            out.append(self._ones(jnp.logical_and(member > 0.5, place == here)))
        return out

    def packing(self, transposed):
        small, large = self.experts * self.cap, self.experts * PAD
        shape, dims = ((large, small), (1, 0)) if transposed else ((small, large), (0, 1))
        row, col = self._iota(shape, dims[0]), self._iota(shape, dims[1])
        return self._ones(jnp.logical_and(row == col // PAD * self.cap + col % PAD, col % PAD < self.cap))


def swiglu(x, weights):
    both = jnp.dot(x, weights, preferred_element_type=f32)
    gate, up = both[:, :LANES], both[:, LANES:]
    return (gate / (1.0 + jnp.exp(-gate)) * up).astype(bf16)


class Ring:
    def __init__(self, nz, kbuf, vbuf, recv, send, pass_send):
        self.nz = nz
        self.up_steps, self.down_steps = nz // 2, nz - 1 - nz // 2
        self.bufs = (kbuf, vbuf)
        self.recv, self.send, self.pass_send = recv, send, pass_send
        ep = lax.axis_index("ep")
        self.tp = lax.axis_index("tp")
        self.z, self.c = ep // CORES, ep % CORES

    def _device(self, z, c):
        return (z * CORES + c, self.tp)

    def neighbours(self):
        up = lax.rem(self.z + 1, self.nz)
        down = lax.rem(self.z + self.nz - 1, self.nz)
        return [self._device(up, self.c), self._device(down, self.c), self._device(self.z, 1 - self.c)]

    def copy(self, source, part, to_z, sem):
        slot = source * CORES + self.c
        ref = self.bufs[part].at[slot]
        return pltpu.make_async_remote_copy(
            src_ref=ref,
            dst_ref=ref,
            send_sem=self.send.at[sem, part],
            recv_sem=self.recv.at[slot, part],
            device_id=self._device(to_z, self.c),
            device_id_type=MESH,
        )

    def up(self, source, part):
        return self.copy(source, part, lax.rem(self.z + 1, self.nz), source)

    def down(self, source, part, sem=None):
        to = lax.rem(self.z + self.nz - 1, self.nz)
        return self.copy(source, part, to, source if sem is None else sem)

    def handed(self, source, part, core):
        slot = source * CORES + core
        ref = self.bufs[part].at[slot]
        return pltpu.make_async_remote_copy(
            src_ref=ref,
            dst_ref=ref,
            send_sem=self.pass_send.at[source, part],
            recv_sem=self.recv.at[slot, part],
            device_id=self._device(self.z, 1 - self.c),
            device_id_type=MESH,
        )

    def up_source(self, t):
        return self.z - t, self.z - t >= 0

    def down_source(self, t):
        source = lax.rem(self.z + t, self.nz)
        return source, jnp.logical_and(source < self.down_steps, t <= self.down_steps)

    def start_own(self):
        for part in range(2):

            @pl.when(self.z < self.nz - 1)
            def _():
                self.up(self.z, part).start()

            @pl.when(self.z < self.down_steps)
            def _():
                self.down(self.z, part, self.nz).start()

            @pl.when(self.c == 0)
            def _():
                self.handed(self.z, part, self.c).start()

    def serve(self, t, part):
        source, here = self.up_source(t)

        @pl.when(here)
        def _():
            self.up(source, part).wait_recv()

            @pl.when(jnp.logical_and(t < self.up_steps, self.z < self.nz - 1))
            def _():
                self.up(source, part).start()

            self.handed(source, part, self.c).start()

        source_d, here_d = self.down_source(t)

        @pl.when(here_d)
        def _():
            self.down(source_d, part).wait_recv()

            @pl.when(t < self.down_steps)
            def _():
                self.down(source_d, part).start()

            @pl.when(source_d < self.z)
            def _():
                self.handed(source_d, part, self.c).start()

    def wait_handed(self, source):
        for part in range(2):
            self.handed(source, part, 1 - self.c).wait_recv()

    def wait_sends(self):
        for part in range(2):

            @pl.when(self.z < self.nz - 1)
            def _():
                self.up(self.z, part).wait_send()

            @pl.when(self.z < self.down_steps)
            def _():
                self.down(self.z, part, self.nz).wait_send()

            @pl.when(self.c == 0)
            def _():
                self.handed(self.z, part, self.c).wait_send()

        @pl.loop(1, self.up_steps + 1)
        def _(t):
            source, here = self.up_source(t)
            source_d, here_d = self.down_source(t)

            @pl.when(here)
            def _():
                for part in range(2):
                    self.handed(source, part, self.c).wait_send()

                    @pl.when(jnp.logical_and(t < self.up_steps, self.z < self.nz - 1))
                    def _():
                        self.up(source, part).wait_send()

            @pl.when(here_d)
            def _():
                for part in range(2):

                    @pl.when(t < self.down_steps)
                    def _():
                        self.down(source_d, part).wait_send()

                    @pl.when(source_d < self.z)
                    def _():
                        self.handed(source_d, part, self.c).wait_send()


class Softmax:
    def __init__(self, rows, tile, qz, kbuf, vbuf, top, acc, scores):
        self.rows, self.tile = rows, tile
        self.qz, self.kbuf, self.vbuf = qz, kbuf, vbuf
        self.top, self.acc, self.scores = top, acc, scores
        self.tiles = [pl.ds(i * tile, tile) for i in range(2 * rows // tile)]

    @staticmethod
    def _summed(p, values):
        ones = jnp.ones(values.shape, bf16)
        return jnp.dot(p.astype(bf16), jnp.concatenate([values, ones], axis=1), preferred_element_type=f32)

    def diagonal(self, slot):
        keys, values = self.kbuf[slot], self.vbuf[slot]
        for i, rows in enumerate(self.tiles):
            s = jnp.dot(self.qz[rows, :], keys, preferred_element_type=f32)
            row = i * self.tile + lax.broadcasted_iota(jnp.int32, s.shape, 0)
            row = jnp.where(row >= self.rows, row - self.rows, row)
            allowed = lax.broadcasted_iota(jnp.int32, s.shape, 1) <= row
            s = jnp.where(allowed, s, masked_low)
            top = jnp.max(s, axis=1, keepdims=True)
            p = jnp.where(allowed, jnp.exp(s - top), 0.0)
            self.top[rows, :] = jnp.broadcast_to(top, (self.tile, LANES))
            self.acc[rows, :] = self._summed(p, values)

    def _add(self, keys, values):
        count = keys.shape[1]
        cuts = [(j, min(2 * LANES, count - j)) for j in range(0, count, 2 * LANES)]
        tops = {}

        def score(i, j, width):
            s = jnp.dot(self.qz[self.tiles[i], :], keys[:, j : j + width], preferred_element_type=f32)
            self.scores[i % 2, :, j : j + width] = s
            for k in range(0, width, LANES):
                part = s[:, k : k + LANES]
                tops[i] = jnp.maximum(tops[i], part) if i in tops else part

        for j, width in cuts:
            score(0, j, width)
        for i, rows in enumerate(self.tiles):
            before = self.top[rows, :]
            top = jnp.maximum(before, jnp.max(tops[i], axis=1, keepdims=True))
            scale = jnp.exp(before - top)
            self.top[rows, :] = top
            total = self.acc[rows, :] * jnp.concatenate([scale, scale], axis=1)
            for j, width in cuts:
                if i + 1 < len(self.tiles):
                    score(i + 1, j, width)
                s = self.scores[i % 2, :, j : j + width]
                p = jnp.exp(s - jnp.concatenate([top] * (width // LANES), axis=1))
                total = total + self._summed(p, values[j : j + width])
            self.acc[rows, :] = total

    def one(self, slot):
        self._add(self.kbuf[slot], self.vbuf[slot])

    def chip(self, source):
        first, second = source * CORES, source * CORES + 1
        self._add(
            jnp.concatenate([self.kbuf[first], self.kbuf[second]], axis=1),
            jnp.concatenate([self.vbuf[first], self.vbuf[second]], axis=0),
        )

    def heads(self, lam, gain):
        acc = self.acc[...]
        out = acc[:, :LANES] / acc[:, LANES:]
        diff = out[: self.rows] - lam * out[self.rows :]
        mean = jnp.mean(diff * diff, axis=1, keepdims=True)
        return (diff * lax.rsqrt(mean + norm_eps) * gain).astype(bf16)


def kernel(dims, *refs):
    nz, ny, nx, rows, tile, tokens, experts, cap = dims
    refs = list(refs)

    def take(n):
        out = refs[:n]
        del refs[:n]
        return out

    inputs = take(8)
    (v_hbm,) = take(1)
    lam_ref, wo_hbm, wg_hbm, wu_hbm, wd_hbm, sg_hbm, su_hbm, sd_hbm = take(8)
    attn_hbm, moe_hbm = take(2)
    buffers = take(7)
    (load_sem,) = take(1)
    q_ref, k_ref, freq_ref, gain_ref, x_ref, fgain_ref, routes_ref = buffers
    kbuf, vbuf, qz, top, acc, scores, ring_recv, ring_send, pass_send = take(9)
    xn, wgu, sgu = take(3)
    out_slots, in_slots, xg, back_out, back_in = take(5)
    a_sems, g_sems, b_sems = take(3)
    attn_ref, moe_ref, rweight_ref, sine_ref, cosine_ref = take(5)
    grid = (ny, nx)
    ep, tp = lax.axis_index("ep"), lax.axis_index("tp")
    eps, tps = nz * CORES, ny * nx

    ring = Ring(nz, kbuf, vbuf, ring_recv, ring_send, pass_send)
    soft = Softmax(rows, tile, qz, kbuf, vbuf, top, acc, scores)
    projections = []
    for axis, weight in zip(AXES, (wo_hbm, wd_hbm, sd_hbm)):
        wb, hx, pr, rr, sems = take(5)
        projections.append(Projection(grid, axis, weight, wb, hx, pr, rr, sems))
    out_proj, down, shared_down = projections
    routing = Routing(tokens, experts, cap)

    barrier = pltpu.get_barrier_semaphore()
    for axis, me, size in (("ep", ep, eps), ("tp", tp, tps)):

        @pl.loop(1, size)
        def _(i):
            to = lax.rem(me + i, size)
            pl.semaphore_signal(barrier, inc=1, device_id={axis: to}, device_id_type=MESH)

    pairs = zip(inputs, buffers + [rweight_ref])
    loads = [pltpu.make_async_copy(a, b, load_sem.at[i]) for i, (a, b) in enumerate(pairs)]
    q_load, k_load, freq_load, gain_load, x_load, fgain_load, routes_load, rweight_load = loads
    weights = []
    for i, (source, buf, k) in enumerate(((sg_hbm, sgu, 0), (su_hbm, sgu, 1), (wg_hbm, wgu, 0), (wu_hbm, wgu, 1))):
        sem = load_sem.at[len(loads) + i]
        weights.append(pltpu.make_async_copy(source, buf.at[:, pl.ds(k * LANES, LANES)], sem))
    v_load = pltpu.make_async_copy(v_hbm, vbuf.at[ep], load_sem.at[len(loads) + 4])
    for load in (freq_load, k_load, v_load, x_load, fgain_load, routes_load, q_load, gain_load, rweight_load):
        load.start()
    for load in weights:
        load.start()
    for projection in projections:
        projection.start_own_weights()

    with jax.named_scope("pre_angles"):
        freq_load.wait()
        cosine, sine = angle_tables(ep, rows, freq_ref[...])
        cosine_ref[...] = cosine
        sine_ref[...] = sine
    with jax.named_scope("pre_keys"):
        k_load.wait()
        kbuf[ep] = jnp.transpose(rotated(k_ref[...], cosine_ref[...], sine_ref[...])).astype(bf16)
    with jax.named_scope("pre_norm"):
        x_load.wait()
        fgain_load.wait()
        x = x_ref[...].astype(f32)
        inverse = lax.rsqrt(jnp.mean(x * x, axis=1, keepdims=True) + norm_eps)
        xn[...] = (x * inverse * fgain_ref[...]).astype(bf16)
    with jax.named_scope("pre_routes"):
        routes_load.wait()
        to_slots = routing.to_slots(routes_ref[...])
        sent = jnp.dot(to_slots, xn[:, block(tp)], preferred_element_type=f32).astype(bf16)
        out_slots[...] = sent.reshape(experts, PAD, LANES)
        in_slots[ep] = out_slots[ep]
        v_load.wait()

    with jax.named_scope("barrier"):
        pl.semaphore_wait(barrier, eps + tps - 2)
    slots = pl.ds(0, eps - 1)
    there = Exchange("ep", eps, lambda i: out_slots.at[i], lambda i: in_slots.at[i], in_slots.at[slots], a_sems)
    spread = Spread(grid, xg, g_sems)
    back = Exchange("ep", eps, lambda i: back_out.at[i], lambda i: back_in.at[i], back_in.at[slots], b_sems)
    there.start()
    ring.start_own()
    down.start_weights()
    shared_down.start_weights()
    out_proj.start_weights()

    q_load.wait()
    q = rotated(q_ref[...], cosine_ref[...], sine_ref[...]).astype(bf16).astype(f32) * 0.125
    lane = lax.broadcasted_iota(jnp.int32, q.shape, 1)
    qz[:rows, :] = jnp.where(lane < 64, q, 0.0).astype(bf16)
    qz[rows:, :] = jnp.where(lane < 64, 0.0, q).astype(bf16)
    weights[0].wait()
    weights[1].wait()
    with jax.named_scope("shared_diagonal"):
        shared_down.start_gather(swiglu(xn[...], sgu[...]))
        soft.diagonal(ep)

    @pl.when(ring.c == 1)
    def _():
        ring.wait_handed(ring.z)
        soft.one(ep - 1)

    def use(source):
        ring.wait_handed(source)
        soft.chip(source)

    def use_up(t):
        source, here = ring.up_source(t)

        @pl.when(jnp.logical_and(here, t >= 1))
        def _():
            with jax.named_scope("use_up"):
                use(source)

    def use_down(t):
        source, here = ring.down_source(t)

        @pl.when(jnp.logical_and(jnp.logical_and(here, t >= 1), source < ring.z))
        def _():
            with jax.named_scope("use_down"):
                use(source)

    @pl.loop(1, ring.up_steps + 1)
    def _(t):
        with jax.named_scope("serve_keys"):
            ring.serve(t, 0)
        use_up(t - 1)
        with jax.named_scope("serve_values"):
            ring.serve(t, 1)
        use_down(t - 1)

        @pl.when(t == SPREAD_AT)
        def _():
            with jax.named_scope("there_wait"):
                there.wait()
            rows_in = in_slots[...].reshape(experts * PAD, LANES)
            rows_in = jnp.dot(routing.packing(False), rows_in, preferred_element_type=f32)
            xg[:, block(tp)] = rows_in.astype(bf16)
            spread.start()

        @pl.when(t == SHARED_AT)
        def _():
            with jax.named_scope("shared_multiply"):
                shared_down.wait_weights()
                shared_down.multiply_and_send()

        @pl.when(t == RELAY_AT)
        def _():
            with jax.named_scope("relay"):
                spread.relay()

        @pl.when(t == EXPERT_AT)
        def _():
            weights[2].wait()
            weights[3].wait()
            with jax.named_scope("spread_wait"):
                spread.wait()
            with jax.named_scope("experts"):
                down.start_gather(swiglu(xg[...], wgu[...]))

        @pl.when(t == DOWN_AT)
        def _():
            with jax.named_scope("down_multiply"):
                down.wait_weights()
                down.multiply_and_send()

        @pl.when(t == BACK_AT)
        def _():
            with jax.named_scope("down_finish"):
                y = down.finish().astype(bf16)
            y = jnp.dot(routing.packing(True), y, preferred_element_type=f32).astype(bf16)
            back_out[...] = y.reshape(experts, PAD, LANES)
            back_in[ep] = back_out[ep]
            back.start()

    use_up(ring.up_steps)
    gain_load.wait()
    with jax.named_scope("heads"):
        out_proj.start_gather(soft.heads(lam_ref[0], gain_ref[...]))
    with jax.named_scope("shared_finish"):
        mixed = shared_down.finish()
        chosen = routing.from_slots(routes_ref[...])
    with jax.named_scope("out_multiply"):
        out_proj.wait_weights()
        out_proj.multiply_and_send()
    rweight_load.wait()
    with jax.named_scope("back_wait"):
        back.wait()
    returned = back_in[...].reshape(experts * PAD, LANES)
    for k in range(TOP_K):
        picked = jnp.dot(chosen[k], returned, preferred_element_type=f32)
        mixed = mixed + routing.column(rweight_ref[k : k + 1, :]) * picked
    moe_ref[...] = mixed.astype(bf16)
    moe_store = pltpu.make_async_copy(moe_ref, moe_hbm, load_sem.at[0])
    moe_store.start()
    with jax.named_scope("out_finish"):
        attn_ref[...] = out_proj.finish().astype(bf16)
    attn_store = pltpu.make_async_copy(attn_ref, attn_hbm, load_sem.at[1])
    attn_store.start()
    with jax.named_scope("wait_sends"):
        ring.wait_sends()
    moe_store.wait()
    attn_store.wait()


def local(
    sizes,
    query_pairs,
    key_pairs,
    value_rows,
    head_lambda,
    head_gain,
    out_weight,
    moe_input,
    ffn_gain,
    routes,
    route_weight,
    gate_weight,
    up_weight,
    down_weight,
    shared_gate,
    shared_up,
    shared_down,
):
    nz, ny, nx = sizes
    grid = (ny, nx)
    rows, tokens, width = query_pairs.shape[0], moe_input.shape[0], moe_input.shape[1]
    slots, experts = nz * CORES, nz * CORES
    cap = 12
    tile = 256 if (2 * rows) % 256 == 0 else 2 * rows
    hbm = pl.BlockSpec(memory_space=pl.ANY)
    dma = pltpu.SemaphoreType.DMA
    scratch = [
        pltpu.VMEM((rows, LANES), bf16),
        pltpu.VMEM((rows, LANES), bf16),
        pltpu.VMEM((1, LANES), f32),
        pltpu.VMEM((1, LANES), f32),
        pltpu.VMEM((tokens, width), bf16),
        pltpu.VMEM((1, width), f32),
        pltpu.VMEM((TOP_K, tokens), jnp.int32),
        dma((13,)),
        pltpu.VMEM((slots, LANES, rows), bf16),
        pltpu.VMEM((slots, rows, LANES), bf16),
        pltpu.VMEM((2 * rows, LANES), bf16),
        pltpu.VMEM((2 * rows, LANES), f32),
        pltpu.VMEM((2 * rows, 2 * LANES), f32),
        pltpu.VMEM((2, tile, CORES * rows), f32),
        dma((slots, 2)),
        dma((nz + 1, 2)),
        dma((nz, 2)),
        pltpu.VMEM((tokens, width), bf16),
        pltpu.VMEM((width, 2 * LANES), bf16),
        pltpu.VMEM((width, 2 * LANES), bf16),
        pltpu.VMEM((experts, PAD, LANES), bf16),
        pltpu.VMEM((experts, PAD, LANES), bf16),
        pltpu.VMEM((experts * cap, width), bf16),
        pltpu.VMEM((experts, PAD, LANES), bf16),
        pltpu.VMEM((experts, PAD, LANES), bf16),
        dma((2,)),
        dma((8,)),
        dma((2,)),
        pltpu.VMEM((rows, LANES), bf16),
        pltpu.VMEM((tokens, LANES), bf16),
        pltpu.VMEM((TOP_K, tokens), f32),
        pltpu.VMEM((rows, LANES), f32),
        pltpu.VMEM((rows, LANES), f32),
    ]
    for axis, height in zip(AXES, (rows, experts * cap, tokens)):
        scratch += Projection.scratch(grid, axis, height)
    return tuple(
        pl.pallas_call(
            functools.partial(kernel, (nz, ny, nx, rows, tile, tokens, experts, cap)),
            out_shape=[
                jax.ShapeDtypeStruct((rows, LANES), bf16),
                jax.ShapeDtypeStruct((tokens, LANES), bf16),
            ],
            in_specs=[hbm] * 9 + [pl.BlockSpec(memory_space=pltpu.SMEM)] + [hbm] * 7,
            out_specs=[hbm, hbm],
            scratch_shapes=scratch,
            compiler_params=pltpu.CompilerParams(
                collective_id=0, has_side_effects=True, vmem_limit_bytes=56 * 1024 * 1024
            ),
            name="layer",
        )(
            query_pairs,
            key_pairs,
            frequencies(),
            head_gain.reshape(1, -1),
            moe_input,
            ffn_gain.reshape(1, -1),
            routes.T,
            route_weight.T,
            value_rows,
            head_lambda,
            out_weight,
            gate_weight[0],
            up_weight[0],
            down_weight[0],
            shared_gate,
            shared_up,
            shared_down,
        )
    )


def grid_of(mesh):
    side = int(round(mesh.shape["tp"] ** 0.5))
    return mesh.shape["ep"] // CORES, mesh.shape["tp"] // side, side


def solution(mesh):
    return jax.shard_map(
        functools.partial(local, grid_of(mesh)),
        mesh=mesh,
        in_specs=(
            P("ep", "tp"),
            P("ep", "tp"),
            P("ep", "tp"),
            P("tp"),
            P(),
            P("tp", None),
            P("ep", None),
            P(),
            P("ep", None),
            P("ep", None),
            P("ep", None, "tp"),
            P("ep", None, "tp"),
            P("ep", "tp", None),
            P(None, "tp"),
            P(None, "tp"),
            P("tp", None),
        ),
        out_specs=(P("ep", "tp"), P("ep", "tp")),
        check_vma=False,
    )
```

```python
import functools

import jax
import jax.numpy as jnp
import numpy as np
from jax import lax
from jax.experimental import pallas as pl
from jax.experimental.pallas import tpu as pltpu
from jax.sharding import PartitionSpec as P

TOP_K = 2

theta_base = 500000.0
norm_eps = 1e-06
masked_low = -1e30

CORES = 2
LANES = 128
PAD = 16
PARTS = 4
MESH = pl.DeviceIdType.MESH
f32 = jnp.float32
bf16 = jnp.bfloat16

AXES = ("x", "y", "x", "y")
RELAY_AT, SHARED_AT, EXPERT_AT, DOWN_AT, BACK_AT = 1, 3, 4, 6, 8


def frequencies():
    place = (np.arange(LANES) % 32).astype(np.float32)
    return np.power(np.float32(theta_base), -(place * np.float32(2.0)) / np.float32(64)).reshape(1, LANES)


def angle_tables(ep, rows, frequency):
    quarter = rows // 4
    shape = (quarter, LANES)
    lane = lax.broadcasted_iota(jnp.int32, shape, 1)
    group = lane // 32
    positions = ep * rows + group * quarter + lax.broadcasted_iota(jnp.int32, shape, 0)
    angles = positions.astype(f32) * frequency
    sign = jnp.where(lane % 64 < 32, -1.0, 1.0)

    def spread(table, g):
        x = jnp.where(group == g, table, 0.0)
        x = x + pltpu.roll(x, 32, 1)
        return x + pltpu.roll(x, 64, 1)

    cosine, sine = jnp.cos(angles), jnp.sin(angles)
    return (
        jnp.concatenate([spread(cosine, g) for g in range(4)], axis=0),
        jnp.concatenate([spread(sine, g) * sign for g in range(4)], axis=0),
    )


def rotated(x, cosine, sine):
    x = x.astype(f32)
    lane = lax.broadcasted_iota(jnp.int32, x.shape, 1)
    swapped = jnp.where(lane % 64 < 32, pltpu.roll(x, 96, 1), pltpu.roll(x, 32, 1))
    return x * cosine + swapped * sine


def block(i, width=LANES):
    return pl.ds(pl.multiple_of(i * width, width), width)


def split_tp(nx):
    tp = lax.axis_index("tp")
    return tp // nx, tp % nx


def arrived(ref, sem):
    pltpu.make_async_copy(ref, ref, sem).wait()


class Projection:
    def __init__(self, grid, axis, w_hbm, wb, hx, pr, rr, sems):
        self.ny, self.nx = grid
        self.axis = axis
        self.w, self.wb, self.hx, self.pr, self.rr = w_hbm, wb, hx, pr, rr
        names = ("w_send", "w_recv", "w_local", "h_send", "h_recv", "p_send", "p_recv")
        for i, name in enumerate(names):
            setattr(self, name, sems.at[i])
        y, x = split_tp(self.nx)
        self.g, self.o, self.ng, self.no = (y, x, self.ny, self.nx) if axis == "y" else (x, y, self.nx, self.ny)
        self.ep = lax.axis_index("ep")

    @staticmethod
    def scratch(grid, axis, rows):
        ng, no = grid if axis == "y" else grid[::-1]
        dma = pltpu.SemaphoreType.DMA
        return [
            pltpu.VMEM((ng * LANES, no * LANES), bf16),
            pltpu.VMEM((rows, ng * LANES), bf16),
            pltpu.VMEM((no, rows, LANES), bf16),
            pltpu.VMEM((no, rows, LANES), bf16),
            dma((7,)),
        ]

    def _tp(self, g, o):
        return g * self.nx + o if self.axis == "y" else o * self.nx + g

    def _weights(self, g):
        rows = block(self.g)
        if self.axis == "y":
            width = self.no * LANES
            yield self.w.at[:, block(g, width)], self.wb.at[rows, :]
            return
        for o in range(self.no):
            yield self.w.at[:, block(self._tp(g, o))], self.wb.at[rows, pl.ds(o * LANES, LANES)]

    def start_own_weights(self):
        for source, target in self._weights(self.g):
            pltpu.make_async_copy(source, target, self.w_local).start()

    def start_weights(self):
        for i in range(1, self.ng):
            g = lax.rem(self.g + i, self.ng)
            for source, target in self._weights(g):
                pltpu.make_async_remote_copy(
                    src_ref=source,
                    dst_ref=target,
                    send_sem=self.w_send,
                    recv_sem=self.w_recv,
                    device_id=(self.ep, self._tp(g, self.o)),
                    device_id_type=MESH,
                ).start()

    def wait_weights(self):
        one, others = self.wb.at[pl.ds(0, LANES), :], self.wb.at[pl.ds(0, (self.ng - 1) * LANES), :]
        arrived(one, self.w_local)
        arrived(others, self.w_recv)
        arrived(others, self.w_send)

    def _gather(self, i):
        own = self.hx.at[:, block(self.g)]
        return pltpu.make_async_remote_copy(
            src_ref=own,
            dst_ref=own,
            send_sem=self.h_send,
            recv_sem=self.h_recv,
            device_id=(self.ep, self._tp(lax.rem(self.g + i, self.ng), self.o)),
            device_id_type=MESH,
        )

    def start_gather(self, h):
        self.hx[:, block(self.g)] = h
        for i in range(1, self.ng):
            self._gather(i).start()

    def _partial(self, i):
        return pltpu.make_async_remote_copy(
            src_ref=self.pr.at[i],
            dst_ref=self.rr.at[i],
            send_sem=self.p_send,
            recv_sem=self.p_recv,
            device_id=(self.ep, self._tp(self.g, lax.rem(self.o + i, self.no))),
            device_id_type=MESH,
        )

    def multiply_and_send(self):
        others = self.hx.at[:, pl.ds(0, (self.ng - 1) * LANES)]
        arrived(others, self.h_recv)
        arrived(others, self.h_send)
        h = self.hx[...]
        for i in list(range(1, self.no)) + [0]:
            w = self.wb[:, block(lax.rem(self.o + i, self.no))]
            self.pr[i] = jnp.dot(h, w, preferred_element_type=f32).astype(bf16)
            if i:
                self._partial(i).start()

    def finish(self):
        others = self.rr.at[pl.ds(1, self.no - 1)]
        arrived(others, self.p_recv)
        arrived(others, self.p_send)
        total = self.pr[0].astype(f32)
        for i in range(1, self.no):
            total = total + self.rr[i].astype(f32)
        return total


class Exchange:
    def __init__(self, axis, size, send_at, recv_at, others, sems):
        self.axis, self.size = axis, size
        self.send_at, self.recv_at, self.others = send_at, recv_at, others
        self.send, self.recv = sems.at[0], sems.at[1]
        self.me = lax.axis_index(axis)

    def start(self):
        middle = self.size // 2

        @pl.loop(1, self.size)
        def _(i):
            away = jnp.where(i % 2 == 0, middle - i // 2, middle + i // 2)
            to = lax.rem(self.me + away, self.size)
            pltpu.make_async_remote_copy(
                src_ref=self.send_at(to),
                dst_ref=self.recv_at(self.me),
                send_sem=self.send,
                recv_sem=self.recv,
                device_id={self.axis: to},
                device_id_type=MESH,
            ).start()

    def wait(self):
        arrived(self.others, self.recv)
        arrived(self.others, self.send)


class Spread:
    def __init__(self, grid, ref, sems):
        self.ny, self.nx = grid
        self.ref, self.sems = ref, sems
        self.y, self.x = split_tp(self.nx)
        self.ep, self.tp = lax.axis_index("ep"), lax.axis_index("tp")
        half = ref.shape[0] // 2
        self.upper, self.lower = pl.ds(0, half), pl.ds(half, half)

    def _send(self, ref, y, x, stage):
        pltpu.make_async_remote_copy(
            src_ref=ref,
            dst_ref=ref,
            send_sem=self.sems.at[stage],
            recv_sem=self.sems.at[4 + stage],
            device_id=(self.ep, y * self.nx + x),
            device_id_type=MESH,
        ).start()

    def _wait(self, rows, blocks, stage):
        ref = self.ref.at[rows, pl.ds(0, blocks * LANES)]
        arrived(ref, self.sems.at[4 + stage])
        return lambda: arrived(ref, self.sems.at[stage])

    def start(self):
        for i in range(1, self.nx):
            self._send(self.ref.at[self.upper, block(self.tp)], self.y, lax.rem(self.x + i, self.nx), 0)
        for i in range(1, self.ny):
            self._send(self.ref.at[self.lower, block(self.tp)], lax.rem(self.y + i, self.ny), self.x, 1)

    def relay(self):
        sent = [self._wait(self.upper, self.nx - 1, 0), self._wait(self.lower, self.ny - 1, 1)]
        for i in range(1, self.ny):
            ref = self.ref.at[self.upper, block(self.y, self.nx * LANES)]
            self._send(ref, lax.rem(self.y + i, self.ny), self.x, 2)
        for i in range(1, self.nx):
            for y in range(self.ny):
                ref = self.ref.at[self.lower, block(y * self.nx + self.x)]
                self._send(ref, self.y, lax.rem(self.x + i, self.nx), 3)
        for wait in sent:
            wait()

    def wait(self):
        blocks = (self.nx - 1) * self.ny
        sent = [self._wait(self.upper, (self.ny - 1) * self.nx, 2), self._wait(self.lower, blocks, 3)]
        for wait in sent:
            wait()


class Routing:
    def __init__(self, tokens, experts, cap):
        self.tokens, self.experts, self.cap = tokens, experts, cap

    @staticmethod
    def _iota(shape, dim):
        return lax.broadcasted_iota(jnp.int32, shape, dim)

    @staticmethod
    def _ones(cond):
        return jnp.where(cond, 1.0, 0.0).astype(bf16)

    def to_slots(self, routes_t):
        n, e = self.tokens, self.experts
        expert = self._iota((e, n), 0)
        member = self._ones(jnp.logical_or(expert == routes_t[0:1, :], expert == routes_t[1:2, :]))
        earlier = self._ones(self._iota((n, n), 0) < self._iota((n, n), 1))
        place = jnp.dot(member, earlier, preferred_element_type=f32).astype(bf16)
        spread = self._ones(self._iota((e * PAD, e), 0) // PAD == self._iota((e * PAD, e), 1))
        member = jnp.dot(spread, member, preferred_element_type=f32)
        place = jnp.dot(spread, place, preferred_element_type=f32)
        here = (self._iota((e * PAD, n), 0) % PAD).astype(f32)
        return self._ones(jnp.logical_and(member > 0.5, place == here))

    def column(self, row):
        n = self.tokens
        same = self._iota((n, n), 0) == self._iota((n, n), 1)
        return jnp.sum(jnp.where(same, row.astype(f32), 0.0), axis=1, keepdims=True)

    def from_slots(self, routes_t):
        n, e = self.tokens, self.experts
        expert = self._iota((n, e), 1).astype(f32)
        members = [self._ones(expert == self.column(routes_t[k : k + 1, :])) for k in range(TOP_K)]
        earlier = self._ones(self._iota((n, n), 1) < self._iota((n, n), 0))
        place = jnp.dot(earlier, members[0] + members[1], preferred_element_type=f32).astype(bf16)
        spread = self._ones(self._iota((e, e * PAD), 1) // PAD == self._iota((e, e * PAD), 0))
        place = jnp.dot(place, spread, preferred_element_type=f32)
        here = (self._iota((n, e * PAD), 1) % PAD).astype(f32)
        out = []
        for member in members:
            member = jnp.dot(member, spread, preferred_element_type=f32)
            out.append(self._ones(jnp.logical_and(member > 0.5, place == here)))
        return out

    def packing(self, transposed):
        small, large = self.experts * self.cap, self.experts * PAD
        shape, dims = ((large, small), (1, 0)) if transposed else ((small, large), (0, 1))
        row, col = self._iota(shape, dims[0]), self._iota(shape, dims[1])
        return self._ones(jnp.logical_and(row == col // PAD * self.cap + col % PAD, col % PAD < self.cap))


def swiglu(x, weights):
    both = jnp.dot(x, weights, preferred_element_type=f32)
    gate, up = both[:, :LANES], both[:, LANES:]
    return (gate / (1.0 + jnp.exp(-gate)) * up).astype(bf16)


class Ring:
    def __init__(self, nz, kbuf, vbuf, recv, handed_recv, up_send, down_send, pass_send):
        self.nz = nz
        self.up_steps, self.down_steps = nz // 2, nz - 1 - nz // 2
        self.kbuf, self.vbuf = kbuf, vbuf
        self.recv, self.handed_recv = recv, handed_recv
        self.up_send, self.down_send, self.pass_send = up_send, down_send, pass_send
        ep = lax.axis_index("ep")
        self.tp = lax.axis_index("tp")
        self.z, self.c = ep // CORES, ep % CORES

    def _device(self, z, c):
        return (z * CORES + c, self.tp)

    def _piece(self, slot, part):
        buf = self.kbuf if part < 2 else self.vbuf
        half = buf.shape[1] // 2
        return buf.at[slot, pl.ds(part % 2 * half, half)]

    def _copy(self, source, part, to_z, sems):
        ref = self._piece(source * CORES + self.c, part)
        return pltpu.make_async_remote_copy(
            src_ref=ref,
            dst_ref=ref,
            send_sem=sems.at[part],
            recv_sem=self.recv.at[source, part],
            device_id=self._device(to_z, self.c),
            device_id_type=MESH,
        )

    def up(self, source, part):
        return self._copy(source, part, lax.rem(self.z + 1, self.nz), self.up_send)

    def down(self, source, part):
        return self._copy(source, part, lax.rem(self.z + self.nz - 1, self.nz), self.down_send)

    def _hand(self, source, way):
        for buf in (self.kbuf, self.vbuf):
            ref = buf.at[source * CORES + self.c]
            pltpu.make_async_remote_copy(
                src_ref=ref,
                dst_ref=ref,
                send_sem=self.pass_send.at[way],
                recv_sem=self.handed_recv.at[source],
                device_id=self._device(self.z, 1 - self.c),
                device_id_type=MESH,
            ).start()

    def _both(self, source):
        return self.kbuf.at[pl.ds(source * CORES, CORES)]

    def wait_handed(self, source):
        arrived(self._both(source), self.handed_recv.at[source])

    def _wait_hand_sent(self, way):
        arrived(self._both(0), self.pass_send.at[way])

    def up_source(self, t):
        return self.z - t, self.z - t >= 0

    def down_source(self, t):
        source = lax.rem(self.z + t, self.nz)
        return source, jnp.logical_and(source < self.down_steps, t <= self.down_steps)

    def down_used(self, t):
        source, here = self.down_source(t)
        return source, jnp.logical_and(here, source < self.z)

    def start_own(self):
        for part in range(PARTS):

            @pl.when(self.z < self.nz - 1)
            def _():
                self.up(self.z, part).start()

            @pl.when(self.z < self.down_steps)
            def _():
                self.down(self.z, part).start()

        @pl.when(self.c == 0)
        def _():
            self._hand(self.z, 0)

    def serve(self, t, part):
        source, here = self.up_source(t)

        @pl.when(here)
        def _():
            self.up(source, part).wait_recv()

            @pl.when(jnp.logical_and(t < self.up_steps, self.z < self.nz - 1))
            def _():
                self.up(source, part).wait_send()
                self.up(source, part).start()

        source_d, here_d = self.down_source(t)
        _, sent_before = self.down_source(t - 1)

        @pl.when(here_d)
        def _():
            self.down(source_d, part).wait_recv()

            @pl.when(t < self.down_steps)
            def _():
                @pl.when(sent_before)
                def _():
                    self.down(source_d, part).wait_send()

                self.down(source_d, part).start()

    def hand(self, t):
        source, here = self.up_source(t)

        @pl.when(here)
        def _():
            @pl.when(jnp.logical_or(t > 1, self.c == 0))
            def _():
                self._wait_hand_sent(0)

            self._hand(source, 0)

        source_d, used = self.down_used(t)
        _, used_before = self.down_used(t - 1)

        @pl.when(used)
        def _():
            @pl.when(used_before)
            def _():
                self._wait_hand_sent(1)

            self._hand(source_d, 1)

    def wait_sends(self):
        first_down = self.nz - self.down_steps

        @pl.when(self.z < self.nz - 1)
        def _():
            for part in range(PARTS):
                self.up(self.z, part).wait_send()

        @pl.when(jnp.logical_or(self.z < self.down_steps, self.z > first_down))
        def _():
            for part in range(PARTS):
                self.down(self.z, part).wait_send()

        @pl.when(jnp.logical_or(self.c == 0, self.z >= 1))
        def _():
            self._wait_hand_sent(0)

        @pl.when(self.z >= first_down)
        def _():
            self._wait_hand_sent(1)


class Softmax:
    def __init__(self, rows, tile, qz, kbuf, vbuf, top, acc, scores):
        self.rows, self.tile = rows, tile
        self.qz, self.kbuf, self.vbuf = qz, kbuf, vbuf
        self.top, self.acc, self.scores = top, acc, scores
        self.tiles = [pl.ds(i * tile, tile) for i in range(2 * rows // tile)]

    @staticmethod
    def _summed(p, values):
        ones = jnp.ones(values.shape, bf16)
        return jnp.dot(p.astype(bf16), jnp.concatenate([values, ones], axis=1), preferred_element_type=f32)

    def diagonal(self, slot):
        keys, values = self.kbuf[slot], self.vbuf[slot]
        for i, rows in enumerate(self.tiles):
            s = jnp.dot(self.qz[rows, :], keys, preferred_element_type=f32)
            row = i * self.tile + lax.broadcasted_iota(jnp.int32, s.shape, 0)
            row = jnp.where(row >= self.rows, row - self.rows, row)
            allowed = lax.broadcasted_iota(jnp.int32, s.shape, 1) <= row
            s = jnp.where(allowed, s, masked_low)
            top = jnp.max(s, axis=1, keepdims=True)
            p = jnp.where(allowed, jnp.exp(s - top), 0.0)
            self.top[rows, :] = jnp.broadcast_to(top, (self.tile, LANES))
            self.acc[rows, :] = self._summed(p, values)

    def _add(self, keys, values):
        count = keys.shape[1]
        cuts = [(j, min(2 * LANES, count - j)) for j in range(0, count, 2 * LANES)]
        tops = {}

        def score(i, j, width):
            s = jnp.dot(self.qz[self.tiles[i], :], keys[:, j : j + width], preferred_element_type=f32)
            self.scores[i % 2, :, j : j + width] = s
            for k in range(0, width, LANES):
                part = s[:, k : k + LANES]
                tops[i] = jnp.maximum(tops[i], part) if i in tops else part

        for j, width in cuts:
            score(0, j, width)
        for i, rows in enumerate(self.tiles):
            before = self.top[rows, :]
            top = jnp.maximum(before, jnp.max(tops[i], axis=1, keepdims=True))
            scale = jnp.exp(before - top)
            self.top[rows, :] = top
            total = self.acc[rows, :] * jnp.concatenate([scale, scale], axis=1)
            for j, width in cuts:
                if i + 1 < len(self.tiles):
                    score(i + 1, j, width)
                s = self.scores[i % 2, :, j : j + width]
                p = jnp.exp(s - jnp.concatenate([top] * (width // LANES), axis=1))
                total = total + self._summed(p, values[j : j + width])
            self.acc[rows, :] = total

    def one(self, slot):
        self._add(self.kbuf[slot], self.vbuf[slot])

    def chip(self, source):
        first, second = source * CORES, source * CORES + 1
        self._add(
            jnp.concatenate([self.kbuf[first], self.kbuf[second]], axis=1),
            jnp.concatenate([self.vbuf[first], self.vbuf[second]], axis=0),
        )

    def heads(self, lam, gain):
        acc = self.acc[...]
        out = acc[:, :LANES] / acc[:, LANES:]
        diff = out[: self.rows] - lam * out[self.rows :]
        mean = jnp.mean(diff * diff, axis=1, keepdims=True)
        return (diff * lax.rsqrt(mean + norm_eps) * gain).astype(bf16)


def kernel(dims, *refs):
    nz, ny, nx, rows, tile, tokens, experts, cap = dims
    refs = list(refs)

    def take(n):
        out = refs[:n]
        del refs[:n]
        return out

    inputs = take(8)
    (v_hbm,) = take(1)
    lam_ref, wo_hbm, wg_hbm, wu_hbm, wd_hbm, sg_hbm, su_hbm, sd_hbm = take(8)
    attn_hbm, moe_hbm = take(2)
    buffers = take(7)
    (load_sem,) = take(1)
    q_ref, k_ref, freq_ref, gain_ref, x_ref, fgain_ref, routes_ref = buffers
    kbuf, vbuf, qz, top, acc, scores = take(6)
    ring_sems = take(5)
    xn, wgu, sgu = take(3)
    out_slots, in_slots, xg, back_out, back_in = take(5)
    a_sems, g_sems, b_sems = take(3)
    attn_ref, moe_ref, rweight_ref, sine_ref, cosine_ref = take(5)
    grid = (ny, nx)
    ep, tp = lax.axis_index("ep"), lax.axis_index("tp")
    eps, tps = nz * CORES, ny * nx

    ring = Ring(nz, kbuf, vbuf, *ring_sems)
    soft = Softmax(rows, tile, qz, kbuf, vbuf, top, acc, scores)
    projections = []
    for axis, weight in zip(AXES, (wo_hbm, wo_hbm, wd_hbm, sd_hbm)):
        wb, hx, pr, rr, sems = take(5)
        projections.append(Projection(grid, axis, weight, wb, hx, pr, rr, sems))
    out_upper, out_lower, down, shared_down = projections
    half = rows // 2
    routing = Routing(tokens, experts, cap)

    barrier = pltpu.get_barrier_semaphore()
    for axis, me, size in (("ep", ep, eps), ("tp", tp, tps)):

        @pl.loop(1, size)
        def _(i):
            to = lax.rem(me + i, size)
            pl.semaphore_signal(barrier, inc=1, device_id={axis: to}, device_id_type=MESH)

    pairs = zip(inputs, buffers + [rweight_ref])
    loads = [pltpu.make_async_copy(a, b, load_sem.at[i]) for i, (a, b) in enumerate(pairs)]
    q_load, k_load, freq_load, gain_load, x_load, fgain_load, routes_load, rweight_load = loads
    weights = []
    for i, (source, buf, k) in enumerate(((sg_hbm, sgu, 0), (su_hbm, sgu, 1), (wg_hbm, wgu, 0), (wu_hbm, wgu, 1))):
        sem = load_sem.at[len(loads) + i]
        weights.append(pltpu.make_async_copy(source, buf.at[:, pl.ds(k * LANES, LANES)], sem))
    v_load = pltpu.make_async_copy(v_hbm, vbuf.at[ep], load_sem.at[len(loads) + 4])
    for load in (freq_load, k_load, v_load, x_load, fgain_load, routes_load, q_load, gain_load, rweight_load):
        load.start()
    for load in weights:
        load.start()
    for projection in projections:
        projection.start_own_weights()

    with jax.named_scope("pre_angles"):
        freq_load.wait()
        cosine, sine = angle_tables(ep, rows, freq_ref[...])
        cosine_ref[...] = cosine
        sine_ref[...] = sine
    with jax.named_scope("pre_keys"):
        k_load.wait()
        kbuf[ep] = jnp.transpose(rotated(k_ref[...], cosine_ref[...], sine_ref[...])).astype(bf16)
    with jax.named_scope("pre_norm"):
        x_load.wait()
        fgain_load.wait()
        x = x_ref[...].astype(f32)
        inverse = lax.rsqrt(jnp.mean(x * x, axis=1, keepdims=True) + norm_eps)
        xn[...] = (x * inverse * fgain_ref[...]).astype(bf16)
    with jax.named_scope("pre_routes"):
        routes_load.wait()
        to_slots = routing.to_slots(routes_ref[...])
        sent = jnp.dot(to_slots, xn[:, block(tp)], preferred_element_type=f32).astype(bf16)
        out_slots[...] = sent.reshape(experts, PAD, LANES)
        in_slots[ep] = out_slots[ep]
        v_load.wait()

    with jax.named_scope("barrier"):
        pl.semaphore_wait(barrier, eps + tps - 2)
    slots = pl.ds(0, eps - 1)
    there = Exchange("ep", eps, lambda i: out_slots.at[i], lambda i: in_slots.at[i], in_slots.at[slots], a_sems)
    spread = Spread(grid, xg, g_sems)
    back = Exchange("ep", eps, lambda i: back_out.at[i], lambda i: back_in.at[i], back_in.at[slots], b_sems)
    there.start()
    down.start_weights()
    shared_down.start_weights()

    q_load.wait()
    q = rotated(q_ref[...], cosine_ref[...], sine_ref[...]).astype(bf16).astype(f32) * 0.125
    lane = lax.broadcasted_iota(jnp.int32, q.shape, 1)
    qz[:rows, :] = jnp.where(lane < 64, q, 0.0).astype(bf16)
    qz[rows:, :] = jnp.where(lane < 64, 0.0, q).astype(bf16)
    weights[0].wait()
    weights[1].wait()
    with jax.named_scope("shared_diagonal"):
        shared_down.start_gather(swiglu(xn[...], sgu[...]))
    ring.start_own()
    with jax.named_scope("diagonal"):
        soft.diagonal(ep)

    @pl.when(ring.c == 1)
    def _():
        ring.wait_handed(ring.z)
        soft.one(ep - 1)

    def use(source):
        ring.wait_handed(source)
        soft.chip(source)

    def use_up(t):
        source, here = ring.up_source(t)

        @pl.when(jnp.logical_and(here, t >= 1))
        def _():
            with jax.named_scope("use_up"):
                use(source)

    def use_down(t):
        source, used = ring.down_used(t)

        @pl.when(used)
        def _():
            with jax.named_scope("use_down"):
                use(source)

    with jax.named_scope("there_wait"):
        there.wait()
    rows_in = in_slots[...].reshape(experts * PAD, LANES)
    rows_in = jnp.dot(routing.packing(False), rows_in, preferred_element_type=f32)
    xg[:, block(tp)] = rows_in.astype(bf16)
    spread.start()

    @pl.loop(1, ring.up_steps + 1)
    def _(t):
        with jax.named_scope("serve_0"):
            ring.serve(t, 0)
        use_up(t - 1)
        with jax.named_scope("serve_1_2"):
            ring.serve(t, 1)
            ring.serve(t, 2)
        use_down(t - 1)
        with jax.named_scope("serve_3"):
            ring.serve(t, 3)
            ring.hand(t)

        @pl.when(t == RELAY_AT)
        def _():
            with jax.named_scope("relay"):
                spread.relay()

        @pl.when(t == SHARED_AT)
        def _():
            with jax.named_scope("shared_multiply"):
                shared_down.wait_weights()
                shared_down.multiply_and_send()

        @pl.when(t == EXPERT_AT)
        def _():
            weights[2].wait()
            weights[3].wait()
            with jax.named_scope("spread_wait"):
                spread.wait()
            with jax.named_scope("experts"):
                down.start_gather(swiglu(xg[...], wgu[...]))
            out_upper.start_weights()
            out_lower.start_weights()

        @pl.when(t == DOWN_AT)
        def _():
            with jax.named_scope("down_multiply"):
                down.wait_weights()
                down.multiply_and_send()

        @pl.when(t == BACK_AT)
        def _():
            with jax.named_scope("down_finish"):
                y = down.finish().astype(bf16)
                y = jnp.dot(routing.packing(True), y, preferred_element_type=f32).astype(bf16)
                back_out[...] = y.reshape(experts, PAD, LANES)
                back_in[ep] = back_out[ep]
                back.start()

    use_up(ring.up_steps)
    gain_load.wait()
    with jax.named_scope("heads"):
        heads = soft.heads(lam_ref[0], gain_ref[...])
        out_upper.start_gather(heads[:half])
        out_lower.start_gather(heads[half:])
    with jax.named_scope("shared_finish"):
        mixed = shared_down.finish()
        chosen = routing.from_slots(routes_ref[...])
    with jax.named_scope("out_multiply"):
        for projection in (out_upper, out_lower):
            projection.wait_weights()
            projection.multiply_and_send()
    rweight_load.wait()
    with jax.named_scope("back_wait"):
        back.wait()
    returned = back_in[...].reshape(experts * PAD, LANES)
    for k in range(TOP_K):
        picked = jnp.dot(chosen[k], returned, preferred_element_type=f32)
        mixed = mixed + routing.column(rweight_ref[k : k + 1, :]) * picked
    moe_ref[...] = mixed.astype(bf16)
    moe_store = pltpu.make_async_copy(moe_ref, moe_hbm, load_sem.at[0])
    moe_store.start()
    with jax.named_scope("out_finish"):
        attn_ref[:half, :] = out_upper.finish().astype(bf16)
        attn_ref[half:, :] = out_lower.finish().astype(bf16)
    attn_store = pltpu.make_async_copy(attn_ref, attn_hbm, load_sem.at[1])
    attn_store.start()
    with jax.named_scope("wait_sends"):
        ring.wait_sends()
    moe_store.wait()
    attn_store.wait()


def local(
    sizes,
    query_pairs,
    key_pairs,
    value_rows,
    head_lambda,
    head_gain,
    out_weight,
    moe_input,
    ffn_gain,
    routes,
    route_weight,
    gate_weight,
    up_weight,
    down_weight,
    shared_gate,
    shared_up,
    shared_down,
):
    nz, ny, nx = sizes
    grid = (ny, nx)
    rows, tokens, width = query_pairs.shape[0], moe_input.shape[0], moe_input.shape[1]
    slots, experts = nz * CORES, nz * CORES
    cap = 12
    tile = 256 if (2 * rows) % 256 == 0 else 2 * rows
    hbm = pl.BlockSpec(memory_space=pl.ANY)
    dma = pltpu.SemaphoreType.DMA
    scratch = [
        pltpu.VMEM((rows, LANES), bf16),
        pltpu.VMEM((rows, LANES), bf16),
        pltpu.VMEM((1, LANES), f32),
        pltpu.VMEM((1, LANES), f32),
        pltpu.VMEM((tokens, width), bf16),
        pltpu.VMEM((1, width), f32),
        pltpu.VMEM((TOP_K, tokens), jnp.int32),
        dma((13,)),
        pltpu.VMEM((slots, LANES, rows), bf16),
        pltpu.VMEM((slots, rows, LANES), bf16),
        pltpu.VMEM((2 * rows, LANES), bf16),
        pltpu.VMEM((2 * rows, LANES), f32),
        pltpu.VMEM((2 * rows, 2 * LANES), f32),
        pltpu.VMEM((2, tile, CORES * rows), f32),
        dma((nz, PARTS)),
        dma((nz,)),
        dma((PARTS,)),
        dma((PARTS,)),
        dma((2,)),
        pltpu.VMEM((tokens, width), bf16),
        pltpu.VMEM((width, 2 * LANES), bf16),
        pltpu.VMEM((width, 2 * LANES), bf16),
        pltpu.VMEM((experts, PAD, LANES), bf16),
        pltpu.VMEM((experts, PAD, LANES), bf16),
        pltpu.VMEM((experts * cap, width), bf16),
        pltpu.VMEM((experts, PAD, LANES), bf16),
        pltpu.VMEM((experts, PAD, LANES), bf16),
        dma((2,)),
        dma((8,)),
        dma((2,)),
        pltpu.VMEM((rows, LANES), bf16),
        pltpu.VMEM((tokens, LANES), bf16),
        pltpu.VMEM((TOP_K, tokens), f32),
        pltpu.VMEM((rows, LANES), f32),
        pltpu.VMEM((rows, LANES), f32),
    ]
    for axis, height in zip(AXES, (rows // 2, rows // 2, experts * cap, tokens)):
        scratch += Projection.scratch(grid, axis, height)
    return tuple(
        pl.pallas_call(
            functools.partial(kernel, (nz, ny, nx, rows, tile, tokens, experts, cap)),
            out_shape=[
                jax.ShapeDtypeStruct((rows, LANES), bf16),
                jax.ShapeDtypeStruct((tokens, LANES), bf16),
            ],
            in_specs=[hbm] * 9 + [pl.BlockSpec(memory_space=pltpu.SMEM)] + [hbm] * 7,
            out_specs=[hbm, hbm],
            scratch_shapes=scratch,
            compiler_params=pltpu.CompilerParams(
                collective_id=0, has_side_effects=True, vmem_limit_bytes=56 * 1024 * 1024
            ),
            name="layer",
        )(
            query_pairs,
            key_pairs,
            frequencies(),
            head_gain.reshape(1, -1),
            moe_input,
            ffn_gain.reshape(1, -1),
            routes.T,
            route_weight.T,
            value_rows,
            head_lambda,
            out_weight,
            gate_weight[0],
            up_weight[0],
            down_weight[0],
            shared_gate,
            shared_up,
            shared_down,
        )
    )


def grid_of(mesh):
    side = int(round(mesh.shape["tp"] ** 0.5))
    return mesh.shape["ep"] // CORES, mesh.shape["tp"] // side, side


def solution(mesh):
    return jax.shard_map(
        functools.partial(local, grid_of(mesh)),
        mesh=mesh,
        in_specs=(
            P("ep", "tp"),
            P("ep", "tp"),
            P("ep", "tp"),
            P("tp"),
            P(),
            P("tp", None),
            P("ep", None),
            P(),
            P("ep", None),
            P("ep", None),
            P("ep", None, "tp"),
            P("ep", None, "tp"),
            P("ep", "tp", None),
            P(None, "tp"),
            P(None, "tp"),
            P("tp", None),
        ),
        out_specs=(P("ep", "tp"), P("ep", "tp")),
        check_vma=False,
    )
```

```python
import functools

import jax
import jax.numpy as jnp
import numpy as np
from jax import lax
from jax.experimental import pallas as pl
from jax.experimental.pallas import tpu as pltpu
from jax.sharding import PartitionSpec as P

TOP_K = 2

theta_base = 500000.0
norm_eps = 1e-06
masked_low = -1e30

CORES = 2
LANES = 128
PAD = 16
PARTS = 4
MESH = pl.DeviceIdType.MESH
f32 = jnp.float32
bf16 = jnp.bfloat16

AXES = ("x", "y", "x", "y")
RELAY_AT, SHARED_AT, EXPERT_AT, DOWN_AT, BACK_AT = 1, 3, 4, 6, 7


def frequencies():
    place = (np.arange(LANES) % 32).astype(np.float32)
    return np.power(np.float32(theta_base), -(place * np.float32(2.0)) / np.float32(64)).reshape(1, LANES)


def angle_tables(ep, rows, frequency):
    quarter = rows // 4
    shape = (quarter, LANES)
    lane = lax.broadcasted_iota(jnp.int32, shape, 1)
    group = lane // 32
    positions = ep * rows + group * quarter + lax.broadcasted_iota(jnp.int32, shape, 0)
    angles = positions.astype(f32) * frequency
    sign = jnp.where(lane % 64 < 32, -1.0, 1.0)

    def spread(table, g):
        x = jnp.where(group == g, table, 0.0)
        x = x + pltpu.roll(x, 32, 1)
        return x + pltpu.roll(x, 64, 1)

    cosine, sine = jnp.cos(angles), jnp.sin(angles)
    return (
        jnp.concatenate([spread(cosine, g) for g in range(4)], axis=0),
        jnp.concatenate([spread(sine, g) * sign for g in range(4)], axis=0),
    )


def rotated(x, cosine, sine):
    x = x.astype(f32)
    lane = lax.broadcasted_iota(jnp.int32, x.shape, 1)
    swapped = jnp.where(lane % 64 < 32, pltpu.roll(x, 96, 1), pltpu.roll(x, 32, 1))
    return x * cosine + swapped * sine


def block(i, width=LANES):
    return pl.ds(pl.multiple_of(i * width, width), width)


def split_tp(nx):
    tp = lax.axis_index("tp")
    return tp // nx, tp % nx


def arrived(ref, sem):
    pltpu.make_async_copy(ref, ref, sem).wait()


class Projection:
    def __init__(self, grid, axis, w_hbm, wb, hx, pr, rr, sems):
        self.ny, self.nx = grid
        self.axis = axis
        self.w, self.wb, self.hx, self.pr, self.rr = w_hbm, wb, hx, pr, rr
        names = ("w_send", "w_recv", "w_local", "h_send", "h_recv", "p_send", "p_recv")
        for i, name in enumerate(names):
            setattr(self, name, sems.at[i])
        y, x = split_tp(self.nx)
        self.g, self.o, self.ng, self.no = (y, x, self.ny, self.nx) if axis == "y" else (x, y, self.nx, self.ny)
        self.ep = lax.axis_index("ep")

    @staticmethod
    def scratch(grid, axis, rows):
        ng, no = grid if axis == "y" else grid[::-1]
        dma = pltpu.SemaphoreType.DMA
        return [
            pltpu.VMEM((ng * LANES, no * LANES), bf16),
            pltpu.VMEM((rows, ng * LANES), bf16),
            pltpu.VMEM((no, rows, LANES), bf16),
            pltpu.VMEM((no, rows, LANES), bf16),
            dma((7,)),
        ]

    def _tp(self, g, o):
        return g * self.nx + o if self.axis == "y" else o * self.nx + g

    def _weights(self, g):
        rows = block(self.g)
        if self.axis == "y":
            width = self.no * LANES
            yield self.w.at[:, block(g, width)], self.wb.at[rows, :]
            return
        for o in range(self.no):
            yield self.w.at[:, block(self._tp(g, o))], self.wb.at[rows, pl.ds(o * LANES, LANES)]

    def start_own_weights(self):
        for source, target in self._weights(self.g):
            pltpu.make_async_copy(source, target, self.w_local).start()

    def start_weights(self):
        for i in range(1, self.ng):
            g = lax.rem(self.g + i, self.ng)
            for source, target in self._weights(g):
                pltpu.make_async_remote_copy(
                    src_ref=source,
                    dst_ref=target,
                    send_sem=self.w_send,
                    recv_sem=self.w_recv,
                    device_id=(self.ep, self._tp(g, self.o)),
                    device_id_type=MESH,
                ).start()

    def wait_weights(self):
        one, others = self.wb.at[pl.ds(0, LANES), :], self.wb.at[pl.ds(0, (self.ng - 1) * LANES), :]
        arrived(one, self.w_local)
        arrived(others, self.w_recv)
        arrived(others, self.w_send)

    def _gather(self, i):
        own = self.hx.at[:, block(self.g)]
        return pltpu.make_async_remote_copy(
            src_ref=own,
            dst_ref=own,
            send_sem=self.h_send,
            recv_sem=self.h_recv,
            device_id=(self.ep, self._tp(lax.rem(self.g + i, self.ng), self.o)),
            device_id_type=MESH,
        )

    def start_gather(self, h):
        self.hx[:, block(self.g)] = h
        for i in range(1, self.ng):
            self._gather(i).start()

    def _partial(self, i):
        return pltpu.make_async_remote_copy(
            src_ref=self.pr.at[i],
            dst_ref=self.rr.at[i],
            send_sem=self.p_send,
            recv_sem=self.p_recv,
            device_id=(self.ep, self._tp(self.g, lax.rem(self.o + i, self.no))),
            device_id_type=MESH,
        )

    def multiply_and_send(self):
        others = self.hx.at[:, pl.ds(0, (self.ng - 1) * LANES)]
        arrived(others, self.h_recv)
        arrived(others, self.h_send)
        h = self.hx[...]
        for i in list(range(1, self.no)) + [0]:
            w = self.wb[:, block(lax.rem(self.o + i, self.no))]
            self.pr[i] = jnp.dot(h, w, preferred_element_type=f32).astype(bf16)
            if i:
                self._partial(i).start()

    def finish(self):
        others = self.rr.at[pl.ds(1, self.no - 1)]
        arrived(others, self.p_recv)
        arrived(others, self.p_send)
        total = self.pr[0].astype(f32)
        for i in range(1, self.no):
            total = total + self.rr[i].astype(f32)
        return total


class Exchange:
    def __init__(self, axis, size, send_at, recv_at, others, sems):
        self.axis, self.size = axis, size
        self.send_at, self.recv_at, self.others = send_at, recv_at, others
        self.send, self.recv = sems.at[0], sems.at[1]
        self.me = lax.axis_index(axis)

    def start(self):
        middle = self.size // 2

        @pl.loop(1, self.size)
        def _(i):
            away = jnp.where(i % 2 == 0, middle - i // 2, middle + i // 2)
            to = lax.rem(self.me + away, self.size)
            pltpu.make_async_remote_copy(
                src_ref=self.send_at(to),
                dst_ref=self.recv_at(self.me),
                send_sem=self.send,
                recv_sem=self.recv,
                device_id={self.axis: to},
                device_id_type=MESH,
            ).start()

    def wait(self):
        arrived(self.others, self.recv)
        arrived(self.others, self.send)


class Spread:
    def __init__(self, grid, ref, sems):
        self.ny, self.nx = grid
        self.ref, self.sems = ref, sems
        self.y, self.x = split_tp(self.nx)
        self.ep, self.tp = lax.axis_index("ep"), lax.axis_index("tp")
        half = ref.shape[0] // 2
        self.upper, self.lower = pl.ds(0, half), pl.ds(half, half)

    def _send(self, ref, y, x, stage):
        pltpu.make_async_remote_copy(
            src_ref=ref,
            dst_ref=ref,
            send_sem=self.sems.at[stage],
            recv_sem=self.sems.at[4 + stage],
            device_id=(self.ep, y * self.nx + x),
            device_id_type=MESH,
        ).start()

    def _wait(self, rows, blocks, stage):
        ref = self.ref.at[rows, pl.ds(0, blocks * LANES)]
        arrived(ref, self.sems.at[4 + stage])
        return lambda: arrived(ref, self.sems.at[stage])

    def start(self):
        for i in range(1, self.nx):
            self._send(self.ref.at[self.upper, block(self.tp)], self.y, lax.rem(self.x + i, self.nx), 0)
        for i in range(1, self.ny):
            self._send(self.ref.at[self.lower, block(self.tp)], lax.rem(self.y + i, self.ny), self.x, 1)

    def relay(self):
        sent = [self._wait(self.upper, self.nx - 1, 0), self._wait(self.lower, self.ny - 1, 1)]
        for i in range(1, self.ny):
            ref = self.ref.at[self.upper, block(self.y, self.nx * LANES)]
            self._send(ref, lax.rem(self.y + i, self.ny), self.x, 2)
        for i in range(1, self.nx):
            for y in range(self.ny):
                ref = self.ref.at[self.lower, block(y * self.nx + self.x)]
                self._send(ref, self.y, lax.rem(self.x + i, self.nx), 3)
        for wait in sent:
            wait()

    def wait(self):
        blocks = (self.nx - 1) * self.ny
        sent = [self._wait(self.upper, (self.ny - 1) * self.nx, 2), self._wait(self.lower, blocks, 3)]
        for wait in sent:
            wait()


class Routing:
    def __init__(self, tokens, experts, cap):
        self.tokens, self.experts, self.cap = tokens, experts, cap

    @staticmethod
    def _iota(shape, dim):
        return lax.broadcasted_iota(jnp.int32, shape, dim)

    @staticmethod
    def _ones(cond):
        return jnp.where(cond, 1.0, 0.0).astype(bf16)

    def to_slots(self, routes_t):
        n, e = self.tokens, self.experts
        expert = self._iota((e, n), 0)
        member = self._ones(jnp.logical_or(expert == routes_t[0:1, :], expert == routes_t[1:2, :]))
        earlier = self._ones(self._iota((n, n), 0) < self._iota((n, n), 1))
        place = jnp.dot(member, earlier, preferred_element_type=f32).astype(bf16)
        spread = self._ones(self._iota((e * PAD, e), 0) // PAD == self._iota((e * PAD, e), 1))
        member = jnp.dot(spread, member, preferred_element_type=f32)
        place = jnp.dot(spread, place, preferred_element_type=f32)
        here = (self._iota((e * PAD, n), 0) % PAD).astype(f32)
        return self._ones(jnp.logical_and(member > 0.5, place == here))

    def column(self, row):
        n = self.tokens
        same = self._iota((n, n), 0) == self._iota((n, n), 1)
        return jnp.sum(jnp.where(same, row.astype(f32), 0.0), axis=1, keepdims=True)

    def from_slots(self, routes_t):
        n, e = self.tokens, self.experts
        expert = self._iota((n, e), 1).astype(f32)
        members = [self._ones(expert == self.column(routes_t[k : k + 1, :])) for k in range(TOP_K)]
        earlier = self._ones(self._iota((n, n), 1) < self._iota((n, n), 0))
        place = jnp.dot(earlier, members[0] + members[1], preferred_element_type=f32).astype(bf16)
        spread = self._ones(self._iota((e, e * PAD), 1) // PAD == self._iota((e, e * PAD), 0))
        place = jnp.dot(place, spread, preferred_element_type=f32)
        here = (self._iota((n, e * PAD), 1) % PAD).astype(f32)
        out = []
        for member in members:
            member = jnp.dot(member, spread, preferred_element_type=f32)
            out.append(self._ones(jnp.logical_and(member > 0.5, place == here)))
        return out

    def packing(self, transposed):
        small, large = self.experts * self.cap, self.experts * PAD
        shape, dims = ((large, small), (1, 0)) if transposed else ((small, large), (0, 1))
        row, col = self._iota(shape, dims[0]), self._iota(shape, dims[1])
        return self._ones(jnp.logical_and(row == col // PAD * self.cap + col % PAD, col % PAD < self.cap))


def swiglu(x, weights):
    both = jnp.dot(x, weights, preferred_element_type=f32)
    gate, up = both[:, :LANES], both[:, LANES:]
    return (gate / (1.0 + jnp.exp(-gate)) * up).astype(bf16)


class Ring:
    def __init__(self, nz, kbuf, vbuf, recv, handed_recv, up_send, down_send, pass_send):
        self.nz = nz
        self.up_steps, self.down_steps = nz // 2, nz - 1 - nz // 2
        self.kbuf, self.vbuf = kbuf, vbuf
        self.recv, self.handed_recv = recv, handed_recv
        self.up_send, self.down_send, self.pass_send = up_send, down_send, pass_send
        ep = lax.axis_index("ep")
        self.tp = lax.axis_index("tp")
        self.z, self.c = ep // CORES, ep % CORES

    def _device(self, z, c):
        return (z * CORES + c, self.tp)

    def _piece(self, slot, part):
        buf = self.kbuf if part < 2 else self.vbuf
        half = buf.shape[1] // 2
        return buf.at[slot, pl.ds(part % 2 * half, half)]

    def _copy(self, source, part, to_z, sems):
        ref = self._piece(source * CORES + self.c, part)
        return pltpu.make_async_remote_copy(
            src_ref=ref,
            dst_ref=ref,
            send_sem=sems.at[part],
            recv_sem=self.recv.at[source, part],
            device_id=self._device(to_z, self.c),
            device_id_type=MESH,
        )

    def up(self, source, part):
        return self._copy(source, part, lax.rem(self.z + 1, self.nz), self.up_send)

    def down(self, source, part):
        return self._copy(source, part, lax.rem(self.z + self.nz - 1, self.nz), self.down_send)

    def _hand(self, source, way):
        for buf in (self.kbuf, self.vbuf):
            ref = buf.at[source * CORES + self.c]
            pltpu.make_async_remote_copy(
                src_ref=ref,
                dst_ref=ref,
                send_sem=self.pass_send.at[way],
                recv_sem=self.handed_recv.at[source],
                device_id=self._device(self.z, 1 - self.c),
                device_id_type=MESH,
            ).start()

    def _both(self, source):
        return self.kbuf.at[pl.ds(source * CORES, CORES)]

    def wait_handed(self, source):
        arrived(self._both(source), self.handed_recv.at[source])

    def _wait_hand_sent(self, way):
        arrived(self._both(0), self.pass_send.at[way])

    def up_source(self, t):
        return self.z - t, self.z - t >= 0

    def down_source(self, t):
        source = lax.rem(self.z + t, self.nz)
        return source, jnp.logical_and(source < self.down_steps, t <= self.down_steps)

    def down_used(self, t):
        source, here = self.down_source(t)
        return source, jnp.logical_and(here, source < self.z)

    def start_own(self):
        for part in range(PARTS):

            @pl.when(self.z < self.nz - 1)
            def _():
                self.up(self.z, part).start()

            @pl.when(self.z < self.down_steps)
            def _():
                self.down(self.z, part).start()

        @pl.when(self.c == 0)
        def _():
            self._hand(self.z, 0)

    def serve(self, t, part):
        source, here = self.up_source(t)

        @pl.when(here)
        def _():
            self.up(source, part).wait_recv()

            @pl.when(jnp.logical_and(t < self.up_steps, self.z < self.nz - 1))
            def _():
                self.up(source, part).wait_send()
                self.up(source, part).start()

        source_d, here_d = self.down_source(t)
        _, sent_before = self.down_source(t - 1)

        @pl.when(here_d)
        def _():
            self.down(source_d, part).wait_recv()

            @pl.when(t < self.down_steps)
            def _():
                @pl.when(sent_before)
                def _():
                    self.down(source_d, part).wait_send()

                self.down(source_d, part).start()

    def hand(self, t):
        source, here = self.up_source(t)

        @pl.when(here)
        def _():
            @pl.when(jnp.logical_or(t > 1, self.c == 0))
            def _():
                self._wait_hand_sent(0)

            self._hand(source, 0)

        source_d, used = self.down_used(t)
        _, used_before = self.down_used(t - 1)

        @pl.when(used)
        def _():
            @pl.when(used_before)
            def _():
                self._wait_hand_sent(1)

            self._hand(source_d, 1)

    def wait_sends(self):
        first_down = self.nz - self.down_steps

        @pl.when(self.z < self.nz - 1)
        def _():
            for part in range(PARTS):
                self.up(self.z, part).wait_send()

        @pl.when(jnp.logical_or(self.z < self.down_steps, self.z > first_down))
        def _():
            for part in range(PARTS):
                self.down(self.z, part).wait_send()

        @pl.when(jnp.logical_or(self.c == 0, self.z >= 1))
        def _():
            self._wait_hand_sent(0)

        @pl.when(self.z >= first_down)
        def _():
            self._wait_hand_sent(1)


class Softmax:
    def __init__(self, rows, tile, qz, kbuf, vbuf, top, acc, scores):
        self.rows, self.tile = rows, tile
        self.qz, self.kbuf, self.vbuf = qz, kbuf, vbuf
        self.top, self.acc, self.scores = top, acc, scores
        self.tiles = [pl.ds(i * tile, tile) for i in range(2 * rows // tile)]

    @staticmethod
    def _summed(p, values):
        ones = jnp.ones(values.shape, bf16)
        return jnp.dot(p.astype(bf16), jnp.concatenate([values, ones], axis=1), preferred_element_type=f32)

    def diagonal(self, slot):
        keys, values = self.kbuf[slot], self.vbuf[slot]
        for i, rows in enumerate(self.tiles):
            s = jnp.dot(self.qz[rows, :], keys, preferred_element_type=f32)
            row = i * self.tile + lax.broadcasted_iota(jnp.int32, s.shape, 0)
            row = jnp.where(row >= self.rows, row - self.rows, row)
            allowed = lax.broadcasted_iota(jnp.int32, s.shape, 1) <= row
            s = jnp.where(allowed, s, masked_low)
            top = jnp.max(s, axis=1, keepdims=True)
            p = jnp.where(allowed, jnp.exp(s - top), 0.0)
            self.top[rows, :] = jnp.broadcast_to(top, (self.tile, LANES))
            self.acc[rows, :] = self._summed(p, values)

    def _add(self, keys, values):
        count = keys.shape[1]
        cuts = [(j, min(2 * LANES, count - j)) for j in range(0, count, 2 * LANES)]
        tops = {}

        def score(i, j, width):
            s = jnp.dot(self.qz[self.tiles[i], :], keys[:, j : j + width], preferred_element_type=f32)
            self.scores[i % 2, :, j : j + width] = s
            for k in range(0, width, LANES):
                part = s[:, k : k + LANES]
                tops[i] = jnp.maximum(tops[i], part) if i in tops else part

        for j, width in cuts:
            score(0, j, width)
        for i, rows in enumerate(self.tiles):
            before = self.top[rows, :]
            top = jnp.maximum(before, jnp.max(tops[i], axis=1, keepdims=True))
            scale = jnp.exp(before - top)
            self.top[rows, :] = top
            total = self.acc[rows, :] * jnp.concatenate([scale, scale], axis=1)
            for j, width in cuts:
                if i + 1 < len(self.tiles):
                    score(i + 1, j, width)
                s = self.scores[i % 2, :, j : j + width]
                p = jnp.exp(s - jnp.concatenate([top] * (width // LANES), axis=1))
                total = total + self._summed(p, values[j : j + width])
            self.acc[rows, :] = total

    def one(self, slot):
        self._add(self.kbuf[slot], self.vbuf[slot])

    def chip(self, source):
        first, second = source * CORES, source * CORES + 1
        self._add(
            jnp.concatenate([self.kbuf[first], self.kbuf[second]], axis=1),
            jnp.concatenate([self.vbuf[first], self.vbuf[second]], axis=0),
        )

    def heads(self, lam, gain):
        acc = self.acc[...]
        out = acc[:, :LANES] / acc[:, LANES:]
        diff = out[: self.rows] - lam * out[self.rows :]
        mean = jnp.mean(diff * diff, axis=1, keepdims=True)
        return (diff * lax.rsqrt(mean + norm_eps) * gain).astype(bf16)


def kernel(dims, *refs):
    nz, ny, nx, rows, tile, tokens, experts, cap = dims
    refs = list(refs)

    def take(n):
        out = refs[:n]
        del refs[:n]
        return out

    inputs = take(8)
    (v_hbm,) = take(1)
    lam_ref, wo_hbm, wg_hbm, wu_hbm, wd_hbm, sg_hbm, su_hbm, sd_hbm = take(8)
    attn_hbm, moe_hbm = take(2)
    buffers = take(7)
    (load_sem,) = take(1)
    q_ref, k_ref, freq_ref, gain_ref, x_ref, fgain_ref, routes_ref = buffers
    kbuf, vbuf, qz, top, acc, scores = take(6)
    ring_sems = take(5)
    xn, wgu, sgu = take(3)
    out_slots, in_slots, xg, back_out, back_in = take(5)
    a_sems, g_sems, b_sems = take(3)
    attn_ref, moe_ref, rweight_ref, sine_ref, cosine_ref = take(5)
    grid = (ny, nx)
    ep, tp = lax.axis_index("ep"), lax.axis_index("tp")
    eps, tps = nz * CORES, ny * nx

    ring = Ring(nz, kbuf, vbuf, *ring_sems)
    soft = Softmax(rows, tile, qz, kbuf, vbuf, top, acc, scores)
    projections = []
    for axis, weight in zip(AXES, (wo_hbm, wo_hbm, wd_hbm, sd_hbm)):
        wb, hx, pr, rr, sems = take(5)
        projections.append(Projection(grid, axis, weight, wb, hx, pr, rr, sems))
    out_upper, out_lower, down, shared_down = projections
    half = rows // 2
    routing = Routing(tokens, experts, cap)

    barrier = pltpu.get_barrier_semaphore()
    for axis, me, size in (("ep", ep, eps), ("tp", tp, tps)):

        @pl.loop(1, size)
        def _(i):
            to = lax.rem(me + i, size)
            pl.semaphore_signal(barrier, inc=1, device_id={axis: to}, device_id_type=MESH)

    pairs = zip(inputs, buffers + [rweight_ref])
    loads = [pltpu.make_async_copy(a, b, load_sem.at[i]) for i, (a, b) in enumerate(pairs)]
    q_load, k_load, freq_load, gain_load, x_load, fgain_load, routes_load, rweight_load = loads
    weights = []
    for i, (source, buf, k) in enumerate(((sg_hbm, sgu, 0), (su_hbm, sgu, 1), (wg_hbm, wgu, 0), (wu_hbm, wgu, 1))):
        sem = load_sem.at[len(loads) + i]
        weights.append(pltpu.make_async_copy(source, buf.at[:, pl.ds(k * LANES, LANES)], sem))
    v_load = pltpu.make_async_copy(v_hbm, vbuf.at[ep], load_sem.at[len(loads) + 4])
    for load in (x_load, fgain_load, routes_load, freq_load, k_load, v_load, q_load, gain_load, rweight_load):
        load.start()
    for load in weights:
        load.start()
    for projection in projections:
        projection.start_own_weights()

    with jax.named_scope("pre_norm"):
        x_load.wait()
        fgain_load.wait()
        x = x_ref[...].astype(f32)
        inverse = lax.rsqrt(jnp.mean(x * x, axis=1, keepdims=True) + norm_eps)
        xn[...] = (x * inverse * fgain_ref[...]).astype(bf16)
    with jax.named_scope("pre_routes"):
        routes_load.wait()
        to_slots = routing.to_slots(routes_ref[...])
        sent = jnp.dot(to_slots, xn[:, block(tp)], preferred_element_type=f32).astype(bf16)
        out_slots[...] = sent.reshape(experts, PAD, LANES)
        in_slots[ep] = out_slots[ep]

    with jax.named_scope("barrier"):
        pl.semaphore_wait(barrier, eps + tps - 2)
    slots = pl.ds(0, eps - 1)
    there = Exchange("ep", eps, lambda i: out_slots.at[i], lambda i: in_slots.at[i], in_slots.at[slots], a_sems)
    spread = Spread(grid, xg, g_sems)
    back = Exchange("ep", eps, lambda i: back_out.at[i], lambda i: back_in.at[i], back_in.at[slots], b_sems)
    there.start()
    down.start_weights()
    shared_down.start_weights()

    with jax.named_scope("pre_angles"):
        freq_load.wait()
        cosine, sine = angle_tables(ep, rows, freq_ref[...])
        cosine_ref[...] = cosine
        sine_ref[...] = sine
    with jax.named_scope("pre_keys"):
        k_load.wait()
        kbuf[ep] = jnp.transpose(rotated(k_ref[...], cosine_ref[...], sine_ref[...])).astype(bf16)
        v_load.wait()
    ring.start_own()

    q_load.wait()
    q = rotated(q_ref[...], cosine_ref[...], sine_ref[...]).astype(bf16).astype(f32) * 0.125
    lane = lax.broadcasted_iota(jnp.int32, q.shape, 1)
    qz[:rows, :] = jnp.where(lane < 64, q, 0.0).astype(bf16)
    qz[rows:, :] = jnp.where(lane < 64, 0.0, q).astype(bf16)
    weights[0].wait()
    weights[1].wait()
    with jax.named_scope("shared_diagonal"):
        shared_down.start_gather(swiglu(xn[...], sgu[...]))
    with jax.named_scope("diagonal"):
        soft.diagonal(ep)

    @pl.when(ring.c == 1)
    def _():
        ring.wait_handed(ring.z)
        soft.one(ep - 1)

    def use(source):
        ring.wait_handed(source)
        soft.chip(source)

    def use_up(t):
        source, here = ring.up_source(t)

        @pl.when(jnp.logical_and(here, t >= 1))
        def _():
            with jax.named_scope("use_up"):
                use(source)

    def use_down(t):
        source, used = ring.down_used(t)

        @pl.when(used)
        def _():
            with jax.named_scope("use_down"):
                use(source)

    with jax.named_scope("there_wait"):
        there.wait()
    rows_in = in_slots[...].reshape(experts * PAD, LANES)
    rows_in = jnp.dot(routing.packing(False), rows_in, preferred_element_type=f32)
    xg[:, block(tp)] = rows_in.astype(bf16)
    spread.start()

    @pl.loop(1, ring.up_steps + 1)
    def _(t):
        with jax.named_scope("serve_0"):
            ring.serve(t, 0)
        use_up(t - 1)
        with jax.named_scope("serve_1_2"):
            ring.serve(t, 1)
            ring.serve(t, 2)
        use_down(t - 1)
        with jax.named_scope("serve_3"):
            ring.serve(t, 3)
            ring.hand(t)

        @pl.when(t == RELAY_AT)
        def _():
            with jax.named_scope("relay"):
                spread.relay()

        @pl.when(t == SHARED_AT)
        def _():
            with jax.named_scope("shared_multiply"):
                shared_down.wait_weights()
                shared_down.multiply_and_send()

        @pl.when(t == EXPERT_AT)
        def _():
            weights[2].wait()
            weights[3].wait()
            with jax.named_scope("spread_wait"):
                spread.wait()
            with jax.named_scope("experts"):
                down.start_gather(swiglu(xg[...], wgu[...]))
            out_upper.start_weights()
            out_lower.start_weights()

        @pl.when(t == DOWN_AT)
        def _():
            with jax.named_scope("down_multiply"):
                down.wait_weights()
                down.multiply_and_send()

        @pl.when(t == BACK_AT)
        def _():
            with jax.named_scope("down_finish"):
                y = down.finish().astype(bf16)
                y = jnp.dot(routing.packing(True), y, preferred_element_type=f32).astype(bf16)
                back_out[...] = y.reshape(experts, PAD, LANES)
                back_in[ep] = back_out[ep]
                back.start()

    use_up(ring.up_steps)
    gain_load.wait()
    with jax.named_scope("heads"):
        heads = soft.heads(lam_ref[0], gain_ref[...])
        out_upper.start_gather(heads[:half])
        out_lower.start_gather(heads[half:])
    with jax.named_scope("shared_finish"):
        mixed = shared_down.finish()
        chosen = routing.from_slots(routes_ref[...])
    with jax.named_scope("out_multiply"):
        for projection in (out_upper, out_lower):
            projection.wait_weights()
            projection.multiply_and_send()
    with jax.named_scope("wait_sends"):
        ring.wait_sends()
    with jax.named_scope("out_finish"):
        attn_ref[:half, :] = out_upper.finish().astype(bf16)
        attn_ref[half:, :] = out_lower.finish().astype(bf16)
    attn_store = pltpu.make_async_copy(attn_ref, attn_hbm, load_sem.at[1])
    attn_store.start()
    rweight_load.wait()
    with jax.named_scope("back_wait"):
        back.wait()
    returned = back_in[...].reshape(experts * PAD, LANES)
    for k in range(TOP_K):
        picked = jnp.dot(chosen[k], returned, preferred_element_type=f32)
        mixed = mixed + routing.column(rweight_ref[k : k + 1, :]) * picked
    moe_ref[...] = mixed.astype(bf16)
    moe_store = pltpu.make_async_copy(moe_ref, moe_hbm, load_sem.at[0])
    moe_store.start()
    moe_store.wait()
    attn_store.wait()


def hand_over(*refs):
    sources, targets, buffers, sems = refs[:2], refs[2:4], refs[4:6], refs[6]
    loads = [pltpu.make_async_copy(a, b, sems.at[i]) for i, (a, b) in enumerate(zip(sources, buffers))]
    stores = [pltpu.make_async_copy(a, b, sems.at[2 + i]) for i, (a, b) in enumerate(zip(buffers, targets))]
    for load in loads:
        load.start()
    for load, store in zip(loads, stores):
        load.wait()
        store.start()
    for store in stores:
        store.wait()


def local(
    sizes,
    query_pairs,
    key_pairs,
    value_rows,
    head_lambda,
    head_gain,
    out_weight,
    moe_input,
    ffn_gain,
    routes,
    route_weight,
    gate_weight,
    up_weight,
    down_weight,
    shared_gate,
    shared_up,
    shared_down,
):
    nz, ny, nx = sizes
    grid = (ny, nx)
    rows, tokens, width = query_pairs.shape[0], moe_input.shape[0], moe_input.shape[1]
    slots, experts = nz * CORES, nz * CORES
    cap = 12
    tile = 256 if (2 * rows) % 256 == 0 else 2 * rows
    hbm = pl.BlockSpec(memory_space=pl.ANY)
    dma = pltpu.SemaphoreType.DMA
    scratch = [
        pltpu.VMEM((rows, LANES), bf16),
        pltpu.VMEM((rows, LANES), bf16),
        pltpu.VMEM((1, LANES), f32),
        pltpu.VMEM((1, LANES), f32),
        pltpu.VMEM((tokens, width), bf16),
        pltpu.VMEM((1, width), f32),
        pltpu.VMEM((TOP_K, tokens), jnp.int32),
        dma((13,)),
        pltpu.VMEM((slots, LANES, rows), bf16),
        pltpu.VMEM((slots, rows, LANES), bf16),
        pltpu.VMEM((2 * rows, LANES), bf16),
        pltpu.VMEM((2 * rows, LANES), f32),
        pltpu.VMEM((2 * rows, 2 * LANES), f32),
        pltpu.VMEM((2, tile, CORES * rows), f32),
        dma((nz, PARTS)),
        dma((nz,)),
        dma((PARTS,)),
        dma((PARTS,)),
        dma((2,)),
        pltpu.VMEM((tokens, width), bf16),
        pltpu.VMEM((width, 2 * LANES), bf16),
        pltpu.VMEM((width, 2 * LANES), bf16),
        pltpu.VMEM((experts, PAD, LANES), bf16),
        pltpu.VMEM((experts, PAD, LANES), bf16),
        pltpu.VMEM((experts * cap, width), bf16),
        pltpu.VMEM((experts, PAD, LANES), bf16),
        pltpu.VMEM((experts, PAD, LANES), bf16),
        dma((2,)),
        dma((8,)),
        dma((2,)),
        pltpu.VMEM((rows, LANES), bf16),
        pltpu.VMEM((tokens, LANES), bf16),
        pltpu.VMEM((TOP_K, tokens), f32),
        pltpu.VMEM((rows, LANES), f32),
        pltpu.VMEM((rows, LANES), f32),
    ]
    for axis, height in zip(AXES, (rows // 2, rows // 2, experts * cap, tokens)):
        scratch += Projection.scratch(grid, axis, height)
    results = (
        pl.pallas_call(
            functools.partial(kernel, (nz, ny, nx, rows, tile, tokens, experts, cap)),
            out_shape=[
                jax.ShapeDtypeStruct((rows, LANES), bf16),
                jax.ShapeDtypeStruct((tokens, LANES), bf16),
            ],
            in_specs=[hbm] * 9 + [pl.BlockSpec(memory_space=pltpu.SMEM)] + [hbm] * 7,
            out_specs=[hbm, hbm],
            scratch_shapes=scratch,
            compiler_params=pltpu.CompilerParams(
                collective_id=0, has_side_effects=True, vmem_limit_bytes=56 * 1024 * 1024
            ),
            name="layer",
        )(
            query_pairs,
            key_pairs,
            frequencies(),
            head_gain.reshape(1, -1),
            moe_input,
            ffn_gain.reshape(1, -1),
            routes.T,
            route_weight.T,
            value_rows,
            head_lambda,
            out_weight,
            gate_weight[0],
            up_weight[0],
            down_weight[0],
            shared_gate,
            shared_up,
            shared_down,
        )
    )
    shapes = [jax.ShapeDtypeStruct(x.shape, x.dtype) for x in results]
    return tuple(
        pl.pallas_call(
            hand_over,
            out_shape=shapes,
            in_specs=[hbm, hbm],
            out_specs=[hbm, hbm],
            scratch_shapes=[pltpu.VMEM(s.shape, s.dtype) for s in shapes] + [dma((4,))],
            name="hand_over",
        )(*results)
    )


def grid_of(mesh):
    side = int(round(mesh.shape["tp"] ** 0.5))
    return mesh.shape["ep"] // CORES, mesh.shape["tp"] // side, side


def solution(mesh):
    return jax.shard_map(
        functools.partial(local, grid_of(mesh)),
        mesh=mesh,
        in_specs=(
            P("ep", "tp"),
            P("ep", "tp"),
            P("ep", "tp"),
            P("tp"),
            P(),
            P("tp", None),
            P("ep", None),
            P(),
            P("ep", None),
            P("ep", None),
            P("ep", None, "tp"),
            P("ep", None, "tp"),
            P("ep", "tp", None),
            P(None, "tp"),
            P(None, "tp"),
            P("tp", None),
        ),
        out_specs=(P("ep", "tp"), P("ep", "tp")),
        check_vma=False,
    )
```

```python
import functools

import jax
import jax.numpy as jnp
import numpy as np
from jax import lax
from jax.experimental import pallas as pl
from jax.experimental.pallas import tpu as pltpu
from jax.sharding import PartitionSpec as P

TOP_K = 2

theta_base = 500000.0
norm_eps = 1e-06
masked_low = -1e30

CORES = 2
LANES = 128
PAD = 16
PARTS = 4
MESH = pl.DeviceIdType.MESH
f32 = jnp.float32
bf16 = jnp.bfloat16

AXES = ("x", "y", "x", "y")
SAME = (True, True, False, True)
RELAY_AT, SHARED_AT, EXPERT_AT, DOWN_AT, BACK_AT = 1, 3, 4, 6, 7


def frequencies():
    place = (np.arange(LANES) % 32).astype(np.float32)
    return np.power(np.float32(theta_base), -(place * np.float32(2.0)) / np.float32(64)).reshape(1, LANES)


def angle_tables(ep, rows, frequency):
    quarter = rows // 4
    shape = (quarter, LANES)
    lane = lax.broadcasted_iota(jnp.int32, shape, 1)
    group = lane // 32
    positions = ep * rows + group * quarter + lax.broadcasted_iota(jnp.int32, shape, 0)
    angles = positions.astype(f32) * frequency
    sign = jnp.where(lane % 64 < 32, -1.0, 1.0)

    def spread(table, g):
        x = jnp.where(group == g, table, 0.0)
        x = x + pltpu.roll(x, 32, 1)
        return x + pltpu.roll(x, 64, 1)

    cosine, sine = jnp.cos(angles), jnp.sin(angles)
    return (
        jnp.concatenate([spread(cosine, g) for g in range(4)], axis=0),
        jnp.concatenate([spread(sine, g) * sign for g in range(4)], axis=0),
    )


def rotated(x, cosine, sine):
    x = x.astype(f32)
    lane = lax.broadcasted_iota(jnp.int32, x.shape, 1)
    swapped = jnp.where(lane % 64 < 32, pltpu.roll(x, 96, 1), pltpu.roll(x, 32, 1))
    return x * cosine + swapped * sine


def block(i, width=LANES):
    return pl.ds(pl.multiple_of(i * width, width), width)


def split_tp(nx):
    tp = lax.axis_index("tp")
    return tp // nx, tp % nx


def arrived(ref, sem):
    pltpu.make_async_copy(ref, ref, sem).wait()


class Projection:
    def __init__(self, grid, axis, same, w_hbm, wb, hx, pr, rr, sems):
        self.ny, self.nx = grid
        self.axis, self.same = axis, same
        self.w, self.wb, self.hx, self.pr, self.rr = w_hbm, wb, hx, pr, rr
        names = ("w_send", "w_recv", "w_local", "h_send", "h_recv", "p_send", "p_recv", "d_send", "d_recv")
        for i, name in enumerate(names):
            setattr(self, name, sems.at[i])
        y, x = split_tp(self.nx)
        self.g, self.o, self.ng, self.no = (y, x, self.ny, self.nx) if axis == "y" else (x, y, self.nx, self.ny)
        self.ep = lax.axis_index("ep")

    @staticmethod
    def scratch(grid, axis, rows):
        ng, no = grid if axis == "y" else grid[::-1]
        dma = pltpu.SemaphoreType.DMA
        return [
            pltpu.VMEM((ng * LANES, no * LANES), bf16),
            pltpu.VMEM((rows, ng * LANES), bf16),
            pltpu.VMEM((no, rows, LANES), bf16),
            pltpu.VMEM((no, rows, LANES), bf16),
            dma((9,)),
        ]

    def _tp(self, g, o):
        return g * self.nx + o if self.axis == "y" else o * self.nx + g

    def _weights(self, g, first, count):
        source = pl.ds(first, count)
        rows = pl.ds(pl.multiple_of(self.g * LANES + first, LANES // CORES), count)
        if self.axis == "y":
            yield self.w.at[source, block(g, self.no * LANES)], self.wb.at[rows, :]
            return
        for o in range(self.no):
            yield self.w.at[source, block(self._tp(g, o))], self.wb.at[rows, pl.ds(o * LANES, LANES)]

    def start_own_weights(self):
        for source, target in self._weights(self.g, 0, LANES):
            pltpu.make_async_copy(source, target, self.w_local).start()

    def _share(self):
        if not self.same:
            return 0, LANES
        count = LANES // CORES
        return pl.multiple_of(lax.rem(self.ep, CORES) * count, count), count

    def _others(self):
        return self.wb.at[pl.ds(0, (self.ng - 1) * self._share()[1]), :]

    def start_weights(self):
        for i in range(1, self.ng):
            g = lax.rem(self.g + i, self.ng)
            for source, target in self._weights(g, *self._share()):
                pltpu.make_async_remote_copy(
                    src_ref=source,
                    dst_ref=target,
                    send_sem=self.w_send,
                    recv_sem=self.w_recv,
                    device_id=(self.ep, self._tp(g, self.o)),
                    device_id_type=MESH,
                ).start()

    def take_weights(self):
        arrived(self._others(), self.w_recv)
        arrived(self._others(), self.w_send)
        if not self.same:
            return
        first, count = self._share()
        for i in range(1, self.ng):
            g = lax.rem(self.g + i, self.ng)
            ref = self.wb.at[pl.ds(pl.multiple_of(g * LANES + first, count), count), :]
            pltpu.make_async_remote_copy(
                src_ref=ref,
                dst_ref=ref,
                send_sem=self.d_send,
                recv_sem=self.d_recv,
                device_id=(self.ep + 1 - 2 * lax.rem(self.ep, CORES), self._tp(self.g, self.o)),
                device_id_type=MESH,
            ).start()

    def wait_weights(self):
        arrived(self.wb.at[pl.ds(0, LANES), :], self.w_local)
        if self.same:
            arrived(self._others(), self.d_recv)
            arrived(self._others(), self.d_send)

    def _gather(self, i):
        own = self.hx.at[:, block(self.g)]
        return pltpu.make_async_remote_copy(
            src_ref=own,
            dst_ref=own,
            send_sem=self.h_send,
            recv_sem=self.h_recv,
            device_id=(self.ep, self._tp(lax.rem(self.g + i, self.ng), self.o)),
            device_id_type=MESH,
        )

    def start_gather(self, h):
        self.hx[:, block(self.g)] = h
        for i in range(1, self.ng):
            self._gather(i).start()

    def _partial(self, i):
        return pltpu.make_async_remote_copy(
            src_ref=self.pr.at[i],
            dst_ref=self.rr.at[i],
            send_sem=self.p_send,
            recv_sem=self.p_recv,
            device_id=(self.ep, self._tp(self.g, lax.rem(self.o + i, self.no))),
            device_id_type=MESH,
        )

    def multiply_and_send(self):
        others = self.hx.at[:, pl.ds(0, (self.ng - 1) * LANES)]
        arrived(others, self.h_recv)
        arrived(others, self.h_send)
        h = self.hx[...]
        for i in list(range(1, self.no)) + [0]:
            w = self.wb[:, block(lax.rem(self.o + i, self.no))]
            self.pr[i] = jnp.dot(h, w, preferred_element_type=f32).astype(bf16)
            if i:
                self._partial(i).start()

    def finish(self):
        others = self.rr.at[pl.ds(1, self.no - 1)]
        arrived(others, self.p_recv)
        arrived(others, self.p_send)
        total = self.pr[0].astype(f32)
        for i in range(1, self.no):
            total = total + self.rr[i].astype(f32)
        return total


class Exchange:
    def __init__(self, axis, size, send_at, recv_at, others, sems):
        self.axis, self.size = axis, size
        self.send_at, self.recv_at, self.others = send_at, recv_at, others
        self.send, self.recv = sems.at[0], sems.at[1]
        self.me = lax.axis_index(axis)

    def start(self):
        middle = self.size // 2

        @pl.loop(1, self.size)
        def _(i):
            away = jnp.where(i % 2 == 0, middle - i // 2, middle + i // 2)
            to = lax.rem(self.me + away, self.size)
            pltpu.make_async_remote_copy(
                src_ref=self.send_at(to),
                dst_ref=self.recv_at(self.me),
                send_sem=self.send,
                recv_sem=self.recv,
                device_id={self.axis: to},
                device_id_type=MESH,
            ).start()

    def wait(self):
        arrived(self.others, self.recv)
        arrived(self.others, self.send)


class Spread:
    def __init__(self, grid, ref, sems):
        self.ny, self.nx = grid
        self.ref, self.sems = ref, sems
        self.y, self.x = split_tp(self.nx)
        self.ep, self.tp = lax.axis_index("ep"), lax.axis_index("tp")
        half = ref.shape[0] // 2
        self.upper, self.lower = pl.ds(0, half), pl.ds(half, half)

    def _send(self, ref, y, x, stage):
        pltpu.make_async_remote_copy(
            src_ref=ref,
            dst_ref=ref,
            send_sem=self.sems.at[stage],
            recv_sem=self.sems.at[4 + stage],
            device_id=(self.ep, y * self.nx + x),
            device_id_type=MESH,
        ).start()

    def _wait(self, rows, blocks, stage):
        ref = self.ref.at[rows, pl.ds(0, blocks * LANES)]
        arrived(ref, self.sems.at[4 + stage])
        return lambda: arrived(ref, self.sems.at[stage])

    def start(self):
        for i in range(1, self.nx):
            self._send(self.ref.at[self.upper, block(self.tp)], self.y, lax.rem(self.x + i, self.nx), 0)
        for i in range(1, self.ny):
            self._send(self.ref.at[self.lower, block(self.tp)], lax.rem(self.y + i, self.ny), self.x, 1)

    def relay(self):
        sent = [self._wait(self.upper, self.nx - 1, 0), self._wait(self.lower, self.ny - 1, 1)]
        for i in range(1, self.ny):
            ref = self.ref.at[self.upper, block(self.y, self.nx * LANES)]
            self._send(ref, lax.rem(self.y + i, self.ny), self.x, 2)
        for i in range(1, self.nx):
            for y in range(self.ny):
                ref = self.ref.at[self.lower, block(y * self.nx + self.x)]
                self._send(ref, self.y, lax.rem(self.x + i, self.nx), 3)
        for wait in sent:
            wait()

    def wait(self):
        blocks = (self.nx - 1) * self.ny
        sent = [self._wait(self.upper, (self.ny - 1) * self.nx, 2), self._wait(self.lower, blocks, 3)]
        for wait in sent:
            wait()


class Routing:
    def __init__(self, tokens, experts, cap):
        self.tokens, self.experts, self.cap = tokens, experts, cap

    @staticmethod
    def _iota(shape, dim):
        return lax.broadcasted_iota(jnp.int32, shape, dim)

    @staticmethod
    def _ones(cond):
        return jnp.where(cond, 1.0, 0.0).astype(bf16)

    def to_slots(self, routes_t):
        n, e = self.tokens, self.experts
        expert = self._iota((e, n), 0)
        member = self._ones(jnp.logical_or(expert == routes_t[0:1, :], expert == routes_t[1:2, :]))
        earlier = self._ones(self._iota((n, n), 0) < self._iota((n, n), 1))
        place = jnp.dot(member, earlier, preferred_element_type=f32).astype(bf16)
        spread = self._ones(self._iota((e * PAD, e), 0) // PAD == self._iota((e * PAD, e), 1))
        member = jnp.dot(spread, member, preferred_element_type=f32)
        place = jnp.dot(spread, place, preferred_element_type=f32)
        here = (self._iota((e * PAD, n), 0) % PAD).astype(f32)
        return self._ones(jnp.logical_and(member > 0.5, place == here))

    def column(self, row):
        n = self.tokens
        same = self._iota((n, n), 0) == self._iota((n, n), 1)
        return jnp.sum(jnp.where(same, row.astype(f32), 0.0), axis=1, keepdims=True)

    def from_slots(self, routes_t):
        n, e = self.tokens, self.experts
        expert = self._iota((n, e), 1).astype(f32)
        members = [self._ones(expert == self.column(routes_t[k : k + 1, :])) for k in range(TOP_K)]
        earlier = self._ones(self._iota((n, n), 1) < self._iota((n, n), 0))
        place = jnp.dot(earlier, members[0] + members[1], preferred_element_type=f32).astype(bf16)
        spread = self._ones(self._iota((e, e * PAD), 1) // PAD == self._iota((e, e * PAD), 0))
        place = jnp.dot(place, spread, preferred_element_type=f32)
        here = (self._iota((n, e * PAD), 1) % PAD).astype(f32)
        out = []
        for member in members:
            member = jnp.dot(member, spread, preferred_element_type=f32)
            out.append(self._ones(jnp.logical_and(member > 0.5, place == here)))
        return out

    def packing(self, transposed):
        small, large = self.experts * self.cap, self.experts * PAD
        shape, dims = ((large, small), (1, 0)) if transposed else ((small, large), (0, 1))
        row, col = self._iota(shape, dims[0]), self._iota(shape, dims[1])
        return self._ones(jnp.logical_and(row == col // PAD * self.cap + col % PAD, col % PAD < self.cap))


def swiglu(x, weights):
    both = jnp.dot(x, weights, preferred_element_type=f32)
    gate, up = both[:, :LANES], both[:, LANES:]
    return (gate / (1.0 + jnp.exp(-gate)) * up).astype(bf16)


class Ring:
    def __init__(self, nz, kbuf, vbuf, recv, handed_recv, up_send, down_send, pass_send):
        self.nz = nz
        self.up_steps, self.down_steps = nz // 2, nz - 1 - nz // 2
        self.kbuf, self.vbuf = kbuf, vbuf
        self.recv, self.handed_recv = recv, handed_recv
        self.up_send, self.down_send, self.pass_send = up_send, down_send, pass_send
        ep = lax.axis_index("ep")
        self.tp = lax.axis_index("tp")
        self.z, self.c = ep // CORES, ep % CORES

    def _device(self, z, c):
        return (z * CORES + c, self.tp)

    def _piece(self, slot, part):
        buf = self.kbuf if part < 2 else self.vbuf
        half = buf.shape[1] // 2
        return buf.at[slot, pl.ds(part % 2 * half, half)]

    def _copy(self, source, part, to_z, sems):
        ref = self._piece(source * CORES + self.c, part)
        return pltpu.make_async_remote_copy(
            src_ref=ref,
            dst_ref=ref,
            send_sem=sems.at[part],
            recv_sem=self.recv.at[source, part],
            device_id=self._device(to_z, self.c),
            device_id_type=MESH,
        )

    def up(self, source, part):
        return self._copy(source, part, lax.rem(self.z + 1, self.nz), self.up_send)

    def down(self, source, part):
        return self._copy(source, part, lax.rem(self.z + self.nz - 1, self.nz), self.down_send)

    def _hand(self, source, way):
        for buf in (self.kbuf, self.vbuf):
            ref = buf.at[source * CORES + self.c]
            pltpu.make_async_remote_copy(
                src_ref=ref,
                dst_ref=ref,
                send_sem=self.pass_send.at[way],
                recv_sem=self.handed_recv.at[source],
                device_id=self._device(self.z, 1 - self.c),
                device_id_type=MESH,
            ).start()

    def _both(self, source):
        return self.kbuf.at[pl.ds(source * CORES, CORES)]

    def wait_handed(self, source):
        arrived(self._both(source), self.handed_recv.at[source])

    def _wait_hand_sent(self, way):
        arrived(self._both(0), self.pass_send.at[way])

    def up_source(self, t):
        return self.z - t, self.z - t >= 0

    def down_source(self, t):
        source = lax.rem(self.z + t, self.nz)
        return source, jnp.logical_and(source < self.down_steps, t <= self.down_steps)

    def down_used(self, t):
        source, here = self.down_source(t)
        return source, jnp.logical_and(here, source < self.z)

    def start_own(self):
        for part in range(PARTS):

            @pl.when(self.z < self.nz - 1)
            def _():
                self.up(self.z, part).start()

            @pl.when(self.z < self.down_steps)
            def _():
                self.down(self.z, part).start()

        @pl.when(self.c == 0)
        def _():
            self._hand(self.z, 0)

    def serve(self, t, part):
        source, here = self.up_source(t)

        @pl.when(here)
        def _():
            self.up(source, part).wait_recv()

            @pl.when(jnp.logical_and(t < self.up_steps, self.z < self.nz - 1))
            def _():
                self.up(source, part).wait_send()
                self.up(source, part).start()

        source_d, here_d = self.down_source(t)
        _, sent_before = self.down_source(t - 1)

        @pl.when(here_d)
        def _():
            self.down(source_d, part).wait_recv()

            @pl.when(t < self.down_steps)
            def _():
                @pl.when(sent_before)
                def _():
                    self.down(source_d, part).wait_send()

                self.down(source_d, part).start()

    def hand(self, t):
        source, here = self.up_source(t)

        @pl.when(here)
        def _():
            @pl.when(jnp.logical_or(t > 1, self.c == 0))
            def _():
                self._wait_hand_sent(0)

            self._hand(source, 0)

        source_d, used = self.down_used(t)
        _, used_before = self.down_used(t - 1)

        @pl.when(used)
        def _():
            @pl.when(used_before)
            def _():
                self._wait_hand_sent(1)

            self._hand(source_d, 1)

    def wait_sends(self):
        first_down = self.nz - self.down_steps

        @pl.when(self.z < self.nz - 1)
        def _():
            for part in range(PARTS):
                self.up(self.z, part).wait_send()

        @pl.when(jnp.logical_or(self.z < self.down_steps, self.z > first_down))
        def _():
            for part in range(PARTS):
                self.down(self.z, part).wait_send()

        @pl.when(jnp.logical_or(self.c == 0, self.z >= 1))
        def _():
            self._wait_hand_sent(0)

        @pl.when(self.z >= first_down)
        def _():
            self._wait_hand_sent(1)


class Softmax:
    def __init__(self, rows, tile, qz, kbuf, vbuf, top, acc, scores):
        self.rows, self.tile = rows, tile
        self.qz, self.kbuf, self.vbuf = qz, kbuf, vbuf
        self.top, self.acc, self.scores = top, acc, scores
        self.tiles = [pl.ds(i * tile, tile) for i in range(2 * rows // tile)]

    @staticmethod
    def _summed(p, values):
        ones = jnp.ones(values.shape, bf16)
        return jnp.dot(p.astype(bf16), jnp.concatenate([values, ones], axis=1), preferred_element_type=f32)

    def diagonal(self, slot):
        keys, values = self.kbuf[slot], self.vbuf[slot]
        for i, rows in enumerate(self.tiles):
            s = jnp.dot(self.qz[rows, :], keys, preferred_element_type=f32)
            row = i * self.tile + lax.broadcasted_iota(jnp.int32, s.shape, 0)
            row = jnp.where(row >= self.rows, row - self.rows, row)
            allowed = lax.broadcasted_iota(jnp.int32, s.shape, 1) <= row
            s = jnp.where(allowed, s, masked_low)
            top = jnp.max(s, axis=1, keepdims=True)
            p = jnp.where(allowed, jnp.exp(s - top), 0.0)
            self.top[rows, :] = jnp.broadcast_to(top, (self.tile, LANES))
            self.acc[rows, :] = self._summed(p, values)

    def _add(self, keys, values):
        count = keys.shape[1]
        cuts = [(j, min(2 * LANES, count - j)) for j in range(0, count, 2 * LANES)]
        tops = {}

        def score(i, j, width):
            s = jnp.dot(self.qz[self.tiles[i], :], keys[:, j : j + width], preferred_element_type=f32)
            self.scores[i % 2, :, j : j + width] = s
            for k in range(0, width, LANES):
                part = s[:, k : k + LANES]
                tops[i] = jnp.maximum(tops[i], part) if i in tops else part

        for j, width in cuts:
            score(0, j, width)
        for i, rows in enumerate(self.tiles):
            before = self.top[rows, :]
            top = jnp.maximum(before, jnp.max(tops[i], axis=1, keepdims=True))
            scale = jnp.exp(before - top)
            self.top[rows, :] = top
            total = self.acc[rows, :] * jnp.concatenate([scale, scale], axis=1)
            for j, width in cuts:
                if i + 1 < len(self.tiles):
                    score(i + 1, j, width)
                s = self.scores[i % 2, :, j : j + width]
                p = jnp.exp(s - jnp.concatenate([top] * (width // LANES), axis=1))
                total = total + self._summed(p, values[j : j + width])
            self.acc[rows, :] = total

    def one(self, slot):
        self._add(self.kbuf[slot], self.vbuf[slot])

    def chip(self, source):
        first, second = source * CORES, source * CORES + 1
        self._add(
            jnp.concatenate([self.kbuf[first], self.kbuf[second]], axis=1),
            jnp.concatenate([self.vbuf[first], self.vbuf[second]], axis=0),
        )

    def heads(self, lam, gain):
        acc = self.acc[...]
        out = acc[:, :LANES] / acc[:, LANES:]
        diff = out[: self.rows] - lam * out[self.rows :]
        mean = jnp.mean(diff * diff, axis=1, keepdims=True)
        return (diff * lax.rsqrt(mean + norm_eps) * gain).astype(bf16)


def kernel(dims, *refs):
    nz, ny, nx, rows, tile, tokens, experts, cap = dims
    refs = list(refs)

    def take(n):
        out = refs[:n]
        del refs[:n]
        return out

    inputs = take(8)
    (v_hbm,) = take(1)
    lam_ref, wo_hbm, wg_hbm, wu_hbm, wd_hbm, sg_hbm, su_hbm, sd_hbm = take(8)
    attn_hbm, moe_hbm = take(2)
    buffers = take(7)
    (load_sem,) = take(1)
    q_ref, k_ref, freq_ref, gain_ref, x_ref, fgain_ref, routes_ref = buffers
    kbuf, vbuf, qz, top, acc, scores = take(6)
    ring_sems = take(5)
    xn, wgu, sgu = take(3)
    out_slots, in_slots, xg, back_out, back_in = take(5)
    a_sems, g_sems, b_sems = take(3)
    attn_ref, moe_ref, rweight_ref, sine_ref, cosine_ref = take(5)
    grid = (ny, nx)
    ep, tp = lax.axis_index("ep"), lax.axis_index("tp")
    eps, tps = nz * CORES, ny * nx

    ring = Ring(nz, kbuf, vbuf, *ring_sems)
    soft = Softmax(rows, tile, qz, kbuf, vbuf, top, acc, scores)
    projections = []
    for axis, same, weight in zip(AXES, SAME, (wo_hbm, wo_hbm, wd_hbm, sd_hbm)):
        wb, hx, pr, rr, sems = take(5)
        projections.append(Projection(grid, axis, same, weight, wb, hx, pr, rr, sems))
    out_upper, out_lower, down, shared_down = projections
    half = rows // 2
    routing = Routing(tokens, experts, cap)

    barrier = pltpu.get_barrier_semaphore()
    for axis, me, size in (("ep", ep, eps), ("tp", tp, tps)):

        @pl.loop(1, size)
        def _(i):
            to = lax.rem(me + i, size)
            pl.semaphore_signal(barrier, inc=1, device_id={axis: to}, device_id_type=MESH)

    pairs = zip(inputs, buffers + [rweight_ref])
    loads = [pltpu.make_async_copy(a, b, load_sem.at[i]) for i, (a, b) in enumerate(pairs)]
    q_load, k_load, freq_load, gain_load, x_load, fgain_load, routes_load, rweight_load = loads
    weights = []
    for i, (source, buf, k) in enumerate(((sg_hbm, sgu, 0), (su_hbm, sgu, 1), (wg_hbm, wgu, 0), (wu_hbm, wgu, 1))):
        sem = load_sem.at[len(loads) + i]
        weights.append(pltpu.make_async_copy(source, buf.at[:, pl.ds(k * LANES, LANES)], sem))
    v_load = pltpu.make_async_copy(v_hbm, vbuf.at[ep], load_sem.at[len(loads) + 4])
    for load in (x_load, fgain_load, routes_load, freq_load, k_load, v_load, q_load, gain_load, rweight_load):
        load.start()
    for load in weights:
        load.start()
    for projection in projections:
        projection.start_own_weights()

    with jax.named_scope("pre_norm"):
        x_load.wait()
        fgain_load.wait()
        x = x_ref[...].astype(f32)
        inverse = lax.rsqrt(jnp.mean(x * x, axis=1, keepdims=True) + norm_eps)
        xn[...] = (x * inverse * fgain_ref[...]).astype(bf16)
    with jax.named_scope("pre_routes"):
        routes_load.wait()
        to_slots = routing.to_slots(routes_ref[...])
        sent = jnp.dot(to_slots, xn[:, block(tp)], preferred_element_type=f32).astype(bf16)
        out_slots[...] = sent.reshape(experts, PAD, LANES)
        in_slots[ep] = out_slots[ep]

    with jax.named_scope("barrier"):
        pl.semaphore_wait(barrier, eps + tps - 2)
    slots = pl.ds(0, eps - 1)
    there = Exchange("ep", eps, lambda i: out_slots.at[i], lambda i: in_slots.at[i], in_slots.at[slots], a_sems)
    spread = Spread(grid, xg, g_sems)
    back = Exchange("ep", eps, lambda i: back_out.at[i], lambda i: back_in.at[i], back_in.at[slots], b_sems)
    there.start()
    down.start_weights()
    shared_down.start_weights()
    out_lower.start_weights()

    with jax.named_scope("pre_angles"):
        freq_load.wait()
        cosine, sine = angle_tables(ep, rows, freq_ref[...])
        cosine_ref[...] = cosine
        sine_ref[...] = sine
    with jax.named_scope("pre_keys"):
        k_load.wait()
        kbuf[ep] = jnp.transpose(rotated(k_ref[...], cosine_ref[...], sine_ref[...])).astype(bf16)
        v_load.wait()
    ring.start_own()

    q_load.wait()
    q = rotated(q_ref[...], cosine_ref[...], sine_ref[...]).astype(bf16).astype(f32) * 0.125
    lane = lax.broadcasted_iota(jnp.int32, q.shape, 1)
    qz[:rows, :] = jnp.where(lane < 64, q, 0.0).astype(bf16)
    qz[rows:, :] = jnp.where(lane < 64, 0.0, q).astype(bf16)
    weights[0].wait()
    weights[1].wait()
    with jax.named_scope("shared_diagonal"):
        shared_down.start_gather(swiglu(xn[...], sgu[...]))
    with jax.named_scope("diagonal"):
        soft.diagonal(ep)

    @pl.when(ring.c == 1)
    def _():
        ring.wait_handed(ring.z)
        soft.one(ep - 1)

    def use(source):
        ring.wait_handed(source)
        soft.chip(source)

    def use_up(t):
        source, here = ring.up_source(t)

        @pl.when(jnp.logical_and(here, t >= 1))
        def _():
            with jax.named_scope("use_up"):
                use(source)

    def use_down(t):
        source, used = ring.down_used(t)

        @pl.when(used)
        def _():
            with jax.named_scope("use_down"):
                use(source)

    with jax.named_scope("there_wait"):
        there.wait()
    rows_in = in_slots[...].reshape(experts * PAD, LANES)
    rows_in = jnp.dot(routing.packing(False), rows_in, preferred_element_type=f32)
    xg[:, block(tp)] = rows_in.astype(bf16)
    spread.start()

    @pl.loop(1, ring.up_steps + 1)
    def _(t):
        with jax.named_scope("serve_0"):
            ring.serve(t, 0)
        use_up(t - 1)
        with jax.named_scope("serve_1_2"):
            ring.serve(t, 1)
            ring.serve(t, 2)
        use_down(t - 1)
        with jax.named_scope("serve_3"):
            ring.serve(t, 3)
            ring.hand(t)

        @pl.when(t == RELAY_AT)
        def _():
            with jax.named_scope("relay"):
                spread.relay()
            shared_down.take_weights()

        @pl.when(t == SHARED_AT)
        def _():
            with jax.named_scope("shared_multiply"):
                shared_down.wait_weights()
                shared_down.multiply_and_send()
            out_lower.take_weights()

        @pl.when(t == EXPERT_AT)
        def _():
            weights[2].wait()
            weights[3].wait()
            with jax.named_scope("spread_wait"):
                spread.wait()
            with jax.named_scope("experts"):
                down.start_gather(swiglu(xg[...], wgu[...]))
            out_upper.start_weights()

        @pl.when(t == DOWN_AT)
        def _():
            with jax.named_scope("down_multiply"):
                down.take_weights()
                down.wait_weights()
                down.multiply_and_send()

        @pl.when(t == BACK_AT)
        def _():
            with jax.named_scope("down_finish"):
                y = down.finish().astype(bf16)
                y = jnp.dot(routing.packing(True), y, preferred_element_type=f32).astype(bf16)
                back_out[...] = y.reshape(experts, PAD, LANES)
                back_in[ep] = back_out[ep]
                back.start()
            out_upper.take_weights()

    use_up(ring.up_steps)
    gain_load.wait()
    with jax.named_scope("heads"):
        heads = soft.heads(lam_ref[0], gain_ref[...])
        out_upper.start_gather(heads[:half])
        out_lower.start_gather(heads[half:])
    with jax.named_scope("shared_finish"):
        mixed = shared_down.finish()
        chosen = routing.from_slots(routes_ref[...])
    with jax.named_scope("out_multiply"):
        for projection in (out_upper, out_lower):
            projection.wait_weights()
            projection.multiply_and_send()
    with jax.named_scope("wait_sends"):
        ring.wait_sends()
    with jax.named_scope("out_finish"):
        attn_ref[:half, :] = out_upper.finish().astype(bf16)
        attn_ref[half:, :] = out_lower.finish().astype(bf16)
    attn_store = pltpu.make_async_copy(attn_ref, attn_hbm, load_sem.at[1])
    attn_store.start()
    rweight_load.wait()
    with jax.named_scope("back_wait"):
        back.wait()
    returned = back_in[...].reshape(experts * PAD, LANES)
    for k in range(TOP_K):
        picked = jnp.dot(chosen[k], returned, preferred_element_type=f32)
        mixed = mixed + routing.column(rweight_ref[k : k + 1, :]) * picked
    moe_ref[...] = mixed.astype(bf16)
    moe_store = pltpu.make_async_copy(moe_ref, moe_hbm, load_sem.at[0])
    moe_store.start()
    moe_store.wait()
    attn_store.wait()


def hand_over(*refs):
    sources, targets, buffers, sems = refs[:2], refs[2:4], refs[4:6], refs[6]
    loads = [pltpu.make_async_copy(a, b, sems.at[i]) for i, (a, b) in enumerate(zip(sources, buffers))]
    stores = [pltpu.make_async_copy(a, b, sems.at[2 + i]) for i, (a, b) in enumerate(zip(buffers, targets))]
    for load in loads:
        load.start()
    for load, store in zip(loads, stores):
        load.wait()
        store.start()
    for store in stores:
        store.wait()


def local(
    sizes,
    query_pairs,
    key_pairs,
    value_rows,
    head_lambda,
    head_gain,
    out_weight,
    moe_input,
    ffn_gain,
    routes,
    route_weight,
    gate_weight,
    up_weight,
    down_weight,
    shared_gate,
    shared_up,
    shared_down,
):
    nz, ny, nx = sizes
    grid = (ny, nx)
    rows, tokens, width = query_pairs.shape[0], moe_input.shape[0], moe_input.shape[1]
    slots, experts = nz * CORES, nz * CORES
    cap = 12
    tile = 256 if (2 * rows) % 256 == 0 else 2 * rows
    hbm = pl.BlockSpec(memory_space=pl.ANY)
    dma = pltpu.SemaphoreType.DMA
    scratch = [
        pltpu.VMEM((rows, LANES), bf16),
        pltpu.VMEM((rows, LANES), bf16),
        pltpu.VMEM((1, LANES), f32),
        pltpu.VMEM((1, LANES), f32),
        pltpu.VMEM((tokens, width), bf16),
        pltpu.VMEM((1, width), f32),
        pltpu.VMEM((TOP_K, tokens), jnp.int32),
        dma((13,)),
        pltpu.VMEM((slots, LANES, rows), bf16),
        pltpu.VMEM((slots, rows, LANES), bf16),
        pltpu.VMEM((2 * rows, LANES), bf16),
        pltpu.VMEM((2 * rows, LANES), f32),
        pltpu.VMEM((2 * rows, 2 * LANES), f32),
        pltpu.VMEM((2, tile, CORES * rows), f32),
        dma((nz, PARTS)),
        dma((nz,)),
        dma((PARTS,)),
        dma((PARTS,)),
        dma((2,)),
        pltpu.VMEM((tokens, width), bf16),
        pltpu.VMEM((width, 2 * LANES), bf16),
        pltpu.VMEM((width, 2 * LANES), bf16),
        pltpu.VMEM((experts, PAD, LANES), bf16),
        pltpu.VMEM((experts, PAD, LANES), bf16),
        pltpu.VMEM((experts * cap, width), bf16),
        pltpu.VMEM((experts, PAD, LANES), bf16),
        pltpu.VMEM((experts, PAD, LANES), bf16),
        dma((2,)),
        dma((8,)),
        dma((2,)),
        pltpu.VMEM((rows, LANES), bf16),
        pltpu.VMEM((tokens, LANES), bf16),
        pltpu.VMEM((TOP_K, tokens), f32),
        pltpu.VMEM((rows, LANES), f32),
        pltpu.VMEM((rows, LANES), f32),
    ]
    for axis, height in zip(AXES, (rows // 2, rows // 2, experts * cap, tokens)):
        scratch += Projection.scratch(grid, axis, height)
    results = (
        pl.pallas_call(
            functools.partial(kernel, (nz, ny, nx, rows, tile, tokens, experts, cap)),
            out_shape=[
                jax.ShapeDtypeStruct((rows, LANES), bf16),
                jax.ShapeDtypeStruct((tokens, LANES), bf16),
            ],
            in_specs=[hbm] * 9 + [pl.BlockSpec(memory_space=pltpu.SMEM)] + [hbm] * 7,
            out_specs=[hbm, hbm],
            scratch_shapes=scratch,
            compiler_params=pltpu.CompilerParams(
                collective_id=0, has_side_effects=True, vmem_limit_bytes=56 * 1024 * 1024
            ),
            name="layer",
        )(
            query_pairs,
            key_pairs,
            frequencies(),
            head_gain.reshape(1, -1),
            moe_input,
            ffn_gain.reshape(1, -1),
            routes.T,
            route_weight.T,
            value_rows,
            head_lambda,
            out_weight,
            gate_weight[0],
            up_weight[0],
            down_weight[0],
            shared_gate,
            shared_up,
            shared_down,
        )
    )
    shapes = [jax.ShapeDtypeStruct(x.shape, x.dtype) for x in results]
    return tuple(
        pl.pallas_call(
            hand_over,
            out_shape=shapes,
            in_specs=[hbm, hbm],
            out_specs=[hbm, hbm],
            scratch_shapes=[pltpu.VMEM(s.shape, s.dtype) for s in shapes] + [dma((4,))],
            name="hand_over",
        )(*results)
    )


def grid_of(mesh):
    side = int(round(mesh.shape["tp"] ** 0.5))
    return mesh.shape["ep"] // CORES, mesh.shape["tp"] // side, side


def solution(mesh):
    return jax.shard_map(
        functools.partial(local, grid_of(mesh)),
        mesh=mesh,
        in_specs=(
            P("ep", "tp"),
            P("ep", "tp"),
            P("ep", "tp"),
            P("tp"),
            P(),
            P("tp", None),
            P("ep", None),
            P(),
            P("ep", None),
            P("ep", None),
            P("ep", None, "tp"),
            P("ep", None, "tp"),
            P("ep", "tp", None),
            P(None, "tp"),
            P(None, "tp"),
            P("tp", None),
        ),
        out_specs=(P("ep", "tp"), P("ep", "tp")),
        check_vma=False,
    )
```
